256 devices in a mesh: sp: 16 (over y, x), tp: 16 (over z, core).
Axes of the slice: x: 4, y: 4, z: 8, core: 2. Of those that a mesh axis runs over, the one named last changes fastest.
Arguments:
- moe_input: bfloat16 [4096, 4096], P('sp', 'tp'), may hold values from -6 to 6
- out_gate: bfloat16 [4096, 4096], P('sp', 'tp'), may hold values from -6 to 6
- in_gate: bfloat16 [4096, 4096], P('sp', 'tp'), may hold values from -6 to 6
- values: bfloat16 [4096, 4096], P('sp', 'tp'), may hold values from -6 to 6
- conv_taps: float32 [3, 4096], P(None, 'tp'), may hold values from -3 to 3
- out_proj: bfloat16 [4096, 4096], P(None, 'tp'), may hold values from -0.09375 to 0.09375
- route_ids: int32 [4096, 2], P('sp'), may hold values from 0 to 15, all different within a row; in each aligned block of 256 rows (0 to 255, 256 to 511, ...) at most 48 rows name the same one
- route_gates: float32 [4096, 2], P('sp'), may hold values from 0.1 to 0.9
- expert_gate: bfloat16 [16, 4096, 2048], P('sp', None, 'tp'), may hold values from -0.09375 to 0.09375
- expert_up: bfloat16 [16, 4096, 2048], P('sp', None, 'tp'), may hold values from -0.09375 to 0.09375
- expert_down: bfloat16 [16, 2048, 4096], P('sp', 'tp'), may hold values from -0.125 to 0.125
- cotangent: bfloat16 [4096, 4096], P('sp', 'tp'), may hold values from -6 to 6
Outputs:
- grad_out_gate: bfloat16 [4096, 4096], P('sp', 'tp')
- grad_in_gate: bfloat16 [4096, 4096], P('sp', 'tp')
- grad_values: bfloat16 [4096, 4096], P('sp', 'tp')
- grad_out_proj: float32 [4096, 4096], P('sp', 'tp')
- grad_expert_gate: float32 [16, 4096, 2048], P('sp', None, 'tp')
- grad_expert_up: float32 [16, 4096, 2048], P('sp', None, 'tp')
- grad_expert_down: float32 [16, 2048, 4096], P('sp', 'tp')
The draws below stay inside these ranges and needn't reach their ends.
Inputs may be any that keep to these rules, and one draw needn't show every extreme that they name: `route_ids`: the 2 experts of a token differ. In the rows of one device no expert is named by more than 48 assignments, and in some device's rows some expert is named by exactly 48.
All inputs are finite; a program needn't handle non-finite values.
Results may differ from the reference program's by a relative error of at most 0.014.
Values may be sent and summed in bfloat16 or wider, within the bound.
A program may use at most 128 MiB of HBM per device.

```python
import math
import jax
import jax.numpy as jnp
import numpy as np
from jax import lax

D = 4096
C = 4096
F = 2048
TOP = 2
TOK = 256
EXPERTS = 16
CAP = 48
TOKENS = 4096
N_SP = 16


def strengthened(drawn, rng, source, target, blocks, factor):
    def block_of(dim):
        return (jnp.arange(drawn.shape[dim]) // (drawn.shape[dim] // blocks)).reshape((-1,) + (1,) * (drawn.ndim - 1 - dim))

    one_side = jax.random.permutation(rng, blocks)[block_of(target)]
    far = (block_of(target) + blocks // 2) % blocks
    return jnp.where((block_of(source) == one_side) | (block_of(source) == far), factor * drawn, drawn)


def steps_of(stream_key, shape, pieces, low, high):
    gain = 1.0
    for dim, parts in pieces:
        steps = jax.random.uniform(jax.random.fold_in(jax.random.fold_in(stream_key, 6), dim), (parts,), jnp.float32, low / len(pieces), high / len(pieces))
        gain = gain * jnp.repeat(jnp.exp(steps), shape[dim] // parts).reshape((-1,) + (1,) * (len(shape) - 1 - dim))
    return gain


def deal_out(key, own, number, rows, number_of, top, bound, slope):
    order = jax.random.permutation(key, number_of)
    crowded, common = load_shares(number_of, rows * top, bound, slope, True), load_shares(number_of, rows * top, bound, slope, False)
    places = jnp.arange(number_of)

    def named(sizes, turn):
        used = int((sizes > 0).sum())
        fixed = max(1, used // 4)
        moved = fixed + (places - fixed + turn * (used - fixed)) % max(1, number_of - fixed)
        return jnp.zeros((number_of,), jnp.int32).at[order[jnp.where(places < fixed, places, moved)]].set(jnp.asarray(sizes, jnp.int32))

    sizes = jnp.where(number % 4 == 0, named(crowded, number // 4), named(common, number - number // 4 - 1))
    mixed = jax.random.permutation(jax.random.fold_in(own, 3), number_of)
    source_of, receiver = mixed[0:number_of // 2 * 2:2], mixed[1:number_of // 2 * 2:2]
    margin = jnp.minimum(sizes[source_of] - 1, bound - sizes[receiver]) // 2
    margin = jnp.where((source_of == order[0]) | (receiver == order[0]) | (sizes[receiver] == 0), 0, jnp.maximum(margin, 0))
    moved = jax.random.randint(jax.random.fold_in(own, 4), (number_of // 2,), 0, 1 << 20) % (margin + 1)
    sizes = sizes.at[source_of].add(-moved).at[receiver].add(moved)
    items = jnp.searchsorted(jnp.cumsum(sizes), jnp.arange(rows * top), side="right").astype(jnp.int32)
    table = items.reshape(top, rows).T
    table = table[jax.random.permutation(jax.random.fold_in(own, 1), rows)]
    turn = jax.random.randint(jax.random.fold_in(own, 2), (rows, 1), 0, top)
    return jnp.take_along_axis(table, (jnp.arange(top)[None, :] + turn) % top, axis=1)


def load_shares(amount, total, bound, skew, full):
    loads = [(1 << 20) // math.isqrt(standing ** skew) + 1 for standing in range(1, amount + 1)]
    largest = bound if full else min(bound, max(-(-total // amount), total * loads[0] // sum(loads)))
    least = 1 if total - largest >= amount - 1 else 0
    holding, rest = [largest] + [least] * (amount - 1), total - largest - least * (amount - 1)
    while rest > 0:
        free = [i for i in range(1, amount) if holding[i] < largest] or [i for i in range(1, amount) if holding[i] < bound]
        whole, remaining = sum([loads[i] for i in free]), rest
        for i in free:
            addition = min(bound - holding[i], max(1, remaining * loads[i] // whole), rest)
            holding[i] = holding[i] + addition
            rest = rest - addition
    return np.array(holding)


def bell_draw(stream_key, shape, spread, most, cuts=(), kind=jnp.bfloat16):
    entries = spread * jax.random.normal(stream_key, shape, jnp.float32)
    if cuts:
        entries = entries * steps_of(stream_key, shape, cuts, -0.22, 0.18)
    return jnp.clip(entries, -most, most).astype(kind)


def gaussian_with(own_key, shape, scale, bound, split, heavy, kind=jnp.bfloat16):
    result = scale * jax.random.normal(own_key, shape, jnp.float32)
    if split:
        result = result * steps_of(own_key, shape, split, -0.22, 0.18)
    return jnp.clip(strengthened(result, jax.random.fold_in(own_key, 3), *heavy), -bound, bound).astype(kind)


def setup_inputs(seed: int = 0) -> dict:
    key_list = jax.random.split(jax.random.key(seed), 13)
    moe_input = bell_draw(key_list[0], (TOKENS, D), 1.0, 6.0, ((0, 16), (1, 16)))
    out_gate = bell_draw(key_list[1], (TOKENS, C), 1.0, 6.0, ((0, 16), (1, 16)))
    in_gate = bell_draw(key_list[2], (TOKENS, C), 1.0, 6.0, ((0, 16), (1, 16)))
    values = bell_draw(key_list[3], (TOKENS, C), 1.0, 6.0, ((0, 16), (1, 16)))
    conv_taps = bell_draw(key_list[4], (3, C), 0.5, 3.0, ((1, 16),), jnp.float32)
    out_proj = bell_draw(key_list[5], (D, C), C ** -0.5, 0.09375, ((1, 16),))
    route_ids_keys = jax.random.split(jax.random.fold_in(key_list[6], 1), TOKENS // TOK)
    route_ids_turns = jax.random.permutation(jax.random.fold_in(key_list[6], 3), TOKENS // TOK)
    route_ids = jax.vmap(lambda own, number: deal_out(jax.random.fold_in(key_list[6], 2), own, number, TOK, EXPERTS, TOP, CAP, 1))(route_ids_keys, route_ids_turns).reshape((TOKENS, TOP))
    route_gates = jnp.clip(0.1 + 0.79999997 * jax.random.uniform(key_list[7], (TOKENS, TOP), jnp.float32) ** steps_of(key_list[7], (TOKENS, TOP), ((0, 16),), -0.2, 0.2), 0.1, 0.9)
    expert_gate = bell_draw(key_list[8], (EXPERTS, D, F), D ** -0.5, 0.09375, ((0, 16), (2, 16)))
    expert_up = bell_draw(key_list[9], (EXPERTS, D, F), D ** -0.5, 0.09375, ((0, 16), (2, 16)))
    expert_down = bell_draw(key_list[10], (EXPERTS, F, D), F ** -0.5, 0.125, ((0, 16), (1, 16)))
    cotangent = gaussian_with(key_list[11], (TOKENS, D), 1.0, 6.0, ((0, 16), (1, 16)), (0, 1, 16, 2.0))
    return {"moe_input": moe_input, "out_gate": out_gate, "in_gate": in_gate, "values": values, "conv_taps": conv_taps, "out_proj": out_proj, "route_ids": route_ids, "route_gates": route_gates, "expert_gate": expert_gate, "expert_up": expert_up, "expert_down": expert_down, "cotangent": cotangent}


def reference(moe_input, out_gate, in_gate, values, conv_taps, out_proj, route_ids, route_gates, expert_gate, expert_up, expert_down, cotangent):
    slots = N_SP * CAP
    flat_ids = route_ids.reshape(-1)
    owner = jnp.arange(TOKENS * TOP, dtype=jnp.int32) // TOP
    one_hot = (flat_ids[:, None] == jnp.arange(EXPERTS, dtype=jnp.int32)[None, :]).astype(jnp.int32)
    blocked = one_hot.reshape(N_SP, TOK * TOP, EXPERTS)
    earlier = (jnp.cumsum(blocked, axis=1) - blocked).reshape(TOKENS * TOP, EXPERTS)
    position = jnp.sum(earlier * one_hot, axis=1).astype(jnp.int32)
    slot_index = (flat_ids * slots + (owner // TOK) * CAP + position).astype(jnp.int32)
    slot_token = jnp.full((EXPERTS * slots,), TOKENS, jnp.int32).at[slot_index].set(owner)
    slot_weight = jnp.zeros((EXPERTS * slots,), jnp.float32).at[slot_index].set(route_gates.reshape(-1))
    padded_input = jnp.concatenate([moe_input, jnp.zeros((1, D), moe_input.dtype)], axis=0)
    padded_cot = jnp.concatenate([cotangent, jnp.zeros((1, D), cotangent.dtype)], axis=0)
    contract_rows = (((0,), (0,)), ((), ()))
    contract_cols = (((1,), (1,)), ((), ()))

    def expert_backward(args):
        tokens_of, weights_of, gate_w, up_w, down_w = args
        rows = padded_input[tokens_of]
        routed = (weights_of[:, None] * padded_cot[tokens_of].astype(jnp.float32)).astype(jnp.bfloat16)
        pre_gate = jnp.dot(rows, gate_w, preferred_element_type=jnp.float32)
        pre_up = jnp.dot(rows, up_w, preferred_element_type=jnp.float32)
        gate_sig = jax.nn.sigmoid(pre_gate)
        activated = pre_gate * gate_sig
        hidden_act = (activated * pre_up).astype(jnp.bfloat16)
        grad_down = lax.dot_general(hidden_act, routed, contract_rows, preferred_element_type=jnp.float32)
        grad_hidden = lax.dot_general(routed, down_w, contract_cols, preferred_element_type=jnp.float32)
        grad_pre_gate = (grad_hidden * pre_up * gate_sig * (1.0 + pre_gate * (1.0 - gate_sig))).astype(jnp.bfloat16)
        grad_pre_up = (grad_hidden * activated).astype(jnp.bfloat16)
        grad_gate = lax.dot_general(rows, grad_pre_gate, contract_rows, preferred_element_type=jnp.float32)
        grad_up = lax.dot_general(rows, grad_pre_up, contract_rows, preferred_element_type=jnp.float32)
        assign = (lax.dot_general(grad_pre_gate, gate_w, contract_cols, preferred_element_type=jnp.float32)
                  + lax.dot_general(grad_pre_up, up_w, contract_cols, preferred_element_type=jnp.float32))
        return grad_gate, grad_up, grad_down, assign

    grad_expert_gate, grad_expert_up, grad_expert_down, assign = lax.map(
        expert_backward,
        (slot_token.reshape(EXPERTS, slots), slot_weight.reshape(EXPERTS, slots), expert_gate, expert_up, expert_down))
    flat_assign = assign.reshape(EXPERTS * slots, D)
    moe_grad = jnp.sum(flat_assign[slot_index].reshape(TOKENS, TOP, D), axis=1)
    mixer_cot = (cotangent.astype(jnp.float32) + moe_grad).astype(jnp.bfloat16)

    conv_in = in_gate.astype(jnp.float32) * values.astype(jnp.float32)
    rimmed = jnp.pad(conv_in, ((1, 1), (0, 0)))
    conv_out = rimmed[:-2] * conv_taps[0] + rimmed[1:-1] * conv_taps[1] + rimmed[2:] * conv_taps[2]
    mixed = (out_gate.astype(jnp.float32) * conv_out).astype(jnp.bfloat16)
    grad_mixed = jnp.dot(mixer_cot, out_proj, preferred_element_type=jnp.float32)
    grad_out_gate = (grad_mixed * conv_out).astype(jnp.bfloat16)
    grad_conv_out = grad_mixed * out_gate.astype(jnp.float32)
    rim_grad = jnp.pad(grad_conv_out, ((1, 1), (0, 0)))
    grad_conv_in = rim_grad[2:] * conv_taps[0] + rim_grad[1:-1] * conv_taps[1] + rim_grad[:-2] * conv_taps[2]
    grad_in_gate = (grad_conv_in * values.astype(jnp.float32)).astype(jnp.bfloat16)
    grad_values = (grad_conv_in * in_gate.astype(jnp.float32)).astype(jnp.bfloat16)
    grad_out_proj = lax.dot_general(mixer_cot, mixed, contract_rows, preferred_element_type=jnp.float32)
    return (grad_out_gate, grad_in_gate, grad_values, grad_out_proj, grad_expert_gate, grad_expert_up, grad_expert_down)
```

```python
import functools
import jax
import jax.numpy as jnp
from jax import lax
from jax.experimental import pallas as pl
from jax.experimental.pallas import tpu as pltpu
from jax.sharding import PartitionSpec as P

F32 = jnp.float32
BF16 = jnp.bfloat16
MESH = pl.DeviceIdType.MESH
NT = (((1,), (1,)), ((), ()))
TN = (((0,), (0,)), ((), ()))


def dot(a, b, dims):
    return lax.dot_general(a, b, dims, preferred_element_type=F32)


def moe_kernel(
    send_ref, wg_ref, wu_ref, wd_ref,
    ret_ref, gg_ref, gu_ref, gd_ref,
    rows, wgu, wd, acc, g2, hid, q, r, in_f, in_b, out_f, out_b, fin, grad_gu, grad_d,
    w_sem, disp_send, disp_recv,
    af_send, af_recv, ab_send, ab_recv, ap_send, ap_recv,
    rp_send, rp_recv, rf_send, rf_recv, rb_send, rb_recv,
    ret_send, ret_recv, out_sem,
):
    s = lax.axis_index("sp")
    t = lax.axis_index("tp")
    z, c = t // 2, t % 2
    y = s // 4
    up, down, mate = ((z + 1) % 8) * 2 + c, ((z + 7) % 8) * 2 + c, z * 2 + (1 - c)

    weights = [
        pltpu.make_async_copy(wg_ref, wgu.at[:, :, pl.ds(0, 128)], w_sem.at[0]),
        pltpu.make_async_copy(wu_ref, wgu.at[:, :, pl.ds(128, 128)], w_sem.at[1]),
        pltpu.make_async_copy(wd_ref, wd, w_sem.at[2]),
    ]
    for w in weights:
        w.start()

    barrier = pltpu.get_barrier_semaphore()

    @pl.loop(1, 16)
    def _(i):
        pl.semaphore_signal(barrier, inc=1, device_id={"sp": (s + i) % 16}, device_id_type=MESH)

    for other in (up, down, mate):
        pl.semaphore_signal(barrier, inc=1, device_id={"tp": other}, device_id_type=MESH)
    pl.semaphore_wait(barrier, 18)

    def remote(src, dst, send_sem, recv_sem, **where):
        return pltpu.make_async_remote_copy(
            src_ref=src, dst_ref=dst, send_sem=send_sem, recv_sem=recv_sem,
            device_id=where, device_id_type=MESH,
        )

    def dispatch(peer, source):
        return remote(
            send_ref.at[peer], rows.at[t, source], disp_send.at[peer], disp_recv.at[source], sp=peer
        )

    own = pltpu.make_async_copy(send_ref.at[s], rows.at[t, s], disp_recv.at[s])
    own.start()

    @pl.loop(1, 16)
    def _(i):
        dispatch((s + i) % 16, s).start()

    acc[...] = jnp.zeros_like(acc)
    for w in weights:
        w.wait()

    def part(k):
        return pl.ds(4 * ((y + 4 - k) % 4), 4)

    def slice_of(zz, core, k):
        return rows.at[zz * 2 + core, part(k)]

    def along_f(d, k):
        at = slice_of((z + 8 - d) % 8, c, k)
        return remote(at, at, af_send.at[d, k], af_recv.at[d, k], tp=up)

    def along_b(d, k):
        at = slice_of((z + d) % 8, c, k)
        return remote(at, at, ab_send.at[d, k], ab_recv.at[d, k], tp=down)

    def to_mate(zz, core, k):
        at = slice_of(zz, core, k)
        return remote(at, at, ap_send.at[zz, k], ap_recv.at[zz, k], tp=mate)

    def multiply(tt, k):
        block = rows[tt, part(k)].reshape(192, 512)
        pre = dot(block[:, :256], wgu[tt], (((1,), (0,)), ((), ())))
        columns = pl.ds(pl.multiple_of(tt * 256, 256), 256)
        hidden = dot(block[:, 256:], wd[:, columns], NT)
        acc[part(k), :, pl.ds(0, 256)] += pre.reshape(4, 48, 256)
        acc[part(k), :, pl.ds(256, 128)] += hidden.reshape(4, 48, 128)

    @pl.loop(0, 4)
    def _(k):
        for x in range(4):
            source = 4 * ((y + 4 - k) % 4) + x

            @pl.when(source == s)
            def _():
                own.wait()

            @pl.when(source != s)
            def _():
                dispatch(source, source).wait_recv()

        along_f(0, k).start()
        along_b(0, k).start()
        to_mate(z, c, k).start()
        multiply(t, k)

    def mate_part(zz, k):
        to_mate(zz, 1 - c, k).wait_recv()
        multiply(zz * 2 + 1 - c, k)

    @pl.loop(0, 16)
    def _(i):
        d, k = i // 4 + 1, i % 4
        even = (k % 2) == 0
        zf, zb = (z + 8 - d) % 8, (z + d) % 8

        @pl.when((d < 4) | even)
        def _():
            at = slice_of(zf, c, k)
            remote(at, at, af_send.at[d - 1, k], af_recv.at[d - 1, k], tp=up).wait_recv()

            @pl.when((d < 3) | ((d == 3) & even))
            def _():
                along_f(d, k).start()

            to_mate(zf, c, k).start()

        @pl.when((d < 4) | (~even))
        def _():
            at = slice_of(zb, c, k)
            remote(at, at, ab_send.at[d - 1, k], ab_recv.at[d - 1, k], tp=down).wait_recv()

            @pl.when((d < 3) | ((d == 3) & (~even)))
            def _():
                along_b(d, k).start()

        @pl.when((d < 4) | (~even))
        def _():
            to_mate(zb, c, k).start()

        @pl.when((d < 4) | even)
        def _():
            multiply(zf * 2 + c, k)

        @pl.when((d < 4) | (~even))
        def _():
            multiply(zb * 2 + c, k)

        e = i // 4

        @pl.when(e == 0)
        def _():
            mate_part(z, k)

        @pl.when(e > 0)
        def _():
            mate_part((z + 8 - e) % 8, k)
            mate_part((z + e) % 8, k)

    @pl.loop(0, 4)
    def _(k):
        mate_part((z + 4) % 8, k)

    def dots_of(tt, k):
        return dot(g2[part(k)].reshape(192, 256), wgu[tt], NT)

    def prepare(zz, k):
        value = dots_of(zz * 2 + 1 - c, k)
        q[zz, part(k)] = value.astype(BF16).reshape(4, 48, 256)
        remote(
            q.at[zz, part(k)], r.at[zz, part(k)], rp_send.at[zz, k], rp_recv.at[zz, k], tp=mate
        ).start()

    @pl.loop(0, 4)
    def _(k):
        block = acc[part(k)].reshape(192, 384)
        pre_gate, pre_up, grad_hidden = block[:, :128], block[:, 128:256], block[:, 256:]
        sig = jax.nn.sigmoid(pre_gate)
        activated = pre_gate * sig
        hid[part(k)] = (activated * pre_up).astype(BF16).reshape(4, 48, 128)
        grad_gate = (grad_hidden * pre_up * sig * (1.0 + pre_gate * (1.0 - sig))).astype(BF16)
        grad_up = (grad_hidden * activated).astype(BF16)
        g2[part(k), :, pl.ds(0, 128)] = grad_gate.reshape(4, 48, 128)
        g2[part(k), :, pl.ds(128, 128)] = grad_up.reshape(4, 48, 128)
        prepare((z + 4) % 8, k)

    def summed(zz, k):
        at = r.at[zz, part(k)]
        remote(at, at, rp_send.at[zz, k], rp_recv.at[zz, k], tp=mate).wait_recv()
        return dots_of(zz * 2 + c, k) + r[zz, part(k)].reshape(192, 256).astype(F32)

    def ring_step(d, k, zz, incoming, outgoing, send_sem, recv_sem, to, starts):
        value = summed(zz, k)

        @pl.when(starts)
        def _():
            outgoing[d - 1, part(k)] = value.astype(BF16).reshape(4, 48, 256)

        @pl.when(jnp.logical_not(starts))
        def _():
            at = incoming.at[d, part(k)]
            remote(at, at, send_sem.at[d, k], recv_sem.at[d, k], tp=to).wait_recv()
            both = value + incoming[d, part(k)].reshape(192, 256).astype(F32)
            outgoing[d - 1, part(k)] = both.astype(BF16).reshape(4, 48, 256)

        remote(
            outgoing.at[d - 1, part(k)], incoming.at[d - 1, part(k)],
            send_sem.at[d - 1, k], recv_sem.at[d - 1, k], tp=to,
        ).start()

    def grads(tt):
        x = rows[tt, :, :, pl.ds(0, 256)].reshape(768, 256)
        cot = rows[tt, :, :, pl.ds(256, 256)].reshape(768, 256)
        grad_gu[tt] = dot(x, g2[...].reshape(768, 256), TN)
        columns = pl.ds(pl.multiple_of(tt * 256, 256), 256)
        grad_d[:, columns] = dot(hid[...].reshape(768, 128), cot, TN)
        for copy in outputs(tt):
            copy.start()

    def outputs(tt):
        columns = pl.ds(pl.multiple_of(tt * 256, 256), 256)
        return [
            pltpu.make_async_copy(grad_gu.at[tt, :, pl.ds(0, 128)], gg_ref.at[tt], out_sem.at[0, tt]),
            pltpu.make_async_copy(grad_gu.at[tt, :, pl.ds(128, 128)], gu_ref.at[tt], out_sem.at[1, tt]),
            pltpu.make_async_copy(grad_d.at[:, columns], gd_ref.at[:, columns], out_sem.at[2, tt]),
        ]

    @pl.loop(0, 16)
    def _(i):
        d, k = 4 - i // 4, i % 4
        even = (k % 2) == 0
        zf, zb = (z + d) % 8, (z + 8 - d) % 8

        @pl.when((d < 4) | even)
        def _():
            ring_step(d, k, zf, in_f, out_f, rf_send, rf_recv, up, (d == 4) | ((d == 3) & (~even)))

        @pl.when((d < 4) | (~even))
        def _():
            ring_step(d, k, zb, in_b, out_b, rb_send, rb_recv, down, (d == 4) | ((d == 3) & even))

        prepare((z + d - 1) % 8, k)

        @pl.when(d > 1)
        def _():
            prepare((z + 9 - d) % 8, k)

        grads(i)

    def giving_back(peer, source):
        return remote(fin.at[peer], ret_ref.at[source], ret_send.at[peer], ret_recv.at[source], sp=peer)

    mine = pltpu.make_async_copy(fin.at[s], ret_ref.at[s], ret_recv.at[s])

    @pl.loop(0, 4)
    def _(k):
        value = summed(z, k)
        for incoming, send_sem, recv_sem, to in ((in_f, rf_send, rf_recv, up), (in_b, rb_send, rb_recv, down)):
            at = incoming.at[0, part(k)]
            remote(at, at, send_sem.at[0, k], recv_sem.at[0, k], tp=to).wait_recv()
            value = value + incoming[0, part(k)].reshape(192, 256).astype(F32)
        fin[part(k)] = value.astype(BF16).reshape(4, 48, 256)
        for x in range(4):
            peer = 4 * ((y + 4 - k) % 4) + x

            @pl.when(peer == s)
            def _():
                mine.start()

            @pl.when(peer != s)
            def _():
                giving_back(peer, s).start()

    @pl.loop(1, 16)
    def _(i):
        giving_back((s + i) % 16, (s + i) % 16).wait_recv()

    mine.wait()

    @pl.loop(1, 16)
    def _(i):
        dispatch((s + i) % 16, s).wait_send()
        giving_back((s + i) % 16, s).wait_send()

    @pl.loop(0, 16)
    def _(i):
        d, k = i // 4, i % 4
        even = (k % 2) == 0

        @pl.when((d < 3) | even)
        def _():
            along_f(d, k).wait_send()
            at = out_f.at[d, part(k)]
            remote(at, at, rf_send.at[d, k], rf_recv.at[d, k], tp=up).wait_send()

        @pl.when((d < 3) | (~even))
        def _():
            along_b(d, k).wait_send()
            at = out_b.at[d, part(k)]
            remote(at, at, rb_send.at[d, k], rb_recv.at[d, k], tp=down).wait_send()

        for half in range(2):
            zz = d * 2 + half
            to_mate(zz, c, k).wait_send()
            at = q.at[zz, part(k)]
            remote(at, at, rp_send.at[zz, k], rp_recv.at[zz, k], tp=mate).wait_send()
        for copy in outputs(i):
            copy.wait()


def moe(send, wg, wu, wd):
    vm = lambda shape, dtype: pltpu.VMEM(shape, dtype)
    dma = lambda *shape: pltpu.SemaphoreType.DMA(shape)
    any_ = pl.BlockSpec(memory_space=pl.ANY)
    vmem = pl.BlockSpec(memory_space=pltpu.VMEM)
    return pl.pallas_call(
        moe_kernel,
        out_shape=(
            jax.ShapeDtypeStruct((16, 48, 256), BF16),
            jax.ShapeDtypeStruct((16, 256, 128), F32),
            jax.ShapeDtypeStruct((16, 256, 128), F32),
            jax.ShapeDtypeStruct((128, 4096), F32),
        ),
        in_specs=[vmem, any_, any_, any_],
        out_specs=(vmem, any_, any_, any_),
        scratch_shapes=[
            vm((16, 16, 48, 512), BF16),
            vm((16, 256, 256), BF16),
            vm((128, 4096), BF16),
            vm((16, 48, 384), F32),
            vm((16, 48, 256), BF16),
            vm((16, 48, 128), BF16),
            vm((8, 16, 48, 256), BF16),
            vm((8, 16, 48, 256), BF16),
            vm((4, 16, 48, 256), BF16),
            vm((4, 16, 48, 256), BF16),
            vm((4, 16, 48, 256), BF16),
            vm((4, 16, 48, 256), BF16),
            vm((16, 48, 256), BF16),
            vm((16, 256, 256), F32),
            vm((128, 4096), F32),
            dma(3), dma(16), dma(16),
            dma(4, 4), dma(4, 4), dma(4, 4), dma(4, 4), dma(8, 4), dma(8, 4),
            dma(8, 4), dma(8, 4), dma(4, 4), dma(4, 4), dma(4, 4), dma(4, 4),
            dma(16), dma(16), dma(3, 16),
        ],
        compiler_params=pltpu.CompilerParams(
            collective_id=1, has_side_effects=True, vmem_limit_bytes=60 * 1024 * 1024
        ),
        cost_estimate=pl.CostEstimate(flops=8_000_000_000, bytes_accessed=20_000_000, transcendentals=100_000),
        name="moe",
    )(send, wg, wu, wd)


def padded(array):
    size = 16
    up = [(i, i + 1) for i in range(size - 1)]
    before = lax.ppermute(array[-1:], "sp", up)
    after = lax.ppermute(array[:1], "sp", [(j, i) for i, j in up])
    return jnp.concatenate([before, array, after], axis=0)


def body(moe_input, out_gate, in_gate, values, conv_taps, out_proj, route_ids, route_gates, expert_gate, expert_up, expert_down, cotangent):
    experts = jnp.arange(16, dtype=jnp.int32)
    chosen = route_ids[:, :, None] == experts[None, None, :]
    member = jnp.sum(chosen.astype(F32), axis=1)
    weight = jnp.sum(jnp.where(chosen, route_gates[:, :, None], 0.0), axis=1)
    tokens = jnp.arange(256, dtype=jnp.int32)
    earlier = (tokens[:, None] > tokens[None, :]).astype(BF16)
    place = jnp.dot(earlier, member.astype(BF16), preferred_element_type=F32)
    place = jnp.where(member > 0, place, -1.0)
    pick = place.T[:, None, :] == jnp.arange(48, dtype=F32)[None, :, None]
    slot_weight = jnp.sum(jnp.where(pick, weight.T[:, None, :], 0.0), axis=2)
    pick = pick.astype(BF16).reshape(768, 256)
    both = jnp.dot(pick, jnp.concatenate([moe_input, cotangent], axis=1), preferred_element_type=F32)
    scale = slot_weight.reshape(768, 1)
    send = jnp.concatenate([both[:, :256], both[:, 256:] * scale], axis=1).astype(BF16).reshape(16, 48, 512)

    ret, gg, gu, gd = moe(
        send,
        expert_gate.reshape(16, 256, 128),
        expert_up.reshape(16, 256, 128),
        expert_down.reshape(128, 4096),
    )
    grad_expert_gate = gg.reshape(1, 4096, 128)
    grad_expert_up = gu.reshape(1, 4096, 128)
    grad_expert_down = gd.reshape(1, 128, 4096)
    moe_grad = lax.dot_general(pick, ret.reshape(768, 256), TN, preferred_element_type=F32)
    mixer_cot = (cotangent.astype(F32) + moe_grad).astype(BF16)

    conv_in = in_gate.astype(F32) * values.astype(F32)
    rimmed = padded(conv_in)
    conv_out = rimmed[:-2] * conv_taps[0] + rimmed[1:-1] * conv_taps[1] + rimmed[2:] * conv_taps[2]
    mixed = (out_gate.astype(F32) * conv_out).astype(BF16)
    all_mixed = lax.all_gather(mixed, "sp", axis=0, tiled=True)
    full_mixer_cot = lax.all_gather(mixer_cot, "tp", axis=1, tiled=True)
    grad_mixed = jnp.dot(full_mixer_cot, out_proj, preferred_element_type=F32)
    grad_out_gate = (grad_mixed * conv_out).astype(BF16)
    grad_conv_out = grad_mixed * out_gate.astype(F32)
    rim_grad = padded(grad_conv_out)
    grad_conv_in = rim_grad[2:] * conv_taps[0] + rim_grad[1:-1] * conv_taps[1] + rim_grad[:-2] * conv_taps[2]
    grad_in_gate = (grad_conv_in * values.astype(F32)).astype(BF16)
    grad_values = (grad_conv_in * in_gate.astype(F32)).astype(BF16)
    columns = lax.all_to_all(full_mixer_cot, "sp", split_axis=1, concat_axis=0, tiled=True)
    grad_out_proj = lax.dot_general(columns, all_mixed, TN, preferred_element_type=F32)
    return (grad_out_gate, grad_in_gate, grad_values, grad_out_proj, grad_expert_gate, grad_expert_up, grad_expert_down)


def solution(mesh):
    in_specs = (
        P("sp", "tp"), P("sp", "tp"), P("sp", "tp"), P("sp", "tp"), P(None, "tp"), P(None, "tp"),
        P("sp", None), P("sp", None),
        P("sp", None, "tp"), P("sp", None, "tp"), P("sp", "tp", None), P("sp", "tp"),
    )
    out_specs = (
        P("sp", "tp"), P("sp", "tp"), P("sp", "tp"), P("sp", "tp"),
        P("sp", None, "tp"), P("sp", None, "tp"), P("sp", "tp", None),
    )
    return jax.shard_map(body, mesh=mesh, in_specs=in_specs, out_specs=out_specs, check_vma=False)
```

```python
import functools
import jax
import jax.numpy as jnp
from jax import lax
from jax.experimental import pallas as pl
from jax.experimental.pallas import tpu as pltpu
from jax.sharding import PartitionSpec as P

F32 = jnp.float32
BF16 = jnp.bfloat16
MESH = pl.DeviceIdType.MESH
NT = (((1,), (1,)), ((), ()))
TN = (((0,), (0,)), ((), ()))


def dot(a, b, dims):
    return lax.dot_general(a, b, dims, preferred_element_type=F32)


def moe_kernel(
    send_ref, pick_ref, cot_ref, og_ref, ig_ref, val_ref, taps_ref, wg_ref, wu_ref, wd_ref, op_ref,
    gog_ref, gig_ref, gval_ref, gop_ref, gg_ref, gu_ref, gd_ref,
    rows, wgu, wd, acc, g2, hid, q, r, in_f, in_b, out_f, out_b, fin, grad_gu, grad_d,
    ret_ref, op, cin, cout, halo, mix, mcf, col, acc2,
    w_sem, disp_send, disp_recv,
    af_send, af_recv, ab_send, ab_recv, ap_send, ap_recv,
    rp_send, rp_recv, rf_send, rf_recv, rb_send, rb_recv,
    ret_send, ret_recv, out_sem,
    halo_send, halo_recv, mix_send, mix_recv,
    mf_send, mf_recv, mb_send, mb_recv, mp_send, mp_recv,
    col_send, col_recv, colp_send, colp_recv,
):
    s = lax.axis_index("sp")
    t = lax.axis_index("tp")
    z, c = t // 2, t % 2
    y = s // 4
    up, down, mate = ((z + 1) % 8) * 2 + c, ((z + 7) % 8) * 2 + c, z * 2 + (1 - c)

    weights = [
        pltpu.make_async_copy(wg_ref, wgu.at[:, :, pl.ds(0, 128)], w_sem.at[0]),
        pltpu.make_async_copy(wu_ref, wgu.at[:, :, pl.ds(128, 128)], w_sem.at[1]),
        pltpu.make_async_copy(wd_ref, wd, w_sem.at[2]),
        pltpu.make_async_copy(op_ref, op, w_sem.at[3]),
    ]
    for w in weights:
        w.start()

    cin[...] = ig_ref[...].astype(F32) * val_ref[...].astype(F32)

    barrier = pltpu.get_barrier_semaphore()

    @pl.loop(1, 16)
    def _(i):
        pl.semaphore_signal(barrier, inc=1, device_id={"sp": (s + i) % 16}, device_id_type=MESH)

    for other in (up, down, mate):
        pl.semaphore_signal(barrier, inc=1, device_id={"tp": other}, device_id_type=MESH)
    pl.semaphore_wait(barrier, 18)

    def remote(src, dst, send_sem, recv_sem, **where):
        return pltpu.make_async_remote_copy(
            src_ref=src, dst_ref=dst, send_sem=send_sem, recv_sem=recv_sem,
            device_id=where, device_id_type=MESH,
        )

    def dispatch(peer, source):
        return remote(
            send_ref.at[peer], rows.at[t, source], disp_send.at[peer], disp_recv.at[source], sp=peer
        )

    own = pltpu.make_async_copy(send_ref.at[s], rows.at[t, s], disp_recv.at[s])
    own.start()

    def halo_copies(h):
        return [
            remote(cin.at[pl.ds(248, 8)], halo.at[h, 0], halo_send.at[h, 0], halo_recv.at[h, 0], sp=(s + 1) % 16),
            remote(cin.at[pl.ds(0, 8)], halo.at[h, 1], halo_send.at[h, 1], halo_recv.at[h, 1], sp=(s + 15) % 16),
        ]

    row = lax.broadcasted_iota(jnp.int32, (256, 256), 0)

    def neighbours(h):
        for copy in halo_copies(h):
            copy.wait()
        array = cin[...]
        first = jnp.where(s > 0, halo[h, 0, 7:8, :], 0.0)
        last = jnp.where(s < 15, halo[h, 1, 0:1, :], 0.0)
        before = jnp.where(row == 0, first, pltpu.roll(array, 1, 0))
        after = jnp.where(row == 255, last, pltpu.roll(array, 255, 0))
        return before, array, after

    for copy in halo_copies(0):
        copy.start()

    @pl.loop(1, 16)
    def _(i):
        dispatch((s + i) % 16, s).start()

    before, here, after = neighbours(0)
    conv = before * taps_ref[0:1, :] + here * taps_ref[1:2, :] + after * taps_ref[2:3, :]
    cout[...] = conv
    mix[s] = (og_ref[...].astype(F32) * conv).astype(BF16)

    def mix_copy(peer, source):
        return remote(mix.at[source], mix.at[source], mix_send.at[peer], mix_recv.at[source], sp=peer)

    acc[...] = jnp.zeros_like(acc)
    for w in weights:
        w.wait()

    def part(k):
        return pl.ds(4 * ((y + 4 - k) % 4), 4)

    def slice_of(zz, core, k):
        return rows.at[zz * 2 + core, part(k)]

    def along_f(d, k):
        at = slice_of((z + 8 - d) % 8, c, k)
        return remote(at, at, af_send.at[d, k], af_recv.at[d, k], tp=up)

    def along_b(d, k):
        at = slice_of((z + d) % 8, c, k)
        return remote(at, at, ab_send.at[d, k], ab_recv.at[d, k], tp=down)

    def to_mate(zz, core, k):
        at = slice_of(zz, core, k)
        return remote(at, at, ap_send.at[zz, k], ap_recv.at[zz, k], tp=mate)

    def multiply(tt, k):
        block = rows[tt, part(k)].reshape(192, 512)
        pre = dot(block[:, :256], wgu[tt], (((1,), (0,)), ((), ())))
        columns = pl.ds(pl.multiple_of(tt * 256, 256), 256)
        hidden = dot(block[:, 256:], wd[:, columns], NT)
        acc[part(k), :, pl.ds(0, 256)] += pre.reshape(4, 48, 256)
        acc[part(k), :, pl.ds(256, 128)] += hidden.reshape(4, 48, 128)

    @pl.loop(0, 4)
    def _(k):
        for x in range(4):
            source = 4 * ((y + 4 - k) % 4) + x

            @pl.when(source == s)
            def _():
                own.wait()

            @pl.when(source != s)
            def _():
                dispatch(source, source).wait_recv()

        along_f(0, k).start()
        along_b(0, k).start()
        to_mate(z, c, k).start()
        multiply(t, k)

    @pl.loop(1, 16)
    def _(i):
        mix_copy((s + i) % 16, s).start()

    def mate_part(zz, k):
        to_mate(zz, 1 - c, k).wait_recv()
        multiply(zz * 2 + 1 - c, k)

    @pl.loop(0, 16)
    def _(i):
        d, k = i // 4 + 1, i % 4
        even = (k % 2) == 0
        zf, zb = (z + 8 - d) % 8, (z + d) % 8

        @pl.when((d < 4) | even)
        def _():
            at = slice_of(zf, c, k)
            remote(at, at, af_send.at[d - 1, k], af_recv.at[d - 1, k], tp=up).wait_recv()

            @pl.when((d < 3) | ((d == 3) & even))
            def _():
                along_f(d, k).start()

            to_mate(zf, c, k).start()

        @pl.when((d < 4) | (~even))
        def _():
            at = slice_of(zb, c, k)
            remote(at, at, ab_send.at[d - 1, k], ab_recv.at[d - 1, k], tp=down).wait_recv()

            @pl.when((d < 3) | ((d == 3) & (~even)))
            def _():
                along_b(d, k).start()

        @pl.when((d < 4) | (~even))
        def _():
            to_mate(zb, c, k).start()

        @pl.when((d < 4) | even)
        def _():
            multiply(zf * 2 + c, k)

        @pl.when((d < 4) | (~even))
        def _():
            multiply(zb * 2 + c, k)

        e = i // 4

        @pl.when(e == 0)
        def _():
            mate_part(z, k)

        @pl.when(e > 0)
        def _():
            mate_part((z + 8 - e) % 8, k)
            mate_part((z + e) % 8, k)

    @pl.loop(0, 4)
    def _(k):
        mate_part((z + 4) % 8, k)

    def dots_of(tt, k):
        return dot(g2[part(k)].reshape(192, 256), wgu[tt], NT)

    def prepare(zz, k):
        value = dots_of(zz * 2 + 1 - c, k)
        q[zz, part(k)] = value.astype(BF16).reshape(4, 48, 256)
        remote(
            q.at[zz, part(k)], r.at[zz, part(k)], rp_send.at[zz, k], rp_recv.at[zz, k], tp=mate
        ).start()

    @pl.loop(0, 4)
    def _(k):
        block = acc[part(k)].reshape(192, 384)
        pre_gate, pre_up, grad_hidden = block[:, :128], block[:, 128:256], block[:, 256:]
        sig = jax.nn.sigmoid(pre_gate)
        activated = pre_gate * sig
        hid[part(k)] = (activated * pre_up).astype(BF16).reshape(4, 48, 128)
        grad_gate = (grad_hidden * pre_up * sig * (1.0 + pre_gate * (1.0 - sig))).astype(BF16)
        grad_up = (grad_hidden * activated).astype(BF16)
        g2[part(k), :, pl.ds(0, 128)] = grad_gate.reshape(4, 48, 128)
        g2[part(k), :, pl.ds(128, 128)] = grad_up.reshape(4, 48, 128)
        prepare((z + 4) % 8, k)

    def summed(zz, k):
        at = r.at[zz, part(k)]
        remote(at, at, rp_send.at[zz, k], rp_recv.at[zz, k], tp=mate).wait_recv()
        return dots_of(zz * 2 + c, k) + r[zz, part(k)].reshape(192, 256).astype(F32)

    def ring_step(d, k, zz, incoming, outgoing, send_sem, recv_sem, to, starts):
        value = summed(zz, k)

        @pl.when(starts)
        def _():
            outgoing[d - 1, part(k)] = value.astype(BF16).reshape(4, 48, 256)

        @pl.when(jnp.logical_not(starts))
        def _():
            at = incoming.at[d, part(k)]
            remote(at, at, send_sem.at[d, k], recv_sem.at[d, k], tp=to).wait_recv()
            both = value + incoming[d, part(k)].reshape(192, 256).astype(F32)
            outgoing[d - 1, part(k)] = both.astype(BF16).reshape(4, 48, 256)

        remote(
            outgoing.at[d - 1, part(k)], incoming.at[d - 1, part(k)],
            send_sem.at[d - 1, k], recv_sem.at[d - 1, k], tp=to,
        ).start()

    def grads(tt):
        x = rows[tt, :, :, pl.ds(0, 256)].reshape(768, 256)
        cot = rows[tt, :, :, pl.ds(256, 256)].reshape(768, 256)
        grad_gu[tt] = dot(x, g2[...].reshape(768, 256), TN)
        columns = pl.ds(pl.multiple_of(tt * 256, 256), 256)
        grad_d[:, columns] = dot(hid[...].reshape(768, 128), cot, TN)
        for copy in outputs(tt):
            copy.start()

    def outputs(tt):
        columns = pl.ds(pl.multiple_of(tt * 256, 256), 256)
        return [
            pltpu.make_async_copy(grad_gu.at[tt, :, pl.ds(0, 128)], gg_ref.at[tt], out_sem.at[0, tt]),
            pltpu.make_async_copy(grad_gu.at[tt, :, pl.ds(128, 128)], gu_ref.at[tt], out_sem.at[1, tt]),
            pltpu.make_async_copy(grad_d.at[:, columns], gd_ref.at[:, columns], out_sem.at[2, tt]),
        ]

    @pl.loop(0, 16)
    def _(i):
        d, k = 4 - i // 4, i % 4
        even = (k % 2) == 0
        zf, zb = (z + d) % 8, (z + 8 - d) % 8

        @pl.when((d < 4) | even)
        def _():
            ring_step(d, k, zf, in_f, out_f, rf_send, rf_recv, up, (d == 4) | ((d == 3) & (~even)))

        @pl.when((d < 4) | (~even))
        def _():
            ring_step(d, k, zb, in_b, out_b, rb_send, rb_recv, down, (d == 4) | ((d == 3) & even))

        prepare((z + d - 1) % 8, k)

        @pl.when(d > 1)
        def _():
            prepare((z + 9 - d) % 8, k)

        grads(i)

    def giving_back(peer, source):
        return remote(fin.at[peer], ret_ref.at[source], ret_send.at[peer], ret_recv.at[source], sp=peer)

    mine = pltpu.make_async_copy(fin.at[s], ret_ref.at[s], ret_recv.at[s])

    @pl.loop(0, 4)
    def _(k):
        value = summed(z, k)
        for incoming, send_sem, recv_sem, to in ((in_f, rf_send, rf_recv, up), (in_b, rb_send, rb_recv, down)):
            at = incoming.at[0, part(k)]
            remote(at, at, send_sem.at[0, k], recv_sem.at[0, k], tp=to).wait_recv()
            value = value + incoming[0, part(k)].reshape(192, 256).astype(F32)
        fin[part(k)] = value.astype(BF16).reshape(4, 48, 256)
        for x in range(4):
            peer = 4 * ((y + 4 - k) % 4) + x

            @pl.when(peer == s)
            def _():
                mine.start()

            @pl.when(peer != s)
            def _():
                giving_back(peer, s).start()

    @pl.loop(1, 16)
    def _(i):
        giving_back((s + i) % 16, (s + i) % 16).wait_recv()

    mine.wait()

    moe_grad = dot(pick_ref[...], ret_ref[...].reshape(768, 256), TN)
    mixer = (cot_ref[...].astype(F32) + moe_grad).astype(BF16)
    mcf[t] = mixer.reshape(2, 128, 256)
    acc2[...] = jnp.zeros_like(acc2)

    def mc_f(d, k):
        at = mcf.at[((z + 8 - d) % 8) * 2 + c, k]
        return remote(at, at, mf_send.at[d, k], mf_recv.at[d, k], tp=up)

    def mc_b(d, k):
        at = mcf.at[((z + d) % 8) * 2 + c, k]
        return remote(at, at, mb_send.at[d, k], mb_recv.at[d, k], tp=down)

    def mc_mate(zz, core, k):
        at = mcf.at[zz * 2 + core, k]
        return remote(at, at, mp_send.at[zz, k], mp_recv.at[zz, k], tp=mate)

    def column(peer, source):
        return remote(mcf.at[peer, c], col.at[source, c], col_send.at[peer], col_recv.at[source], sp=peer)

    def column_mate(source, core):
        at = col.at[source, core]
        return remote(at, at, colp_send.at[source], colp_recv.at[source], tp=mate)

    kept = pltpu.make_async_copy(mcf.at[s, c], col.at[s, c], col_recv.at[s])

    def use(tt, k):
        @pl.when((k == c) & (tt == s))
        def _():
            kept.start()

        @pl.when((k == c) & (tt != s))
        def _():
            column(tt, s).start()

        acc2[k] += dot(mcf[tt, k], op[tt], (((1,), (0,)), ((), ())))

    for k in range(2):
        mc_f(0, k).start()
        mc_b(0, k).start()
        mc_mate(z, c, k).start()
    for k in range(2):
        use(t, k)

    def mc_mate_part(zz, k):
        mc_mate(zz, 1 - c, k).wait_recv()
        use(zz * 2 + 1 - c, k)

    @pl.loop(0, 8)
    def _(i):
        d, k = i // 2 + 1, i % 2
        zf, zb = (z + 8 - d) % 8, (z + d) % 8
        goes_f = (d < 4) | (k == 0)
        goes_b = (d < 4) | (k == 1)

        @pl.when(goes_f)
        def _():
            at = mcf.at[zf * 2 + c, k]
            remote(at, at, mf_send.at[d - 1, k], mf_recv.at[d - 1, k], tp=up).wait_recv()

            @pl.when((d < 3) | ((d == 3) & (k == 0)))
            def _():
                mc_f(d, k).start()

            mc_mate(zf, c, k).start()

        @pl.when(goes_b)
        def _():
            at = mcf.at[zb * 2 + c, k]
            remote(at, at, mb_send.at[d - 1, k], mb_recv.at[d - 1, k], tp=down).wait_recv()

            @pl.when((d < 3) | ((d == 3) & (k == 1)))
            def _():
                mc_b(d, k).start()

        @pl.when(goes_b)
        def _():
            mc_mate(zb, c, k).start()

        @pl.when(goes_f)
        def _():
            use(zf * 2 + c, k)

        @pl.when(goes_b)
        def _():
            use(zb * 2 + c, k)

        e = i // 2

        @pl.when(e == 0)
        def _():
            mc_mate_part(z, k)

        @pl.when(e > 0)
        def _():
            mc_mate_part((z + 8 - e) % 8, k)
            mc_mate_part((z + e) % 8, k)

    @pl.loop(0, 2)
    def _(k):
        mc_mate_part((z + 4) % 8, k)

    grad_mixed = acc2[...].reshape(256, 256)
    gog_ref[...] = (grad_mixed * cout[...]).astype(BF16)
    cin[...] = grad_mixed * og_ref[...].astype(F32)
    for copy in halo_copies(1):
        copy.start()

    kept.wait()
    column_mate(s, c).start()

    @pl.loop(1, 16)
    def _(i):
        source = (s + i) % 16
        column(source, source).wait_recv()
        column_mate(source, c).start()

    gop_ref[...] = jnp.zeros_like(gop_ref)

    @pl.loop(0, 16)
    def _(i):
        source = (s + i) % 16

        @pl.when(i > 0)
        def _():
            mix_copy(source, source).wait_recv()

        column_mate(source, 1 - c).wait_recv()
        gop_ref[...] += dot(col[source].reshape(256, 256), mix[source], TN)

    before, here, after = neighbours(1)
    grad_in = after * taps_ref[0:1, :] + here * taps_ref[1:2, :] + before * taps_ref[2:3, :]
    gig_ref[...] = (grad_in * val_ref[...].astype(F32)).astype(BF16)
    gval_ref[...] = (grad_in * ig_ref[...].astype(F32)).astype(BF16)

    @pl.loop(1, 16)
    def _(i):
        dispatch((s + i) % 16, s).wait_send()
        giving_back((s + i) % 16, s).wait_send()
        mix_copy((s + i) % 16, s).wait_send()
        column((s + i) % 16, s).wait_send()

    @pl.loop(0, 16)
    def _(i):
        column_mate(i, c).wait_send()
        mc_mate(i // 2, c, i % 2).wait_send()

    @pl.loop(0, 8)
    def _(i):
        d, k = i // 2, i % 2

        @pl.when((d < 3) | (k == 0))
        def _():
            mc_f(d, k).wait_send()

        @pl.when((d < 3) | (k == 1))
        def _():
            mc_b(d, k).wait_send()

    @pl.loop(0, 16)
    def _(i):
        d, k = i // 4, i % 4
        even = (k % 2) == 0

        @pl.when((d < 3) | even)
        def _():
            along_f(d, k).wait_send()
            at = out_f.at[d, part(k)]
            remote(at, at, rf_send.at[d, k], rf_recv.at[d, k], tp=up).wait_send()

        @pl.when((d < 3) | (~even))
        def _():
            along_b(d, k).wait_send()
            at = out_b.at[d, part(k)]
            remote(at, at, rb_send.at[d, k], rb_recv.at[d, k], tp=down).wait_send()

        for half in range(2):
            zz = d * 2 + half
            to_mate(zz, c, k).wait_send()
            at = q.at[zz, part(k)]
            remote(at, at, rp_send.at[zz, k], rp_recv.at[zz, k], tp=mate).wait_send()
        for copy in outputs(i):
            copy.wait()


def mixer_and_experts(*operands):
    vm = lambda shape, dtype: pltpu.VMEM(shape, dtype)
    dma = lambda *shape: pltpu.SemaphoreType.DMA(shape)
    any_ = pl.BlockSpec(memory_space=pl.ANY)
    vmem = pl.BlockSpec(memory_space=pltpu.VMEM)
    tile = jax.ShapeDtypeStruct((256, 256), BF16)
    return pl.pallas_call(
        moe_kernel,
        out_shape=(
            tile, tile, tile,
            jax.ShapeDtypeStruct((256, 256), F32),
            jax.ShapeDtypeStruct((16, 256, 128), F32),
            jax.ShapeDtypeStruct((16, 256, 128), F32),
            jax.ShapeDtypeStruct((128, 4096), F32),
        ),
        in_specs=[vmem] * 7 + [any_] * 4,
        out_specs=(vmem,) * 4 + (any_,) * 3,
        scratch_shapes=[
            vm((16, 16, 48, 512), BF16),
            vm((16, 256, 256), BF16),
            vm((128, 4096), BF16),
            vm((16, 48, 384), F32),
            vm((16, 48, 256), BF16),
            vm((16, 48, 128), BF16),
            vm((8, 16, 48, 256), BF16),
            vm((8, 16, 48, 256), BF16),
            vm((4, 16, 48, 256), BF16),
            vm((4, 16, 48, 256), BF16),
            vm((4, 16, 48, 256), BF16),
            vm((4, 16, 48, 256), BF16),
            vm((16, 48, 256), BF16),
            vm((16, 256, 256), F32),
            vm((128, 4096), F32),
            vm((16, 48, 256), BF16),
            vm((16, 256, 256), BF16),
            vm((256, 256), F32),
            vm((256, 256), F32),
            vm((2, 2, 8, 256), F32),
            vm((16, 256, 256), BF16),
            vm((16, 2, 128, 256), BF16),
            vm((16, 2, 128, 256), BF16),
            vm((2, 128, 256), F32),
            dma(4), dma(16), dma(16),
            dma(4, 4), dma(4, 4), dma(4, 4), dma(4, 4), dma(8, 4), dma(8, 4),
            dma(8, 4), dma(8, 4), dma(4, 4), dma(4, 4), dma(4, 4), dma(4, 4),
            dma(16), dma(16), dma(3, 16),
            dma(2, 2), dma(2, 2), dma(16), dma(16),
            dma(4, 2), dma(4, 2), dma(4, 2), dma(4, 2), dma(8, 2), dma(8, 2),
            dma(16), dma(16), dma(16), dma(16),
        ],
        compiler_params=pltpu.CompilerParams(
            collective_id=1, has_side_effects=True, vmem_limit_bytes=60 * 1024 * 1024
        ),
        cost_estimate=pl.CostEstimate(flops=8_000_000_000, bytes_accessed=20_000_000, transcendentals=100_000),
        name="mixer_and_experts",
    )(*operands)


def body(moe_input, out_gate, in_gate, values, conv_taps, out_proj, route_ids, route_gates, expert_gate, expert_up, expert_down, cotangent):
    experts = jnp.arange(16, dtype=jnp.int32)
    chosen = route_ids[:, :, None] == experts[None, None, :]
    member = jnp.sum(chosen.astype(F32), axis=1)
    weight = jnp.sum(jnp.where(chosen, route_gates[:, :, None], 0.0), axis=1)
    tokens = jnp.arange(256, dtype=jnp.int32)
    earlier = (tokens[:, None] > tokens[None, :]).astype(BF16)
    place = jnp.dot(earlier, member.astype(BF16), preferred_element_type=F32)
    place = jnp.where(member > 0, place, -1.0)
    pick = place.T[:, None, :] == jnp.arange(48, dtype=F32)[None, :, None]
    slot_weight = jnp.sum(jnp.where(pick, weight.T[:, None, :], 0.0), axis=2)
    pick = pick.astype(BF16).reshape(768, 256)
    both = jnp.dot(pick, jnp.concatenate([moe_input, cotangent], axis=1), preferred_element_type=F32)
    scale = slot_weight.reshape(768, 1)
    send = jnp.concatenate([both[:, :256], both[:, 256:] * scale], axis=1).astype(BF16).reshape(16, 48, 512)

    gog, gig, gval, gop, gg, gu, gd = mixer_and_experts(
        send, pick, cotangent, out_gate, in_gate, values, conv_taps,
        expert_gate.reshape(16, 256, 128),
        expert_up.reshape(16, 256, 128),
        expert_down.reshape(128, 4096),
        out_proj.reshape(16, 256, 256),
    )
    return (gog, gig, gval, gop, gg.reshape(1, 4096, 128), gu.reshape(1, 4096, 128), gd.reshape(1, 128, 4096))


def solution(mesh):
    in_specs = (
        P("sp", "tp"), P("sp", "tp"), P("sp", "tp"), P("sp", "tp"), P(None, "tp"), P(None, "tp"),
        P("sp", None), P("sp", None),
        P("sp", None, "tp"), P("sp", None, "tp"), P("sp", "tp", None), P("sp", "tp"),
    )
    out_specs = (
        P("sp", "tp"), P("sp", "tp"), P("sp", "tp"), P("sp", "tp"),
        P("sp", None, "tp"), P("sp", None, "tp"), P("sp", "tp", None),
    )
    return jax.shard_map(body, mesh=mesh, in_specs=in_specs, out_specs=out_specs, check_vma=False)
```

```python
import functools
import jax
import jax.numpy as jnp
from jax import lax
from jax.experimental import pallas as pl
from jax.experimental.pallas import tpu as pltpu
from jax.sharding import PartitionSpec as P

F32 = jnp.float32
BF16 = jnp.bfloat16
MESH = pl.DeviceIdType.MESH
NT = (((1,), (1,)), ((), ()))
TN = (((0,), (0,)), ((), ()))
NN = (((1,), (0,)), ((), ()))


def dot(a, b, dims):
    return lax.dot_general(a, b, dims, preferred_element_type=F32)


def moe_kernel(
    ids_ref, gates_ref, x_ref, cot_ref, og_ref, ig_ref, val_ref, taps_ref, wg_ref, wu_ref, wd_ref, op_ref,
    gog_ref, gig_ref, gval_ref, gop_ref, gg_ref, gu_ref, gd_ref,
    pick_ref, scale, tokens, x_send, cot_send, rows, cots, wgu, wd, acc, acc_h, g2, hid, q, r, in_f, in_b, out_f, out_b, fin, grad_gu, grad_d,
    ret_ref, op, cin, cout, halo, mix, mcf, col, acc2,
    w_sem, disp_send, disp_recv,
    af_send, af_recv, ab_send, ab_recv, ap_send, ap_recv,
    rp_send, rp_recv, rf_send, rf_recv, rb_send, rb_recv,
    ret_send, ret_recv, out_sem,
    halo_send, halo_recv, mix_send, mix_recv,
    mf_send, mf_recv, mb_send, mb_recv, mp_send, mp_recv,
    col_send, col_recv, colp_send, colp_recv,
    tf_send, tf_recv, tb_send, tb_recv, cot_sent, cot_recv, cp_send, cp_recv,
):
    s = lax.axis_index("sp")
    t = lax.axis_index("tp")
    z, c = t // 2, t % 2
    y = s // 4
    up, down, mate = ((z + 1) % 8) * 2 + c, ((z + 7) % 8) * 2 + c, z * 2 + (1 - c)

    barrier = pltpu.get_barrier_semaphore()

    @pl.loop(1, 16)
    def _(i):
        pl.semaphore_signal(barrier, inc=1, device_id={"sp": (s + i) % 16}, device_id_type=MESH)

    for other in (up, down, mate):
        pl.semaphore_signal(barrier, inc=1, device_id={"tp": other}, device_id_type=MESH)

    weights = [
        pltpu.make_async_copy(wg_ref, wgu.at[:, :, pl.ds(0, 128)], w_sem.at[0]),
        pltpu.make_async_copy(wu_ref, wgu.at[:, :, pl.ds(128, 128)], w_sem.at[1]),
        pltpu.make_async_copy(wd_ref, wd, w_sem.at[2]),
        pltpu.make_async_copy(op_ref, op, w_sem.at[3]),
    ]
    for w in weights:
        w.start()

    cin[...] = ig_ref[...].astype(F32) * val_ref[...].astype(F32)

    expert = lax.broadcasted_iota(jnp.int32, (16, 256), 0)
    named = [ids_ref[i : i + 1, :] == expert for i in range(2)]
    member = jnp.where(named[0] | named[1], 1.0, 0.0)
    weight = jnp.where(named[0], gates_ref[0:1, :], 0.0) + jnp.where(named[1], gates_ref[1:2, :], 0.0)
    row = lax.broadcasted_iota(jnp.int32, (256, 256), 0)
    earlier = jnp.where(row < lax.broadcasted_iota(jnp.int32, (256, 256), 1), 1.0, 0.0).astype(BF16)
    place = jnp.where(member > 0, dot(member.astype(BF16), earlier, NN), -1.0)
    position = lax.broadcasted_iota(jnp.int32, (48, 256), 0).astype(F32)
    for e in range(16):
        hit = place[e : e + 1, :] == position
        pick_ref[e] = jnp.where(hit, 1.0, 0.0).astype(BF16)
        slot_weight = jnp.sum(jnp.where(hit, weight[e : e + 1, :], 0.0), axis=1, keepdims=True)
        scale[e] = jnp.broadcast_to(slot_weight, (48, 128))
    tokens[z] = cot_ref[...].reshape(2, 128, 256)
    acc[...] = jnp.zeros_like(acc)
    acc_h[...] = jnp.zeros_like(acc_h)

    pl.semaphore_wait(barrier, 18)

    def remote(src, dst, send_sem, recv_sem, **where):
        return pltpu.make_async_remote_copy(
            src_ref=src, dst_ref=dst, send_sem=send_sem, recv_sem=recv_sem,
            device_id=where, device_id_type=MESH,
        )

    def part(k):
        return pl.ds(4 * ((y + 4 - k) % 4), 4)

    def token_f(d, k):
        at = tokens.at[(z + 8 - d) % 8, k]
        return remote(at, at, tf_send.at[d, k], tf_recv.at[d, k], tp=up)

    def token_b(d, k):
        at = tokens.at[(z + d) % 8, k]
        return remote(at, at, tb_send.at[d, k], tb_recv.at[d, k], tp=down)

    for k in range(2):
        from_cot = cot_ref.at[pl.ds(128 * k, 128)]
        remote(from_cot, tokens.at[z, k], tf_send.at[0, k], tf_recv.at[0, k], tp=up).start()
        remote(from_cot, tokens.at[z, k], tb_send.at[0, k], tb_recv.at[0, k], tp=down).start()

    def dispatch(peer, source):
        return remote(
            x_send.at[peer], rows.at[t, source], disp_send.at[peer], disp_recv.at[source], sp=peer
        )

    own = pltpu.make_async_copy(x_send.at[s], rows.at[t, s], disp_recv.at[s])

    def dispatch_cot(zz, peer, source):
        return remote(
            cot_send.at[zz, peer], cots.at[zz * 2 + c, source],
            cot_sent.at[zz, peer], cot_recv.at[zz, source], sp=peer,
        )

    def own_cot(zz):
        return pltpu.make_async_copy(cot_send.at[zz, s], cots.at[zz * 2 + c, s], cot_recv.at[zz, s])

    def halo_copies(h):
        return [
            remote(cin.at[pl.ds(248, 8)], halo.at[h, 0], halo_send.at[h, 0], halo_recv.at[h, 0], sp=(s + 1) % 16),
            remote(cin.at[pl.ds(0, 8)], halo.at[h, 1], halo_send.at[h, 1], halo_recv.at[h, 1], sp=(s + 15) % 16),
        ]

    def neighbours(h):
        for copy in halo_copies(h):
            copy.wait()
        array = cin[...]
        first = jnp.where(s > 0, halo[h, 0, 7:8, :], 0.0)
        last = jnp.where(s < 15, halo[h, 1, 0:1, :], 0.0)
        before = jnp.where(row == 0, first, pltpu.roll(array, 1, 0))
        after = jnp.where(row == 255, last, pltpu.roll(array, 255, 0))
        return before, array, after

    for copy in halo_copies(0):
        copy.start()

    def selected(k, table):
        return dot(pick_ref[part(k)].reshape(192, 256), table, NN)

    @pl.loop(0, 4)
    def _(k):
        x_send[part(k)] = selected(k, x_ref[...]).astype(BF16).reshape(4, 48, 256)
        for x in range(4):
            peer = 4 * ((y + 4 - k) % 4) + x

            @pl.when(peer == s)
            def _():
                own.start()

            @pl.when(peer != s)
            def _():
                dispatch(peer, s).start()

    def send_cot(zz):
        @pl.loop(0, 4)
        def _(k):
            value = selected(k, tokens[zz].reshape(256, 256))
            factor = scale[part(k)].reshape(192, 128)
            cot_send[zz, part(k), :, pl.ds(0, 128)] = (value[:, :128] * factor).astype(BF16).reshape(4, 48, 128)
            cot_send[zz, part(k), :, pl.ds(128, 128)] = (value[:, 128:] * factor).astype(BF16).reshape(4, 48, 128)
            for x in range(4):
                peer = 4 * ((y + 4 - k) % 4) + x

                @pl.when(peer == s)
                def _():
                    own_cot(zz).start()

                @pl.when(peer != s)
                def _():
                    dispatch_cot(zz, peer, s).start()

    send_cot(z)

    before, here, after = neighbours(0)
    conv = before * taps_ref[0:1, :] + here * taps_ref[1:2, :] + after * taps_ref[2:3, :]
    cout[...] = conv
    mix[s] = (og_ref[...].astype(F32) * conv).astype(BF16)

    def mix_copy(peer, source):
        return remote(mix.at[source], mix.at[source], mix_send.at[peer], mix_recv.at[source], sp=peer)

    for w in weights:
        w.wait()

    def slice_of(zz, core, k):
        return rows.at[zz * 2 + core, part(k)]

    def along_f(d, k):
        at = slice_of((z + 8 - d) % 8, c, k)
        return remote(at, at, af_send.at[d, k], af_recv.at[d, k], tp=up)

    def along_b(d, k):
        at = slice_of((z + d) % 8, c, k)
        return remote(at, at, ab_send.at[d, k], ab_recv.at[d, k], tp=down)

    def to_mate(zz, core, k):
        at = slice_of(zz, core, k)
        return remote(at, at, ap_send.at[zz, k], ap_recv.at[zz, k], tp=mate)

    def multiply(tt, k):
        pre = dot(rows[tt, part(k)].reshape(192, 256), wgu[tt], NN)
        acc[part(k)] += pre.reshape(4, 48, 256)

    def ring_start(k):
        for x in range(4):
            source = 4 * ((y + 4 - k) % 4) + x

            @pl.when(source == s)
            def _():
                own.wait()

            @pl.when(source != s)
            def _():
                dispatch(source, source).wait_recv()

        along_f(0, k).start()
        along_b(0, k).start()
        to_mate(z, c, k).start()
        multiply(t, k)

    @pl.loop(1, 5)
    def _(d):
        zf, zb = (z + 8 - d) % 8, (z + d) % 8
        for k in range(2):
            @pl.when((d < 4) | (k == 0))
            def _():
                at = tokens.at[zf, k]
                remote(at, at, tf_send.at[d - 1, k], tf_recv.at[d - 1, k], tp=up).wait_recv()

                @pl.when((d < 3) | ((d == 3) & (k == 0)))
                def _():
                    token_f(d, k).start()

            @pl.when((d < 4) | (k == 1))
            def _():
                at = tokens.at[zb, k]
                remote(at, at, tb_send.at[d - 1, k], tb_recv.at[d - 1, k], tp=down).wait_recv()

                @pl.when((d < 3) | ((d == 3) & (k == 1)))
                def _():
                    token_b(d, k).start()

        send_cot(zf)

        @pl.when(d < 4)
        def _():
            send_cot(zb)

        @pl.when((d == 2) | (d == 3))
        def _():
            @pl.loop(0, 2)
            def _(k):
                ring_start(2 * d - 4 + k)

    def cot_mate(zz, core):
        at = cots.at[zz * 2 + core]
        return remote(at, at, cp_send.at[zz], cp_recv.at[zz], tp=mate)

    def multiply_cot(tt):
        columns = pl.ds(pl.multiple_of(tt * 256, 256), 256)
        acc_h[...] += dot(cots[tt].reshape(768, 256), wd[:, columns], NT).reshape(16, 48, 128)

    def nth(n):
        return (z + 8 + (1 - 2 * (n % 2)) * ((n + 1) // 2)) % 8

    def cot_own_part(n):
        zz = nth(n)
        own_cot(zz).wait()

        @pl.loop(1, 16)
        def _(i):
            dispatch_cot(zz, (s + i) % 16, (s + i) % 16).wait_recv()

        cot_mate(zz, c).start()
        multiply_cot(zz * 2 + c)

    def cot_mate_part(n):
        zz = nth(n)
        cot_mate(zz, 1 - c).wait_recv()
        multiply_cot(zz * 2 + 1 - c)

    def mate_part(zz, k):
        to_mate(zz, 1 - c, k).wait_recv()
        multiply(zz * 2 + 1 - c, k)

    @pl.loop(0, 16)
    def _(i):
        d, k = i // 4 + 1, i % 4
        even = (k % 2) == 0
        zf, zb = (z + 8 - d) % 8, (z + d) % 8

        @pl.when((d < 4) | even)
        def _():
            at = slice_of(zf, c, k)
            remote(at, at, af_send.at[d - 1, k], af_recv.at[d - 1, k], tp=up).wait_recv()

            @pl.when((d < 3) | ((d == 3) & even))
            def _():
                along_f(d, k).start()

            to_mate(zf, c, k).start()

        @pl.when((d < 4) | (~even))
        def _():
            at = slice_of(zb, c, k)
            remote(at, at, ab_send.at[d - 1, k], ab_recv.at[d - 1, k], tp=down).wait_recv()

            @pl.when((d < 3) | ((d == 3) & (~even)))
            def _():
                along_b(d, k).start()

        @pl.when((d < 4) | (~even))
        def _():
            to_mate(zb, c, k).start()

        @pl.when((d < 4) | even)
        def _():
            multiply(zf * 2 + c, k)

        @pl.when((d < 4) | (~even))
        def _():
            multiply(zb * 2 + c, k)

        e = i // 4

        @pl.when(e == 0)
        def _():
            mate_part(z, k)

        @pl.when(e > 0)
        def _():
            mate_part((z + 8 - e) % 8, k)
            mate_part((z + e) % 8, k)

        @pl.when((i >= 3) & (i % 2 == 1))
        def _():
            cot_own_part((i - 3) // 2)

        @pl.when((i >= 4) & (i % 2 == 0))
        def _():
            cot_mate_part((i - 4) // 2)

    @pl.loop(0, 4)
    def _(k):
        mate_part((z + 4) % 8, k)

    cot_own_part(7)

    @pl.loop(6, 8)
    def _(n):
        cot_mate_part(n)

    @pl.loop(1, 16)
    def _(i):
        mix_copy((s + i) % 16, s).start()

    def dots_of(tt, k):
        return dot(g2[part(k)].reshape(192, 256), wgu[tt], NT)

    def prepare(zz, k):
        value = dots_of(zz * 2 + 1 - c, k)
        q[zz, part(k)] = value.astype(BF16).reshape(4, 48, 256)
        remote(
            q.at[zz, part(k)], r.at[zz, part(k)], rp_send.at[zz, k], rp_recv.at[zz, k], tp=mate
        ).start()

    @pl.loop(0, 4)
    def _(k):
        block = acc[part(k)].reshape(192, 256)
        pre_gate, pre_up = block[:, :128], block[:, 128:]
        grad_hidden = acc_h[part(k)].reshape(192, 128)
        sig = jax.nn.sigmoid(pre_gate)
        activated = pre_gate * sig
        hid[part(k)] = (activated * pre_up).astype(BF16).reshape(4, 48, 128)
        grad_gate = (grad_hidden * pre_up * sig * (1.0 + pre_gate * (1.0 - sig))).astype(BF16)
        grad_up = (grad_hidden * activated).astype(BF16)
        g2[part(k), :, pl.ds(0, 128)] = grad_gate.reshape(4, 48, 128)
        g2[part(k), :, pl.ds(128, 128)] = grad_up.reshape(4, 48, 128)
        prepare((z + 4) % 8, k)

    def summed(zz, k):
        at = r.at[zz, part(k)]
        remote(at, at, rp_send.at[zz, k], rp_recv.at[zz, k], tp=mate).wait_recv()
        return dots_of(zz * 2 + c, k) + r[zz, part(k)].reshape(192, 256).astype(F32)

    def ring_step(d, k, zz, incoming, outgoing, send_sem, recv_sem, to, starts):
        value = summed(zz, k)

        @pl.when(starts)
        def _():
            outgoing[d - 1, part(k)] = value.astype(BF16).reshape(4, 48, 256)

        @pl.when(jnp.logical_not(starts))
        def _():
            at = incoming.at[d, part(k)]
            remote(at, at, send_sem.at[d, k], recv_sem.at[d, k], tp=to).wait_recv()
            both = value + incoming[d, part(k)].reshape(192, 256).astype(F32)
            outgoing[d - 1, part(k)] = both.astype(BF16).reshape(4, 48, 256)

        remote(
            outgoing.at[d - 1, part(k)], incoming.at[d - 1, part(k)],
            send_sem.at[d - 1, k], recv_sem.at[d - 1, k], tp=to,
        ).start()

    def grads(tt):
        x = rows[tt].reshape(768, 256)
        cot = cots[tt].reshape(768, 256)
        grad_gu[tt] = dot(x, g2[...].reshape(768, 256), TN)
        columns = pl.ds(pl.multiple_of(tt * 256, 256), 256)
        grad_d[:, columns] = dot(hid[...].reshape(768, 128), cot, TN)
        for copy in outputs(tt):
            copy.start()

    def outputs(tt):
        columns = pl.ds(pl.multiple_of(tt * 256, 256), 256)
        return [
            pltpu.make_async_copy(grad_gu.at[tt, :, pl.ds(0, 128)], gg_ref.at[tt], out_sem.at[0, tt]),
            pltpu.make_async_copy(grad_gu.at[tt, :, pl.ds(128, 128)], gu_ref.at[tt], out_sem.at[1, tt]),
            pltpu.make_async_copy(grad_d.at[:, columns], gd_ref.at[:, columns], out_sem.at[2, tt]),
        ]

    @pl.loop(0, 16)
    def _(i):
        d, k = 4 - i // 4, i % 4
        even = (k % 2) == 0
        zf, zb = (z + d) % 8, (z + 8 - d) % 8

        @pl.when((d < 4) | even)
        def _():
            ring_step(d, k, zf, in_f, out_f, rf_send, rf_recv, up, (d == 4) | ((d == 3) & (~even)))

        @pl.when((d < 4) | (~even))
        def _():
            ring_step(d, k, zb, in_b, out_b, rb_send, rb_recv, down, (d == 4) | ((d == 3) & even))

        prepare((z + d - 1) % 8, k)

        @pl.when(d > 1)
        def _():
            prepare((z + 9 - d) % 8, k)

        grads(i)

    def giving_back(peer, source):
        return remote(fin.at[peer], ret_ref.at[source], ret_send.at[peer], ret_recv.at[source], sp=peer)

    mine = pltpu.make_async_copy(fin.at[s], ret_ref.at[s], ret_recv.at[s])

    @pl.loop(0, 4)
    def _(k):
        value = summed(z, k)
        for incoming, send_sem, recv_sem, to in ((in_f, rf_send, rf_recv, up), (in_b, rb_send, rb_recv, down)):
            at = incoming.at[0, part(k)]
            remote(at, at, send_sem.at[0, k], recv_sem.at[0, k], tp=to).wait_recv()
            value = value + incoming[0, part(k)].reshape(192, 256).astype(F32)
        fin[part(k)] = value.astype(BF16).reshape(4, 48, 256)
        for x in range(4):
            peer = 4 * ((y + 4 - k) % 4) + x

            @pl.when(peer == s)
            def _():
                mine.start()

            @pl.when(peer != s)
            def _():
                giving_back(peer, s).start()

    @pl.loop(1, 16)
    def _(i):
        giving_back((s + i) % 16, (s + i) % 16).wait_recv()

    mine.wait()

    moe_grad = dot(pick_ref[...].reshape(768, 256), ret_ref[...].reshape(768, 256), TN)
    mixer = (cot_ref[...].astype(F32) + moe_grad).astype(BF16)
    mcf[t] = mixer.reshape(2, 128, 256)
    acc2[...] = jnp.zeros_like(acc2)

    def mc_f(d, k):
        at = mcf.at[((z + 8 - d) % 8) * 2 + c, k]
        return remote(at, at, mf_send.at[d, k], mf_recv.at[d, k], tp=up)

    def mc_b(d, k):
        at = mcf.at[((z + d) % 8) * 2 + c, k]
        return remote(at, at, mb_send.at[d, k], mb_recv.at[d, k], tp=down)

    def mc_mate(zz, core, k):
        at = mcf.at[zz * 2 + core, k]
        return remote(at, at, mp_send.at[zz, k], mp_recv.at[zz, k], tp=mate)

    def column(peer, source):
        return remote(mcf.at[peer, c], col.at[source, c], col_send.at[peer], col_recv.at[source], sp=peer)

    def column_mate(source, core):
        at = col.at[source, core]
        return remote(at, at, colp_send.at[source], colp_recv.at[source], tp=mate)

    kept = pltpu.make_async_copy(mcf.at[s, c], col.at[s, c], col_recv.at[s])

    def use(tt):
        @pl.when(tt == s)
        def _():
            kept.start()

        @pl.when(tt != s)
        def _():
            column(tt, s).start()

        acc2[...] += dot(mcf[tt].reshape(256, 256), op[tt], NN)

    for k in range(2):
        mc_f(0, k).start()
        mc_b(0, k).start()
        mc_mate(z, c, k).start()
    use(t)

    def mc_mate_part(zz):
        for k in range(2):
            mc_mate(zz, 1 - c, k).wait_recv()
        use(zz * 2 + 1 - c)

    @pl.loop(1, 5)
    def _(d):
        zf, zb = (z + 8 - d) % 8, (z + d) % 8
        for k in range(2):
            @pl.when((d < 4) | (k == 0))
            def _():
                at = mcf.at[zf * 2 + c, k]
                remote(at, at, mf_send.at[d - 1, k], mf_recv.at[d - 1, k], tp=up).wait_recv()

                @pl.when((d < 3) | ((d == 3) & (k == 0)))
                def _():
                    mc_f(d, k).start()

                mc_mate(zf, c, k).start()

            @pl.when((d < 4) | (k == 1))
            def _():
                at = mcf.at[zb * 2 + c, k]
                remote(at, at, mb_send.at[d - 1, k], mb_recv.at[d - 1, k], tp=down).wait_recv()

                @pl.when((d < 3) | ((d == 3) & (k == 1)))
                def _():
                    mc_b(d, k).start()

            @pl.when((d < 4) | (k == 1))
            def _():
                mc_mate(zb, c, k).start()

        use(zf * 2 + c)
        mc_mate_part((z + 9 - d) % 8)

        @pl.when(d < 4)
        def _():
            use(zb * 2 + c)

        @pl.when(d > 1)
        def _():
            mc_mate_part((z + d - 1) % 8)

    mc_mate_part((z + 4) % 8)

    grad_mixed = acc2[...]
    gog_ref[...] = (grad_mixed * cout[...]).astype(BF16)
    cin[...] = grad_mixed * og_ref[...].astype(F32)
    for copy in halo_copies(1):
        copy.start()

    kept.wait()
    column_mate(s, c).start()

    @pl.loop(1, 16)
    def _(i):
        source = (s + i) % 16
        column(source, source).wait_recv()
        column_mate(source, c).start()

    gop_ref[...] = jnp.zeros_like(gop_ref)

    @pl.loop(0, 16)
    def _(i):
        source = (s + i) % 16

        @pl.when(i > 0)
        def _():
            mix_copy(source, source).wait_recv()

        column_mate(source, 1 - c).wait_recv()
        gop_ref[...] += dot(col[source].reshape(256, 256), mix[source], TN)

    before, here, after = neighbours(1)
    grad_in = after * taps_ref[0:1, :] + here * taps_ref[1:2, :] + before * taps_ref[2:3, :]
    gig_ref[...] = (grad_in * val_ref[...].astype(F32)).astype(BF16)
    gval_ref[...] = (grad_in * ig_ref[...].astype(F32)).astype(BF16)

    @pl.loop(1, 16)
    def _(i):
        dispatch((s + i) % 16, s).wait_send()
        giving_back((s + i) % 16, s).wait_send()
        mix_copy((s + i) % 16, s).wait_send()
        column((s + i) % 16, s).wait_send()

        @pl.loop(0, 8)
        def _(zz):
            dispatch_cot(zz, (s + i) % 16, s).wait_send()

    @pl.loop(0, 16)
    def _(i):
        column_mate(i, c).wait_send()

        @pl.when(i < 8)
        def _():
            cot_mate(i, c).wait_send()

        mc_mate(i // 2, c, i % 2).wait_send()

    @pl.loop(0, 8)
    def _(i):
        d, k = i // 2, i % 2

        @pl.when((d < 3) | (k == 0))
        def _():
            token_f(d, k).wait_send()
            mc_f(d, k).wait_send()

        @pl.when((d < 3) | (k == 1))
        def _():
            token_b(d, k).wait_send()
            mc_b(d, k).wait_send()

    @pl.loop(0, 16)
    def _(i):
        d, k = i // 4, i % 4
        even = (k % 2) == 0

        @pl.when((d < 3) | even)
        def _():
            along_f(d, k).wait_send()
            at = out_f.at[d, part(k)]
            remote(at, at, rf_send.at[d, k], rf_recv.at[d, k], tp=up).wait_send()

        @pl.when((d < 3) | (~even))
        def _():
            along_b(d, k).wait_send()
            at = out_b.at[d, part(k)]
            remote(at, at, rb_send.at[d, k], rb_recv.at[d, k], tp=down).wait_send()

        for half in range(2):
            zz = d * 2 + half
            to_mate(zz, c, k).wait_send()
            at = q.at[zz, part(k)]
            remote(at, at, rp_send.at[zz, k], rp_recv.at[zz, k], tp=mate).wait_send()
        for copy in outputs(i):
            copy.wait()


def mixer_and_experts(*operands):
    vm = lambda shape, dtype: pltpu.VMEM(shape, dtype)
    dma = lambda *shape: pltpu.SemaphoreType.DMA(shape)
    any_ = pl.BlockSpec(memory_space=pl.ANY)
    vmem = pl.BlockSpec(memory_space=pltpu.VMEM)
    tile = jax.ShapeDtypeStruct((256, 256), BF16)
    return pl.pallas_call(
        moe_kernel,
        out_shape=(
            tile, tile, tile,
            jax.ShapeDtypeStruct((256, 256), F32),
            jax.ShapeDtypeStruct((16, 256, 128), F32),
            jax.ShapeDtypeStruct((16, 256, 128), F32),
            jax.ShapeDtypeStruct((128, 4096), F32),
        ),
        in_specs=[vmem] * 8 + [any_] * 4,
        out_specs=(vmem,) * 4 + (any_,) * 3,
        scratch_shapes=[
            vm((16, 48, 256), BF16),
            vm((16, 48, 128), F32),
            vm((8, 2, 128, 256), BF16),
            vm((16, 48, 256), BF16),
            vm((8, 16, 48, 256), BF16),
            vm((16, 16, 48, 256), BF16),
            vm((16, 16, 48, 256), BF16),
            vm((16, 256, 256), BF16),
            vm((128, 4096), BF16),
            vm((16, 48, 256), F32),
            vm((16, 48, 128), F32),
            vm((16, 48, 256), BF16),
            vm((16, 48, 128), BF16),
            vm((8, 16, 48, 256), BF16),
            vm((8, 16, 48, 256), BF16),
            vm((4, 16, 48, 256), BF16),
            vm((4, 16, 48, 256), BF16),
            vm((4, 16, 48, 256), BF16),
            vm((4, 16, 48, 256), BF16),
            vm((16, 48, 256), BF16),
            vm((16, 256, 256), F32),
            vm((128, 4096), F32),
            vm((16, 48, 256), BF16),
            vm((16, 256, 256), BF16),
            vm((256, 256), F32),
            vm((256, 256), F32),
            vm((2, 2, 8, 256), F32),
            vm((16, 256, 256), BF16),
            vm((16, 2, 128, 256), BF16),
            vm((16, 2, 128, 256), BF16),
            vm((256, 256), F32),
            dma(4), dma(16), dma(16),
            dma(4, 4), dma(4, 4), dma(4, 4), dma(4, 4), dma(8, 4), dma(8, 4),
            dma(8, 4), dma(8, 4), dma(4, 4), dma(4, 4), dma(4, 4), dma(4, 4),
            dma(16), dma(16), dma(3, 16),
            dma(2, 2), dma(2, 2), dma(16), dma(16),
            dma(4, 2), dma(4, 2), dma(4, 2), dma(4, 2), dma(8, 2), dma(8, 2),
            dma(16), dma(16), dma(16), dma(16),
            dma(4, 2), dma(4, 2), dma(4, 2), dma(4, 2), dma(8, 16), dma(8, 16), dma(8), dma(8),
        ],
        compiler_params=pltpu.CompilerParams(
            collective_id=1, has_side_effects=True, vmem_limit_bytes=67043328
        ),
        cost_estimate=pl.CostEstimate(flops=8_000_000_000, bytes_accessed=20_000_000, transcendentals=100_000),
        name="mixer_and_experts",
    )(*operands)


def write_out(*refs):
    count = len(refs) // 3
    sources, targets, held = refs[:count], refs[count : 2 * count], refs[2 * count : 3 * count]
    in_sem, out_sem = refs[3 * count :]
    steps = []
    for i, ref in enumerate(sources):
        pieces = 4 if i < 3 else 1
        size = ref.shape[0] // pieces
        for p in range(pieces):
            at = pl.ds(p * size, size)
            n = len(steps)
            steps.append((
                pltpu.make_async_copy(ref.at[at], held[i].at[at], in_sem.at[n]),
                pltpu.make_async_copy(held[i].at[at], targets[i].at[at], out_sem.at[n]),
            ))
    for fetch, _ in steps:
        fetch.start()
    for fetch, store in steps:
        fetch.wait()
        store.start()
    for _, store in steps:
        store.wait()


def written(*arrays):
    any_ = pl.BlockSpec(memory_space=pl.ANY)
    shapes = [jax.ShapeDtypeStruct(a.shape, a.dtype) for a in arrays]
    return pl.pallas_call(
        write_out,
        out_shape=tuple(shapes),
        in_specs=[any_] * len(shapes),
        out_specs=(any_,) * len(shapes),
        scratch_shapes=[pltpu.VMEM(a.shape, a.dtype) for a in shapes]
        + [pltpu.SemaphoreType.DMA((16,)), pltpu.SemaphoreType.DMA((16,))],
        compiler_params=pltpu.CompilerParams(vmem_limit_bytes=16 * 1024 * 1024),
        name="write_out",
    )(*arrays)


def body(moe_input, out_gate, in_gate, values, conv_taps, out_proj, route_ids, route_gates, expert_gate, expert_up, expert_down, cotangent):
    gog, gig, gval, gop, gg, gu, gd = mixer_and_experts(
        route_ids.T, route_gates.T, moe_input, cotangent, out_gate, in_gate, values, conv_taps,
        expert_gate.reshape(16, 256, 128),
        expert_up.reshape(16, 256, 128),
        expert_down.reshape(128, 4096),
        out_proj.reshape(16, 256, 256),
    )
    gg, gu, gd, gop, gog, gig, gval = written(
        gg.reshape(4096, 128), gu.reshape(4096, 128), gd, gop, gog, gig, gval
    )
    return (gog, gig, gval, gop, gg.reshape(1, 4096, 128), gu.reshape(1, 4096, 128), gd.reshape(1, 128, 4096))


def solution(mesh):
    in_specs = (
        P("sp", "tp"), P("sp", "tp"), P("sp", "tp"), P("sp", "tp"), P(None, "tp"), P(None, "tp"),
        P("sp", None), P("sp", None),
        P("sp", None, "tp"), P("sp", None, "tp"), P("sp", "tp", None), P("sp", "tp"),
    )
    out_specs = (
        P("sp", "tp"), P("sp", "tp"), P("sp", "tp"), P("sp", "tp"),
        P("sp", None, "tp"), P("sp", None, "tp"), P("sp", "tp", None),
    )
    return jax.shard_map(body, mesh=mesh, in_specs=in_specs, out_specs=out_specs, check_vma=False)
```

```python
import functools
import jax
import jax.numpy as jnp
from jax import lax
from jax.experimental import pallas as pl
from jax.experimental.pallas import tpu as pltpu
from jax.sharding import PartitionSpec as P

F32 = jnp.float32
BF16 = jnp.bfloat16
MESH = pl.DeviceIdType.MESH
NT = (((1,), (1,)), ((), ()))
TN = (((0,), (0,)), ((), ()))
NN = (((1,), (0,)), ((), ()))


def dot(a, b, dims):
    return lax.dot_general(a, b, dims, preferred_element_type=F32)


(DISPATCH, ROWS, COT, COT_MATE, TOKEN_RING, HALO, HALO_BACK, MIXED, MATE_SUMS, SUMS, RETURNED,
 MIXER, COLUMN, COLUMN_MATE) = range(14)


def moe_kernel(
    ids_ref, gates_ref, x_ref, cot_ref, og_ref, ig_ref, val_ref, taps_ref, wg_ref, wu_ref, wd_ref, op_ref,
    gog_ref, gig_ref, gval_ref, gop_ref, gg_ref, gu_ref, gd_ref,
    pick_ref, scale, tokens, x_send, cot_send, rows, cots, wgu, wd, acc, acc_h, g2, hid, q, r, in_f, in_b, out_f, out_b, fin, grad_gu, grad_d,
    ret_ref, op, cin, cout, halo, mix_t, mcf, col, acc2,
    w_sem, out_sem, sent,
    disp_recv, af_recv, ab_recv, ap_recv, rp_recv, rf_recv, rb_recv, ret_recv,
    halo_recv, mix_recv, mf_recv, mb_recv, mp_recv, col_recv, colp_recv,
    tf_recv, tb_recv, cot_recv, cp_recv,
):
    s = lax.axis_index("sp")
    t = lax.axis_index("tp")
    z, c = t // 2, t % 2
    y = s // 4
    up, down, mate = ((z + 1) % 8) * 2 + c, ((z + 7) % 8) * 2 + c, z * 2 + (1 - c)

    barrier = pltpu.get_barrier_semaphore()

    @pl.loop(1, 16)
    def _(i):
        pl.semaphore_signal(barrier, inc=1, device_id={"sp": (s + i) % 16}, device_id_type=MESH)

    for other in (up, down, mate):
        pl.semaphore_signal(barrier, inc=1, device_id={"tp": other}, device_id_type=MESH)

    weights = [
        pltpu.make_async_copy(wg_ref, wgu.at[:, :, pl.ds(0, 128)], w_sem.at[0]),
        pltpu.make_async_copy(wu_ref, wgu.at[:, :, pl.ds(128, 128)], w_sem.at[1]),
        pltpu.make_async_copy(wd_ref, wd, w_sem.at[2]),
        pltpu.make_async_copy(op_ref, op, w_sem.at[3]),
    ]
    for w in weights:
        w.start()

    cin[...] = ig_ref[...].astype(F32) * val_ref[...].astype(F32)

    expert = lax.broadcasted_iota(jnp.int32, (16, 256), 0)
    named = [ids_ref[i : i + 1, :] == expert for i in range(2)]
    member = jnp.where(named[0] | named[1], 1.0, 0.0)
    weight = jnp.where(named[0], gates_ref[0:1, :], 0.0) + jnp.where(named[1], gates_ref[1:2, :], 0.0)
    row = lax.broadcasted_iota(jnp.int32, (256, 256), 0)
    earlier = jnp.where(row < lax.broadcasted_iota(jnp.int32, (256, 256), 1), 1.0, 0.0).astype(BF16)
    place = jnp.where(member > 0, dot(member.astype(BF16), earlier, NN), -1.0)
    position = lax.broadcasted_iota(jnp.int32, (48, 256), 0).astype(F32)
    for e in range(16):
        hit = place[e : e + 1, :] == position
        pick_ref[e] = jnp.where(hit, 1.0, 0.0).astype(BF16)
        slot_weight = jnp.sum(jnp.where(hit, weight[e : e + 1, :], 0.0), axis=1, keepdims=True)
        scale[e] = jnp.broadcast_to(slot_weight, (48, 128))
    tokens[z] = cot_ref[...].reshape(2, 128, 256)
    acc[...] = jnp.zeros_like(acc)
    acc_h[...] = jnp.zeros_like(acc_h)

    pl.semaphore_wait(barrier, 18)

    def remote(src, dst, send_sem, recv_sem, **where):
        return pltpu.make_async_remote_copy(
            src_ref=src, dst_ref=dst, send_sem=send_sem, recv_sem=recv_sem,
            device_id=where, device_id_type=MESH,
        )

    def part(k):
        return pl.ds(4 * ((y + 4 - k) % 4), 4)

    def token_f(d, k):
        at = tokens.at[(z + 8 - d) % 8, k]
        return remote(at, at, sent.at[TOKEN_RING], tf_recv.at[d, k], tp=up)

    def token_b(d, k):
        at = tokens.at[(z + d) % 8, k]
        return remote(at, at, sent.at[TOKEN_RING], tb_recv.at[d, k], tp=down)

    for k in range(2):
        from_cot = cot_ref.at[pl.ds(128 * k, 128)]
        remote(from_cot, tokens.at[z, k], sent.at[TOKEN_RING], tf_recv.at[0, k], tp=up).start()
        remote(from_cot, tokens.at[z, k], sent.at[TOKEN_RING], tb_recv.at[0, k], tp=down).start()

    def dispatch(peer):
        return remote(x_send.at[peer], rows.at[t, s], sent.at[DISPATCH], disp_recv.at[y], sp=peer)

    own = pltpu.make_async_copy(x_send.at[s], rows.at[t, s], disp_recv.at[y])

    def dispatch_cot(zz, peer):
        return remote(
            cot_send.at[zz, peer], cots.at[zz * 2 + c, s], sent.at[COT], cot_recv.at[zz], sp=peer
        )

    def own_cot(zz):
        return pltpu.make_async_copy(cot_send.at[zz, s], cots.at[zz * 2 + c, s], cot_recv.at[zz])

    def arrived(at, recv_sem):
        remote(at, at, recv_sem, recv_sem, tp=mate).wait_recv()

    def sent_all(at, index):
        remote(at, at, sent.at[index], sent.at[index], tp=mate).wait_send()

    def halo_copies(h):
        return [
            remote(cin.at[pl.ds(248, 8)], halo.at[h, 0], sent.at[HALO + h], halo_recv.at[h, 0], sp=(s + 1) % 16),
            remote(cin.at[pl.ds(0, 8)], halo.at[h, 1], sent.at[HALO + h], halo_recv.at[h, 1], sp=(s + 15) % 16),
        ]

    def neighbours(h):
        for copy in halo_copies(h):
            copy.wait_recv()
        sent_all(halo.at[h], HALO + h)
        array = cin[...]
        first = jnp.where(s > 0, halo[h, 0, 7:8, :], 0.0)
        last = jnp.where(s < 15, halo[h, 1, 0:1, :], 0.0)
        before = jnp.where(row == 0, first, pltpu.roll(array, 1, 0))
        after = jnp.where(row == 255, last, pltpu.roll(array, 255, 0))
        return before, array, after

    for copy in halo_copies(0):
        copy.start()

    def selected(k, table):
        return dot(pick_ref[part(k)].reshape(192, 256), table, NN)

    @pl.loop(0, 4)
    def _(k):
        x_send[part(k)] = selected(k, x_ref[...]).astype(BF16).reshape(4, 48, 256)
        for x in range(4):
            peer = 4 * ((y + 4 - k) % 4) + x

            @pl.when(peer == s)
            def _():
                own.start()

            @pl.when(peer != s)
            def _():
                dispatch(peer).start()

    def send_cot(zz):
        @pl.loop(0, 4)
        def _(k):
            value = selected(k, tokens[zz].reshape(256, 256))
            factor = scale[part(k)].reshape(192, 128)
            cot_send[zz, part(k), :, pl.ds(0, 128)] = (value[:, :128] * factor).astype(BF16).reshape(4, 48, 128)
            cot_send[zz, part(k), :, pl.ds(128, 128)] = (value[:, 128:] * factor).astype(BF16).reshape(4, 48, 128)
            for x in range(4):
                peer = 4 * ((y + 4 - k) % 4) + x

                @pl.when(peer == s)
                def _():
                    own_cot(zz).start()

                @pl.when(peer != s)
                def _():
                    dispatch_cot(zz, peer).start()

    send_cot(z)

    for w in weights:
        w.wait()

    def slice_of(zz, core, k):
        return rows.at[zz * 2 + core, part(k)]

    def along_f(d, k):
        at = slice_of((z + 8 - d) % 8, c, k)
        return remote(at, at, sent.at[ROWS], af_recv.at[d, k], tp=up)

    def along_b(d, k):
        at = slice_of((z + d) % 8, c, k)
        return remote(at, at, sent.at[ROWS], ab_recv.at[d, k], tp=down)

    def to_mate(zz, core, k):
        at = slice_of(zz, core, k)
        return remote(at, at, sent.at[ROWS], ap_recv.at[zz, k], tp=mate)

    def multiply(tt, k):
        pre = dot(rows[tt, part(k)].reshape(192, 256), wgu[tt], NN)
        acc[part(k)] += pre.reshape(4, 48, 256)

    def ring_start(k):
        arrived(slice_of(z, c, k), disp_recv.at[(y + 4 - k) % 4])
        along_f(0, k).start()
        along_b(0, k).start()
        to_mate(z, c, k).start()
        multiply(t, k)

    @pl.loop(1, 5)
    def _(d):
        zf, zb = (z + 8 - d) % 8, (z + d) % 8
        for k in range(2):
            @pl.when((d < 4) | (k == 0))
            def _():
                at = tokens.at[zf, k]
                remote(at, at, sent.at[TOKEN_RING], tf_recv.at[d - 1, k], tp=up).wait_recv()

                @pl.when((d < 3) | ((d == 3) & (k == 0)))
                def _():
                    token_f(d, k).start()

            @pl.when((d < 4) | (k == 1))
            def _():
                at = tokens.at[zb, k]
                remote(at, at, sent.at[TOKEN_RING], tb_recv.at[d - 1, k], tp=down).wait_recv()

                @pl.when((d < 3) | ((d == 3) & (k == 1)))
                def _():
                    token_b(d, k).start()

        ring_start(d - 1)
        send_cot(zf)

        @pl.when(d < 4)
        def _():
            send_cot(zb)

    def cot_mate(zz, core):
        at = cots.at[zz * 2 + core]
        return remote(at, at, sent.at[COT_MATE], cp_recv.at[zz], tp=mate)

    def multiply_cot(tt):
        columns = pl.ds(pl.multiple_of(tt * 256, 256), 256)
        acc_h[...] += dot(cots[tt].reshape(768, 256), wd[:, columns], NT).reshape(16, 48, 128)

    def nth(n):
        return (z + 8 + (1 - 2 * (n % 2)) * ((n + 1) // 2)) % 8

    def cot_own_part(n):
        zz = nth(n)
        arrived(cots.at[zz * 2 + c], cot_recv.at[zz])
        cot_mate(zz, c).start()
        multiply_cot(zz * 2 + c)

    def cot_mate_part(n):
        zz = nth(n)
        cot_mate(zz, 1 - c).wait_recv()
        multiply_cot(zz * 2 + 1 - c)

    def mate_part(zz, k):
        to_mate(zz, 1 - c, k).wait_recv()
        multiply(zz * 2 + 1 - c, k)

    @pl.loop(0, 16)
    def _(i):
        d, k = i // 4 + 1, i % 4
        even = (k % 2) == 0
        zf, zb = (z + 8 - d) % 8, (z + d) % 8

        @pl.when((d < 4) | even)
        def _():
            at = slice_of(zf, c, k)
            remote(at, at, sent.at[ROWS], af_recv.at[d - 1, k], tp=up).wait_recv()

            @pl.when((d < 3) | ((d == 3) & even))
            def _():
                along_f(d, k).start()

            to_mate(zf, c, k).start()

        @pl.when((d < 4) | (~even))
        def _():
            at = slice_of(zb, c, k)
            remote(at, at, sent.at[ROWS], ab_recv.at[d - 1, k], tp=down).wait_recv()

            @pl.when((d < 3) | ((d == 3) & (~even)))
            def _():
                along_b(d, k).start()

        @pl.when((d < 4) | (~even))
        def _():
            to_mate(zb, c, k).start()

        @pl.when((d < 4) | even)
        def _():
            multiply(zf * 2 + c, k)

        @pl.when((d < 4) | (~even))
        def _():
            multiply(zb * 2 + c, k)

        e = i // 4

        @pl.when(e == 0)
        def _():
            mate_part(z, k)

        @pl.when(e > 0)
        def _():
            mate_part((z + 8 - e) % 8, k)
            mate_part((z + e) % 8, k)

        @pl.when((i >= 3) & (i % 2 == 1))
        def _():
            cot_own_part((i - 3) // 2)

        @pl.when((i >= 4) & (i % 2 == 0))
        def _():
            cot_mate_part((i - 4) // 2)

    @pl.loop(0, 4)
    def _(k):
        mate_part((z + 4) % 8, k)

    cot_own_part(7)

    @pl.loop(6, 8)
    def _(n):
        cot_mate_part(n)

    before, here, after = neighbours(0)
    conv = before * taps_ref[0:1, :] + here * taps_ref[1:2, :] + after * taps_ref[2:3, :]
    cout[...] = conv
    mine_t = pl.ds(pl.multiple_of(s * 256, 256), 256)
    mix_t[:, mine_t] = (og_ref[...].astype(F32) * conv).T.astype(BF16)

    @pl.loop(1, 16)
    def _(i):
        remote(
            mix_t.at[:, mine_t], mix_t.at[:, mine_t], sent.at[MIXED], mix_recv.at[0], sp=(s + i) % 16
        ).start()

    def dots_of(tt, k):
        return dot(g2[part(k)].reshape(192, 256), wgu[tt], NT)

    def prepare(zz, k):
        value = dots_of(zz * 2 + 1 - c, k)
        q[zz, part(k)] = value.astype(BF16).reshape(4, 48, 256)
        remote(
            q.at[zz, part(k)], r.at[zz, part(k)], sent.at[MATE_SUMS], rp_recv.at[zz, k], tp=mate
        ).start()

    @pl.loop(0, 4)
    def _(k):
        block = acc[part(k)].reshape(192, 256)
        pre_gate, pre_up = block[:, :128], block[:, 128:]
        grad_hidden = acc_h[part(k)].reshape(192, 128)
        sig = jax.nn.sigmoid(pre_gate)
        activated = pre_gate * sig
        hid[part(k)] = (activated * pre_up).astype(BF16).reshape(4, 48, 128)
        grad_gate = (grad_hidden * pre_up * sig * (1.0 + pre_gate * (1.0 - sig))).astype(BF16)
        grad_up = (grad_hidden * activated).astype(BF16)
        g2[part(k), :, pl.ds(0, 128)] = grad_gate.reshape(4, 48, 128)
        g2[part(k), :, pl.ds(128, 128)] = grad_up.reshape(4, 48, 128)
        prepare((z + 4) % 8, k)

    def summed(zz, k):
        at = r.at[zz, part(k)]
        remote(at, at, sent.at[MATE_SUMS], rp_recv.at[zz, k], tp=mate).wait_recv()
        return dots_of(zz * 2 + c, k) + r[zz, part(k)].reshape(192, 256).astype(F32)

    def ring_step(d, k, zz, incoming, outgoing, recv_sem, to, starts):
        value = summed(zz, k)

        @pl.when(starts)
        def _():
            outgoing[d - 1, part(k)] = value.astype(BF16).reshape(4, 48, 256)

        @pl.when(jnp.logical_not(starts))
        def _():
            at = incoming.at[d, part(k)]
            arrived(at, recv_sem.at[d, k])
            both = value + incoming[d, part(k)].reshape(192, 256).astype(F32)
            outgoing[d - 1, part(k)] = both.astype(BF16).reshape(4, 48, 256)

        remote(
            outgoing.at[d - 1, part(k)], incoming.at[d - 1, part(k)],
            sent.at[SUMS], recv_sem.at[d - 1, k], tp=to,
        ).start()

    def grads(tt):
        x = rows[tt].reshape(768, 256)
        cot = cots[tt].reshape(768, 256)
        grad_gu[tt] = dot(x, g2[...].reshape(768, 256), TN)
        columns = pl.ds(pl.multiple_of(tt * 256, 256), 256)
        grad_d[:, columns] = dot(hid[...].reshape(768, 128), cot, TN)
        for copy in outputs(tt):
            copy.start()

    def outputs(tt):
        columns = pl.ds(pl.multiple_of(tt * 256, 256), 256)
        return [
            pltpu.make_async_copy(grad_gu.at[tt, :, pl.ds(0, 128)], gg_ref.at[tt], out_sem.at[0]),
            pltpu.make_async_copy(grad_gu.at[tt, :, pl.ds(128, 128)], gu_ref.at[tt], out_sem.at[1]),
            pltpu.make_async_copy(grad_d.at[:, columns], gd_ref.at[:, columns], out_sem.at[2]),
        ]

    @pl.loop(0, 16)
    def _(i):
        d, k = 4 - i // 4, i % 4
        even = (k % 2) == 0
        zf, zb = (z + d) % 8, (z + 8 - d) % 8

        @pl.when((d < 4) | even)
        def _():
            ring_step(d, k, zf, in_f, out_f, rf_recv, up, (d == 4) | ((d == 3) & (~even)))

        @pl.when((d < 4) | (~even))
        def _():
            ring_step(d, k, zb, in_b, out_b, rb_recv, down, (d == 4) | ((d == 3) & even))

        prepare((z + d - 1) % 8, k)

        @pl.when(d > 1)
        def _():
            prepare((z + 9 - d) % 8, k)

        grads(i)

    def giving_back(peer):
        return remote(fin.at[peer], ret_ref.at[s], sent.at[RETURNED], ret_recv.at[0], sp=peer)

    mine = pltpu.make_async_copy(fin.at[s], ret_ref.at[s], ret_recv.at[0])

    @pl.loop(0, 4)
    def _(k):
        value = summed(z, k)
        for incoming, recv_sem in ((in_f, rf_recv), (in_b, rb_recv)):
            arrived(incoming.at[0, part(k)], recv_sem.at[0, k])
            value = value + incoming[0, part(k)].reshape(192, 256).astype(F32)
        fin[part(k)] = value.astype(BF16).reshape(4, 48, 256)
        for x in range(4):
            peer = 4 * ((y + 4 - k) % 4) + x

            @pl.when(peer == s)
            def _():
                mine.start()

            @pl.when(peer != s)
            def _():
                giving_back(peer).start()

    arrived(ret_ref, ret_recv.at[0])
    moe_grad = dot(pick_ref[...].reshape(768, 256), ret_ref[...].reshape(768, 256), TN)
    mixer = (cot_ref[...].astype(F32) + moe_grad).astype(BF16)
    mcf[t] = mixer.reshape(4, 64, 256)
    acc2[...] = jnp.zeros_like(acc2)

    def mc_f(d, k):
        at = mcf.at[((z + 8 - d) % 8) * 2 + c, k]
        return remote(at, at, sent.at[MIXER], mf_recv.at[d, k], tp=up)

    def mc_b(d, k):
        at = mcf.at[((z + d) % 8) * 2 + c, k]
        return remote(at, at, sent.at[MIXER], mb_recv.at[d, k], tp=down)

    def mc_mate(zz, core):
        at = mcf.at[zz * 2 + core]
        return remote(at, at, sent.at[MIXER], mp_recv.at[zz], tp=mate)

    half = pl.ds(2 * c, 2)

    def column(peer):
        return remote(mcf.at[peer, half], col.at[s, half], sent.at[COLUMN], col_recv.at[y], sp=peer)

    kept = pltpu.make_async_copy(mcf.at[s, half], col.at[s, half], col_recv.at[y])

    def use(tt):
        @pl.when(tt == s)
        def _():
            kept.start()

        @pl.when(tt != s)
        def _():
            column(tt).start()

        acc2[...] += dot(mcf[tt].reshape(256, 256), op[tt], NN)

    for k in range(4):
        mc_f(0, k).start()
        mc_b(0, k).start()
    mc_mate(z, c).start()
    use(t)

    def mc_mate_part(zz):
        mc_mate(zz, 1 - c).wait_recv()
        use(zz * 2 + 1 - c)

    @pl.loop(1, 5)
    def _(d):
        zf, zb = (z + 8 - d) % 8, (z + d) % 8
        for k in range(4):
            @pl.when((d < 4) | (k < 2))
            def _():
                arrived(mcf.at[zf * 2 + c, k], mf_recv.at[d - 1, k])

                @pl.when((d < 3) | ((d == 3) & (k < 2)))
                def _():
                    mc_f(d, k).start()

            @pl.when((d < 4) | (k >= 2))
            def _():
                arrived(mcf.at[zb * 2 + c, k], mb_recv.at[d - 1, k])

                @pl.when((d < 3) | ((d == 3) & (k >= 2)))
                def _():
                    mc_b(d, k).start()

        mc_mate(zf, c).start()

        @pl.when(d < 4)
        def _():
            mc_mate(zb, c).start()

        use(zf * 2 + c)
        mc_mate_part((z + 9 - d) % 8)

        @pl.when(d < 4)
        def _():
            use(zb * 2 + c)

        @pl.when(d > 1)
        def _():
            mc_mate_part((z + d - 1) % 8)

    mc_mate_part((z + 4) % 8)

    grad_mixed = acc2[...]
    gog_ref[...] = (grad_mixed * cout[...]).astype(BF16)
    cin[...] = grad_mixed * og_ref[...].astype(F32)
    for copy in halo_copies(1):
        copy.start()

    def column_mate(k, core):
        at = col.at[part(k), pl.ds(2 * core, 2)]
        return remote(at, at, sent.at[COLUMN_MATE], colp_recv.at[(y + 4 - k) % 4], tp=mate)

    for k in range(4):
        arrived(col.at[part(k), half], col_recv.at[(y + 4 - k) % 4])
        column_mate(k, c).start()
    arrived(mix_t.at[:, pl.ds(0, 15 * 256)], mix_recv.at[0])
    for k in range(4):
        column_mate(k, 1 - c).wait_recv()
    gop_ref[...] = dot(mix_t[...], col[...].reshape(4096, 256), NN).T

    before, here, after = neighbours(1)
    grad_in = after * taps_ref[0:1, :] + here * taps_ref[1:2, :] + before * taps_ref[2:3, :]
    gig_ref[...] = (grad_in * val_ref[...].astype(F32)).astype(BF16)
    gval_ref[...] = (grad_in * ig_ref[...].astype(F32)).astype(BF16)

    sent_all(rows.at[0, pl.ds(0, 15)], DISPATCH)
    sent_all(rows.at[pl.ds(0, 15)], ROWS)
    sent_all(cots.at[pl.ds(0, 8), pl.ds(0, 15)], COT)
    sent_all(cots.at[pl.ds(0, 8)], COT_MATE)
    sent_all(tokens.at[pl.ds(0, 7)], TOKEN_RING)
    sent_all(mix_t.at[:, pl.ds(0, 15 * 256)], MIXED)
    sent_all(q, MATE_SUMS)
    sent_all(q.at[pl.ds(0, 7)], SUMS)
    sent_all(fin.at[pl.ds(0, 15)], RETURNED)
    sent_all(mcf.at[pl.ds(0, 15)], MIXER)
    sent_all(mcf.at[pl.ds(0, 15), pl.ds(0, 2)], COLUMN)
    sent_all(col.at[:, pl.ds(0, 2)], COLUMN_MATE)
    pltpu.make_async_copy(grad_gu.at[:, :, pl.ds(0, 128)], gg_ref, out_sem.at[0]).wait()
    pltpu.make_async_copy(grad_gu.at[:, :, pl.ds(128, 128)], gu_ref, out_sem.at[1]).wait()
    pltpu.make_async_copy(grad_d, gd_ref, out_sem.at[2]).wait()


def mixer_and_experts(*operands):
    vm = lambda shape, dtype: pltpu.VMEM(shape, dtype)
    dma = lambda *shape: pltpu.SemaphoreType.DMA(shape)
    any_ = pl.BlockSpec(memory_space=pl.ANY)
    vmem = pl.BlockSpec(memory_space=pltpu.VMEM)
    tile = jax.ShapeDtypeStruct((256, 256), BF16)
    return pl.pallas_call(
        moe_kernel,
        out_shape=(
            tile, tile, tile,
            jax.ShapeDtypeStruct((256, 256), F32),
            jax.ShapeDtypeStruct((16, 256, 128), F32),
            jax.ShapeDtypeStruct((16, 256, 128), F32),
            jax.ShapeDtypeStruct((128, 4096), F32),
        ),
        in_specs=[vmem] * 8 + [any_] * 4,
        out_specs=(vmem,) * 4 + (any_,) * 3,
        scratch_shapes=[
            vm((16, 48, 256), BF16),
            vm((16, 48, 128), F32),
            vm((8, 2, 128, 256), BF16),
            vm((16, 48, 256), BF16),
            vm((8, 16, 48, 256), BF16),
            vm((16, 16, 48, 256), BF16),
            vm((16, 16, 48, 256), BF16),
            vm((16, 256, 256), BF16),
            vm((128, 4096), BF16),
            vm((16, 48, 256), F32),
            vm((16, 48, 128), F32),
            vm((16, 48, 256), BF16),
            vm((16, 48, 128), BF16),
            vm((8, 16, 48, 256), BF16),
            vm((8, 16, 48, 256), BF16),
            vm((4, 16, 48, 256), BF16),
            vm((4, 16, 48, 256), BF16),
            vm((4, 16, 48, 256), BF16),
            vm((4, 16, 48, 256), BF16),
            vm((16, 48, 256), BF16),
            vm((16, 256, 256), F32),
            vm((128, 4096), F32),
            vm((16, 48, 256), BF16),
            vm((16, 256, 256), BF16),
            vm((256, 256), F32),
            vm((256, 256), F32),
            vm((2, 2, 8, 256), F32),
            vm((256, 4096), BF16),
            vm((16, 4, 64, 256), BF16),
            vm((16, 4, 64, 256), BF16),
            vm((256, 256), F32),
            dma(4), dma(3), dma(14),
            dma(4), dma(4, 4), dma(4, 4), dma(8, 4), dma(8, 4), dma(4, 4), dma(4, 4), dma(1),
            dma(2, 2), dma(1), dma(4, 4), dma(4, 4), dma(8), dma(4), dma(4),
            dma(4, 2), dma(4, 2), dma(8), dma(8),
        ],
        compiler_params=pltpu.CompilerParams(
            collective_id=1, has_side_effects=True, vmem_limit_bytes=67043328
        ),
        cost_estimate=pl.CostEstimate(flops=8_000_000_000, bytes_accessed=20_000_000, transcendentals=100_000),
        name="mixer_and_experts",
    )(*operands)


def write_out(*refs):
    count = len(refs) // 3
    sources, targets, held = refs[:count], refs[count : 2 * count], refs[2 * count : 3 * count]
    in_sem, out_sem = refs[3 * count :]
    steps = []
    for i, ref in enumerate(sources):
        pieces = 4 if i < 3 else 1
        size = ref.shape[0] // pieces
        for p in range(pieces):
            at = pl.ds(p * size, size)
            n = len(steps)
            steps.append((
                pltpu.make_async_copy(ref.at[at], held[i].at[at], in_sem.at[n]),
                pltpu.make_async_copy(held[i].at[at], targets[i].at[at], out_sem.at[n]),
            ))
    for fetch, _ in steps:
        fetch.start()
    for fetch, store in steps:
        fetch.wait()
        store.start()
    for _, store in steps:
        store.wait()


def written(*arrays):
    any_ = pl.BlockSpec(memory_space=pl.ANY)
    shapes = [jax.ShapeDtypeStruct(a.shape, a.dtype) for a in arrays]
    return pl.pallas_call(
        write_out,
        out_shape=tuple(shapes),
        in_specs=[any_] * len(shapes),
        out_specs=(any_,) * len(shapes),
        scratch_shapes=[pltpu.VMEM(a.shape, a.dtype) for a in shapes]
        + [pltpu.SemaphoreType.DMA((16,)), pltpu.SemaphoreType.DMA((16,))],
        compiler_params=pltpu.CompilerParams(vmem_limit_bytes=67043328),
        name="write_out",
    )(*arrays)


def body(moe_input, out_gate, in_gate, values, conv_taps, out_proj, route_ids, route_gates, expert_gate, expert_up, expert_down, cotangent):
    gog, gig, gval, gop, gg, gu, gd = mixer_and_experts(
        route_ids.T, route_gates.T, moe_input, cotangent, out_gate, in_gate, values, conv_taps,
        expert_gate.reshape(16, 256, 128),
        expert_up.reshape(16, 256, 128),
        expert_down.reshape(128, 4096),
        out_proj.reshape(16, 256, 256),
    )
    gg, gu, gd, gop, gog, gig, gval = written(
        gg.reshape(4096, 128), gu.reshape(4096, 128), gd, gop, gog, gig, gval
    )
    return (gog, gig, gval, gop, gg.reshape(1, 4096, 128), gu.reshape(1, 4096, 128), gd.reshape(1, 128, 4096))


def solution(mesh):
    in_specs = (
        P("sp", "tp"), P("sp", "tp"), P("sp", "tp"), P("sp", "tp"), P(None, "tp"), P(None, "tp"),
        P("sp", None), P("sp", None),
        P("sp", None, "tp"), P("sp", None, "tp"), P("sp", "tp", None), P("sp", "tp"),
    )
    out_specs = (
        P("sp", "tp"), P("sp", "tp"), P("sp", "tp"), P("sp", "tp"),
        P("sp", None, "tp"), P("sp", None, "tp"), P("sp", "tp", None),
    )
    return jax.shard_map(body, mesh=mesh, in_specs=in_specs, out_specs=out_specs, check_vma=False)
```

```python
import functools
import jax
import jax.numpy as jnp
from jax import lax
from jax.experimental import pallas as pl
from jax.experimental.pallas import tpu as pltpu
from jax.sharding import PartitionSpec as P

F32 = jnp.float32
BF16 = jnp.bfloat16
MESH = pl.DeviceIdType.MESH
NT = (((1,), (1,)), ((), ()))
TN = (((0,), (0,)), ((), ()))
NN = (((1,), (0,)), ((), ()))


def dot(a, b, dims):
    return lax.dot_general(a, b, dims, preferred_element_type=F32)


(DISPATCH, ROWS, COT, COT_MATE, TOKEN_RING, HALO, HALO_BACK, MIXED, MATE_SUMS, SUMS, RETURNED,
 MIXER, COLUMN, COLUMN_MATE) = range(14)


def moe_kernel(
    ids_ref, gates_ref, taps_ref, x_hbm, cot_hbm, og_hbm, ig_hbm, val_hbm, wg_ref, wu_ref, wd_ref, op_ref,
    gog_ref, gig_ref, gval_ref, gop_ref, gg_ref, gu_ref, gd_ref,
    x_ref, cot_ref, og_ref, ig_ref, val_ref,
    pick_ref, scale, tokens, x_send, cot_send, rows, cots, wgu, wd, acc, acc_h, g2, hid, q, r, in_f, in_b, out_f, out_b, fin, grad_gu, grad_d,
    ret_ref, op, cin, cout, halo, mix_t, mcf, col, acc2,
    w_sem, out_sem, sent,
    disp_recv, af_recv, ab_recv, ap_recv, rp_recv, rf_recv, rb_recv, ret_recv,
    halo_recv, mix_recv, mf_recv, mb_recv, mp_recv, col_recv, colp_recv,
    tf_recv, tb_recv, cot_recv, cp_recv,
):
    s = lax.axis_index("sp")
    t = lax.axis_index("tp")
    z, c = t // 2, t % 2
    y = s // 4
    up, down, mate = ((z + 1) % 8) * 2 + c, ((z + 7) % 8) * 2 + c, z * 2 + (1 - c)

    barrier = pltpu.get_barrier_semaphore()

    @pl.loop(1, 16)
    def _(i):
        pl.semaphore_signal(barrier, inc=1, device_id={"sp": (s + i) % 16}, device_id_type=MESH)

    for other in (up, down, mate):
        pl.semaphore_signal(barrier, inc=1, device_id={"tp": other}, device_id_type=MESH)

    tiles = [
        pltpu.make_async_copy(source, held, w_sem.at[4 + i])
        for i, (source, held) in enumerate((
            (ig_hbm, ig_ref), (val_hbm, val_ref), (cot_hbm, cot_ref), (x_hbm, x_ref), (og_hbm, og_ref)
        ))
    ]
    for tile in tiles:
        tile.start()

    weights = [
        pltpu.make_async_copy(wg_ref, wgu.at[:, :, pl.ds(0, 128)], w_sem.at[0]),
        pltpu.make_async_copy(wu_ref, wgu.at[:, :, pl.ds(128, 128)], w_sem.at[1]),
        pltpu.make_async_copy(wd_ref, wd, w_sem.at[2]),
        pltpu.make_async_copy(op_ref, op, w_sem.at[3]),
    ]
    for w in weights:
        w.start()

    expert = lax.broadcasted_iota(jnp.int32, (16, 256), 0)
    named = [ids_ref[i : i + 1, :] == expert for i in range(2)]
    member = jnp.where(named[0] | named[1], 1.0, 0.0)
    weight = jnp.where(named[0], gates_ref[0:1, :], 0.0) + jnp.where(named[1], gates_ref[1:2, :], 0.0)
    row = lax.broadcasted_iota(jnp.int32, (256, 256), 0)
    earlier = jnp.where(row < lax.broadcasted_iota(jnp.int32, (256, 256), 1), 1.0, 0.0).astype(BF16)
    place = jnp.where(member > 0, dot(member.astype(BF16), earlier, NN), -1.0)
    position = lax.broadcasted_iota(jnp.int32, (48, 256), 0).astype(F32)
    for e in range(16):
        hit = place[e : e + 1, :] == position
        pick_ref[e] = jnp.where(hit, 1.0, 0.0).astype(BF16)
        slot_weight = jnp.sum(jnp.where(hit, weight[e : e + 1, :], 0.0), axis=1, keepdims=True)
        scale[e] = jnp.broadcast_to(slot_weight, (48, 128))
    for tile in tiles:
        tile.wait()
    cin[...] = ig_ref[...].astype(F32) * val_ref[...].astype(F32)
    tokens[z] = cot_ref[...].reshape(2, 128, 256)
    acc[...] = jnp.zeros_like(acc)
    acc_h[...] = jnp.zeros_like(acc_h)

    pl.semaphore_wait(barrier, 18)

    def remote(src, dst, send_sem, recv_sem, **where):
        return pltpu.make_async_remote_copy(
            src_ref=src, dst_ref=dst, send_sem=send_sem, recv_sem=recv_sem,
            device_id=where, device_id_type=MESH,
        )

    def part(k):
        return pl.ds(4 * ((y + 4 - k) % 4), 4)

    def token_f(d, k):
        at = tokens.at[(z + 8 - d) % 8, k]
        return remote(at, at, sent.at[TOKEN_RING], tf_recv.at[d, k], tp=up)

    def token_b(d, k):
        at = tokens.at[(z + d) % 8, k]
        return remote(at, at, sent.at[TOKEN_RING], tb_recv.at[d, k], tp=down)

    for k in range(2):
        from_cot = cot_ref.at[pl.ds(128 * k, 128)]
        remote(from_cot, tokens.at[z, k], sent.at[TOKEN_RING], tf_recv.at[0, k], tp=up).start()
        remote(from_cot, tokens.at[z, k], sent.at[TOKEN_RING], tb_recv.at[0, k], tp=down).start()

    def dispatch(peer):
        return remote(x_send.at[peer], rows.at[t, s], sent.at[DISPATCH], disp_recv.at[y], sp=peer)

    own = pltpu.make_async_copy(x_send.at[s], rows.at[t, s], disp_recv.at[y])

    def dispatch_cot(zz, peer):
        return remote(
            cot_send.at[zz, peer], cots.at[zz * 2 + c, s], sent.at[COT], cot_recv.at[zz], sp=peer
        )

    def own_cot(zz):
        return pltpu.make_async_copy(cot_send.at[zz, s], cots.at[zz * 2 + c, s], cot_recv.at[zz])

    def arrived(at, recv_sem):
        remote(at, at, recv_sem, recv_sem, tp=mate).wait_recv()

    def sent_all(at, index):
        remote(at, at, sent.at[index], sent.at[index], tp=mate).wait_send()

    def halo_copies(h):
        return [
            remote(cin.at[pl.ds(248, 8)], halo.at[h, 0], sent.at[HALO + h], halo_recv.at[h, 0], sp=(s + 1) % 16),
            remote(cin.at[pl.ds(0, 8)], halo.at[h, 1], sent.at[HALO + h], halo_recv.at[h, 1], sp=(s + 15) % 16),
        ]

    def neighbours(h):
        for copy in halo_copies(h):
            copy.wait_recv()
        sent_all(halo.at[h], HALO + h)
        array = cin[...]
        first = jnp.where(s > 0, halo[h, 0, 7:8, :], 0.0)
        last = jnp.where(s < 15, halo[h, 1, 0:1, :], 0.0)
        before = jnp.where(row == 0, first, pltpu.roll(array, 1, 0))
        after = jnp.where(row == 255, last, pltpu.roll(array, 255, 0))
        return before, array, after

    for copy in halo_copies(0):
        copy.start()

    def selected(k, table):
        return dot(pick_ref[part(k)].reshape(192, 256), table, NN)

    @pl.loop(0, 4)
    def _(k):
        x_send[part(k)] = selected(k, x_ref[...]).astype(BF16).reshape(4, 48, 256)
        for x in range(4):
            peer = 4 * ((y + 4 - k) % 4) + x

            @pl.when(peer == s)
            def _():
                own.start()

            @pl.when(peer != s)
            def _():
                dispatch(peer).start()

    def send_cot(zz):
        @pl.loop(0, 4)
        def _(k):
            value = selected(k, tokens[zz].reshape(256, 256))
            factor = scale[part(k)].reshape(192, 128)
            cot_send[zz, part(k), :, pl.ds(0, 128)] = (value[:, :128] * factor).astype(BF16).reshape(4, 48, 128)
            cot_send[zz, part(k), :, pl.ds(128, 128)] = (value[:, 128:] * factor).astype(BF16).reshape(4, 48, 128)
            for x in range(4):
                peer = 4 * ((y + 4 - k) % 4) + x

                @pl.when(peer == s)
                def _():
                    own_cot(zz).start()

                @pl.when(peer != s)
                def _():
                    dispatch_cot(zz, peer).start()

    send_cot(z)

    for w in weights:
        w.wait()

    def slice_of(zz, core, k):
        return rows.at[zz * 2 + core, part(k)]

    def along_f(d, k):
        at = slice_of((z + 8 - d) % 8, c, k)
        return remote(at, at, sent.at[ROWS], af_recv.at[d, k], tp=up)

    def along_b(d, k):
        at = slice_of((z + d) % 8, c, k)
        return remote(at, at, sent.at[ROWS], ab_recv.at[d, k], tp=down)

    def to_mate(zz, core, k):
        at = slice_of(zz, core, k)
        return remote(at, at, sent.at[ROWS], ap_recv.at[zz, k], tp=mate)

    def multiply(tt, k):
        pre = dot(rows[tt, part(k)].reshape(192, 256), wgu[tt], NN)
        acc[part(k)] += pre.reshape(4, 48, 256)

    def ring_start(k):
        arrived(slice_of(z, c, k), disp_recv.at[(y + 4 - k) % 4])
        along_f(0, k).start()
        along_b(0, k).start()
        to_mate(z, c, k).start()
        multiply(t, k)

    @pl.loop(1, 5)
    def _(d):
        zf, zb = (z + 8 - d) % 8, (z + d) % 8
        for k in range(2):
            @pl.when((d < 4) | (k == 0))
            def _():
                at = tokens.at[zf, k]
                remote(at, at, sent.at[TOKEN_RING], tf_recv.at[d - 1, k], tp=up).wait_recv()

                @pl.when((d < 3) | ((d == 3) & (k == 0)))
                def _():
                    token_f(d, k).start()

            @pl.when((d < 4) | (k == 1))
            def _():
                at = tokens.at[zb, k]
                remote(at, at, sent.at[TOKEN_RING], tb_recv.at[d - 1, k], tp=down).wait_recv()

                @pl.when((d < 3) | ((d == 3) & (k == 1)))
                def _():
                    token_b(d, k).start()

        ring_start(d - 1)
        send_cot(zf)

        @pl.when(d < 4)
        def _():
            send_cot(zb)

    def cot_mate(zz, core):
        at = cots.at[zz * 2 + core]
        return remote(at, at, sent.at[COT_MATE], cp_recv.at[zz], tp=mate)

    def multiply_cot(tt):
        columns = pl.ds(pl.multiple_of(tt * 256, 256), 256)
        acc_h[...] += dot(cots[tt].reshape(768, 256), wd[:, columns], NT).reshape(16, 48, 128)

    def nth(n):
        return (z + 8 + (1 - 2 * (n % 2)) * ((n + 1) // 2)) % 8

    def cot_own_part(n):
        zz = nth(n)
        arrived(cots.at[zz * 2 + c], cot_recv.at[zz])
        cot_mate(zz, c).start()
        multiply_cot(zz * 2 + c)

    def cot_mate_part(n):
        zz = nth(n)
        cot_mate(zz, 1 - c).wait_recv()
        multiply_cot(zz * 2 + 1 - c)

    def mate_part(zz, k):
        to_mate(zz, 1 - c, k).wait_recv()
        multiply(zz * 2 + 1 - c, k)

    @pl.loop(0, 16)
    def _(i):
        d, k = i // 4 + 1, i % 4
        even = (k % 2) == 0
        zf, zb = (z + 8 - d) % 8, (z + d) % 8

        @pl.when((d < 4) | even)
        def _():
            at = slice_of(zf, c, k)
            remote(at, at, sent.at[ROWS], af_recv.at[d - 1, k], tp=up).wait_recv()

            @pl.when((d < 3) | ((d == 3) & even))
            def _():
                along_f(d, k).start()

            to_mate(zf, c, k).start()

        @pl.when((d < 4) | (~even))
        def _():
            at = slice_of(zb, c, k)
            remote(at, at, sent.at[ROWS], ab_recv.at[d - 1, k], tp=down).wait_recv()

            @pl.when((d < 3) | ((d == 3) & (~even)))
            def _():
                along_b(d, k).start()

        @pl.when((d < 4) | (~even))
        def _():
            to_mate(zb, c, k).start()

        @pl.when((d < 4) | even)
        def _():
            multiply(zf * 2 + c, k)

        @pl.when((d < 4) | (~even))
        def _():
            multiply(zb * 2 + c, k)

        e = i // 4

        @pl.when(e == 0)
        def _():
            mate_part(z, k)

        @pl.when(e > 0)
        def _():
            mate_part((z + 8 - e) % 8, k)
            mate_part((z + e) % 8, k)

        @pl.when((i >= 3) & (i % 2 == 1))
        def _():
            cot_own_part((i - 3) // 2)

        @pl.when((i >= 4) & (i % 2 == 0))
        def _():
            cot_mate_part((i - 4) // 2)

    @pl.loop(0, 4)
    def _(k):
        mate_part((z + 4) % 8, k)

    cot_own_part(7)

    @pl.loop(6, 8)
    def _(n):
        cot_mate_part(n)

    before, here, after = neighbours(0)
    conv = before * taps_ref[0:1, :] + here * taps_ref[1:2, :] + after * taps_ref[2:3, :]
    cout[...] = conv
    mine_t = pl.ds(pl.multiple_of(s * 256, 256), 256)
    mix_t[:, mine_t] = (og_ref[...].astype(F32) * conv).T.astype(BF16)

    @pl.loop(1, 16)
    def _(i):
        remote(
            mix_t.at[:, mine_t], mix_t.at[:, mine_t], sent.at[MIXED], mix_recv.at[0], sp=(s + i) % 16
        ).start()

    def eight(k):
        return pl.ds(8 * k, 8)

    def dots_of(tt, k):
        return dot(g2[eight(k)].reshape(384, 256), wgu[tt], NT)

    def prepare(zz, k):
        value = dots_of(zz * 2 + 1 - c, k)
        q[zz, eight(k)] = value.astype(BF16).reshape(8, 48, 256)
        remote(
            q.at[zz, eight(k)], r.at[zz, eight(k)], sent.at[MATE_SUMS], rp_recv.at[zz, k], tp=mate
        ).start()

    @pl.loop(0, 4)
    def _(k):
        block = acc[pl.ds(4 * k, 4)].reshape(192, 256)
        pre_gate, pre_up = block[:, :128], block[:, 128:]
        grad_hidden = acc_h[pl.ds(4 * k, 4)].reshape(192, 128)
        sig = jax.nn.sigmoid(pre_gate)
        activated = pre_gate * sig
        hid[pl.ds(4 * k, 4)] = (activated * pre_up).astype(BF16).reshape(4, 48, 128)
        grad_gate = (grad_hidden * pre_up * sig * (1.0 + pre_gate * (1.0 - sig))).astype(BF16)
        grad_up = (grad_hidden * activated).astype(BF16)
        g2[pl.ds(4 * k, 4), :, pl.ds(0, 128)] = grad_gate.reshape(4, 48, 128)
        g2[pl.ds(4 * k, 4), :, pl.ds(128, 128)] = grad_up.reshape(4, 48, 128)

        @pl.when(k % 2 == 1)
        def _():
            prepare((z + 4) % 8, k // 2)

    def summed(zz, k):
        at = r.at[zz, eight(k)]
        remote(at, at, sent.at[MATE_SUMS], rp_recv.at[zz, k], tp=mate).wait_recv()
        return dots_of(zz * 2 + c, k) + r[zz, eight(k)].reshape(384, 256).astype(F32)

    def ring_send(h, d, k, incoming, outgoing, recv_sem, to):
        remote(
            outgoing.at[h, d - 1, eight(k)], incoming.at[h, d - 1, eight(k)],
            sent.at[SUMS], recv_sem.at[h, d - 1, k], tp=to,
        ).start()

    def half_of(ref, *index):
        return ref[index].reshape(384, 128).astype(F32)

    def ring_step(d, k, zz, incoming, outgoing, recv_sem, to, starts):
        value = summed(zz, k)
        outgoing[1, d - 1, eight(k)] = value[:, 128:].astype(BF16).reshape(8, 48, 128)

        @pl.when(starts)
        def _():
            outgoing[0, d - 1, eight(k)] = value[:, :128].astype(BF16).reshape(8, 48, 128)

        @pl.when(jnp.logical_not(starts))
        def _():
            arrived(incoming.at[0, d, eight(k)], recv_sem.at[0, d, k])
            both = value[:, :128] + half_of(incoming, 0, d, eight(k))
            outgoing[0, d - 1, eight(k)] = both.astype(BF16).reshape(8, 48, 128)

        ring_send(0, d, k, incoming, outgoing, recv_sem, to)

    def ring_step_2(d, k, incoming, outgoing, recv_sem, to, starts):
        @pl.when(jnp.logical_not(starts))
        def _():
            arrived(incoming.at[1, d, eight(k)], recv_sem.at[1, d, k])
            both = half_of(outgoing, 1, d - 1, eight(k)) + half_of(incoming, 1, d, eight(k))
            outgoing[1, d - 1, eight(k)] = both.astype(BF16).reshape(8, 48, 128)

        ring_send(1, d, k, incoming, outgoing, recv_sem, to)

    def grads(tt):
        x = rows[tt].reshape(768, 256)
        cot = cots[tt].reshape(768, 256)
        grad_gu[tt] = dot(x, g2[...].reshape(768, 256), TN).astype(BF16)
        columns = pl.ds(pl.multiple_of(tt * 256, 256), 256)
        grad_d[:, columns] = dot(hid[...].reshape(768, 128), cot, TN).astype(BF16)
        for copy in outputs(tt):
            copy.start()

    def outputs(tt):
        columns = pl.ds(pl.multiple_of(tt * 256, 256), 256)
        return [
            pltpu.make_async_copy(grad_gu.at[tt, :, pl.ds(0, 128)], gg_ref.at[tt], out_sem.at[0]),
            pltpu.make_async_copy(grad_gu.at[tt, :, pl.ds(128, 128)], gu_ref.at[tt], out_sem.at[1]),
            pltpu.make_async_copy(grad_d.at[:, columns], gd_ref.at[:, columns], out_sem.at[2]),
        ]

    @pl.loop(0, 8)
    def _(i):
        d, k = 4 - i // 2, i % 2
        even = (k % 2) == 0
        zf, zb = (z + d) % 8, (z + 8 - d) % 8

        @pl.when((d < 4) | even)
        def _():
            ring_step(d, k, zf, in_f, out_f, rf_recv, up, (d == 4) | ((d == 3) & (~even)))

        @pl.when((d < 4) | (~even))
        def _():
            ring_step(d, k, zb, in_b, out_b, rb_recv, down, (d == 4) | ((d == 3) & even))

        prepare((z + d - 1) % 8, k)

        @pl.when(d > 1)
        def _():
            prepare((z + 9 - d) % 8, k)

    def giving_back(h, peer):
        return remote(fin.at[h, peer], ret_ref.at[h, s], sent.at[RETURNED], ret_recv.at[h], sp=peer)

    def mine(h):
        return pltpu.make_async_copy(fin.at[h, s], ret_ref.at[h, s], ret_recv.at[h])

    def finish(h, k, value):
        for incoming, recv_sem in ((in_f, rf_recv), (in_b, rb_recv)):
            arrived(incoming.at[h, 0, eight(k)], recv_sem.at[h, 0, k])
            value = value + half_of(incoming, h, 0, eight(k))
        fin[h, eight(k)] = value.astype(BF16).reshape(8, 48, 128)
        for x in range(8):
            peer = 8 * k + x

            @pl.when(peer == s)
            def _():
                mine(h).start()

            @pl.when(peer != s)
            def _():
                giving_back(h, peer).start()

    def mc_f(h, d, k):
        at = mcf.at[h, ((z + 8 - d) % 8) * 2 + c, pl.ds(2 * k, 2)]
        return remote(at, at, sent.at[MIXER], mf_recv.at[h, d, k], tp=up)

    def mc_b(h, d, k):
        at = mcf.at[h, ((z + d) % 8) * 2 + c, pl.ds(2 * k, 2)]
        return remote(at, at, sent.at[MIXER], mb_recv.at[h, d, k], tp=down)

    def mc_mate(h, zz, core):
        at = mcf.at[h, zz * 2 + core]
        return remote(at, at, sent.at[MIXER], mp_recv.at[h, zz], tp=mate)

    tokens_half = pl.ds(2 * c, 2)

    def send_column(h, tt):
        @pl.when(tt == s)
        def _():
            pltpu.make_async_copy(
                mcf.at[h, s, tokens_half], col.at[h, s, tokens_half], col_recv.at[h, y]
            ).start()

        @pl.when(tt != s)
        def _():
            remote(
                mcf.at[h, tt, tokens_half], col.at[h, s, tokens_half],
                sent.at[COLUMN], col_recv.at[h, y], sp=tt,
            ).start()

    def use(tt):
        tile = jnp.concatenate([mcf[h, tt].reshape(256, 128) for h in range(2)], axis=1)
        acc2[...] += dot(tile, op[tt], NN)

    def from_mate(h, zz):
        mc_mate(h, zz, 1 - c).wait_recv()
        send_column(h, zz * 2 + 1 - c)

    def mixer_start(h):
        arrived(ret_ref.at[h], ret_recv.at[h])
        moe_grad = dot(pick_ref[...].reshape(768, 256), ret_ref[h].reshape(768, 128), TN)
        mixer = cot_ref[:, pl.ds(128 * h, 128)].astype(F32) + moe_grad
        mcf[h, t] = mixer.astype(BF16).reshape(4, 64, 128)
        for k in range(2):
            mc_f(h, 0, k).start()
            mc_b(h, 0, k).start()
        mc_mate(h, z, c).start()
        send_column(h, t)

    def mixer_step(h, d, compute):
        zf, zb = (z + 8 - d) % 8, (z + d) % 8
        for k in range(2):
            @pl.when((d < 4) | (k == 0))
            def _():
                arrived(mcf.at[h, zf * 2 + c, pl.ds(2 * k, 2)], mf_recv.at[h, d - 1, k])

                @pl.when((d < 3) | ((d == 3) & (k == 0)))
                def _():
                    mc_f(h, d, k).start()

            @pl.when((d < 4) | (k == 1))
            def _():
                arrived(mcf.at[h, zb * 2 + c, pl.ds(2 * k, 2)], mb_recv.at[h, d - 1, k])

                @pl.when((d < 3) | ((d == 3) & (k == 1)))
                def _():
                    mc_b(h, d, k).start()

        mc_mate(h, zf, c).start()
        send_column(h, zf * 2 + c)

        @pl.when(d < 4)
        def _():
            mc_mate(h, zb, c).start()
            send_column(h, zb * 2 + c)

        lf, lb = (zf + 1) % 8, (zb + 7) % 8
        from_mate(h, lf)
        if compute:
            for core in range(2):
                use(lf * 2 + core)

        @pl.when(d > 1)
        def _():
            from_mate(h, lb)
            if compute:
                for core in range(2):
                    use(lb * 2 + core)

    @pl.loop(0, 8)
    def _(i):
        d, k = 4 - i // 2, i % 2
        even = k == 0

        @pl.when((d < 4) | even)
        def _():
            ring_step_2(d, k, in_f, out_f, rf_recv, up, (d == 4) | ((d == 3) & (~even)))

        @pl.when((d < 4) | (~even))
        def _():
            ring_step_2(d, k, in_b, out_b, rb_recv, down, (d == 4) | ((d == 3) & even))

        @pl.when((i >= 1) & (i < 3))
        def _():
            value = summed(z, i - 1)
            fin[1, eight(i - 1)] = value[:, 128:].astype(BF16).reshape(8, 48, 128)
            finish(0, i - 1, value[:, :128])

        @pl.when(i != 1)
        def _():
            grads(i)

    acc2[...] = jnp.zeros_like(acc2)
    finish(1, 0, half_of(fin, 1, eight(0)))
    mixer_start(0)
    finish(1, 1, half_of(fin, 1, eight(1)))
    grads(1)

    @pl.loop(1, 3)
    def _(d):
        mixer_step(0, d, False)
        grads(7 + d)

    mixer_start(1)

    @pl.loop(3, 5)
    def _(d):
        mixer_step(0, d, False)
        mixer_step(1, d - 2, True)

    from_mate(0, (z + 4) % 8)

    @pl.loop(3, 5)
    def _(d):
        mixer_step(1, d, True)
        grads(7 + d)

    from_mate(1, (z + 4) % 8)
    for core in range(2):
        use(((z + 4) % 8) * 2 + core)

    grad_mixed = acc2[...]
    gog_ref[...] = (grad_mixed * cout[...]).astype(BF16)
    cin[...] = grad_mixed * og_ref[...].astype(F32)
    for copy in halo_copies(1):
        copy.start()

    @pl.loop(12, 16)
    def _(i):
        grads(i)

    def column_mate(h, k, core):
        at = col.at[h, part(k), pl.ds(2 * core, 2)]
        return remote(at, at, sent.at[COLUMN_MATE], colp_recv.at[h, (y + 4 - k) % 4], tp=mate)

    for h in range(2):
        for k in range(4):
            arrived(col.at[h, part(k), tokens_half], col_recv.at[h, (y + 4 - k) % 4])
            column_mate(h, k, c).start()
    arrived(mix_t.at[:, pl.ds(0, 15 * 256)], mix_recv.at[0])
    for h in range(2):
        for k in range(4):
            column_mate(h, k, 1 - c).wait_recv()
    columns = jnp.concatenate([col[h].reshape(4096, 128) for h in range(2)], axis=1)
    gop_ref[...] = dot(mix_t[...], columns, NN).T

    before, here, after = neighbours(1)
    grad_in = after * taps_ref[0:1, :] + here * taps_ref[1:2, :] + before * taps_ref[2:3, :]
    gig_ref[...] = (grad_in * val_ref[...].astype(F32)).astype(BF16)
    gval_ref[...] = (grad_in * ig_ref[...].astype(F32)).astype(BF16)

    sent_all(rows.at[0, pl.ds(0, 15)], DISPATCH)
    sent_all(rows.at[pl.ds(0, 15)], ROWS)
    sent_all(cots.at[pl.ds(0, 8), pl.ds(0, 15)], COT)
    sent_all(cots.at[pl.ds(0, 8)], COT_MATE)
    sent_all(tokens.at[pl.ds(0, 7)], TOKEN_RING)
    sent_all(mix_t.at[:, pl.ds(0, 15 * 256)], MIXED)
    sent_all(q, MATE_SUMS)
    sent_all(q.at[pl.ds(0, 7)], SUMS)
    sent_all(fin.at[:, pl.ds(0, 15)], RETURNED)
    sent_all(mcf.at[:, pl.ds(0, 15)], MIXER)
    sent_all(mcf.at[:, pl.ds(0, 15), pl.ds(0, 2)], COLUMN)
    sent_all(col.at[:, :, pl.ds(0, 2)], COLUMN_MATE)
    pltpu.make_async_copy(grad_gu.at[:, :, pl.ds(0, 128)], gg_ref, out_sem.at[0]).wait()
    pltpu.make_async_copy(grad_gu.at[:, :, pl.ds(128, 128)], gu_ref, out_sem.at[1]).wait()
    pltpu.make_async_copy(grad_d, gd_ref, out_sem.at[2]).wait()


def mixer_and_experts(*operands):
    vm = lambda shape, dtype: pltpu.VMEM(shape, dtype)
    dma = lambda *shape: pltpu.SemaphoreType.DMA(shape)
    any_ = pl.BlockSpec(memory_space=pl.ANY)
    vmem = pl.BlockSpec(memory_space=pltpu.VMEM)
    tile = jax.ShapeDtypeStruct((256, 256), BF16)
    return pl.pallas_call(
        moe_kernel,
        out_shape=(
            tile, tile, tile,
            jax.ShapeDtypeStruct((256, 256), F32),
            jax.ShapeDtypeStruct((16, 256, 128), BF16),
            jax.ShapeDtypeStruct((16, 256, 128), BF16),
            jax.ShapeDtypeStruct((128, 4096), BF16),
        ),
        in_specs=[vmem] * 3 + [any_] * 9,
        out_specs=(vmem,) * 4 + (any_,) * 3,
        scratch_shapes=[
            vm((256, 256), BF16),
            vm((256, 256), BF16),
            vm((256, 256), BF16),
            vm((256, 256), BF16),
            vm((256, 256), BF16),
            vm((16, 48, 256), BF16),
            vm((16, 48, 128), F32),
            vm((8, 2, 128, 256), BF16),
            vm((16, 48, 256), BF16),
            vm((8, 16, 48, 256), BF16),
            vm((16, 16, 48, 256), BF16),
            vm((16, 16, 48, 256), BF16),
            vm((16, 256, 256), BF16),
            vm((128, 4096), BF16),
            vm((16, 48, 256), F32),
            vm((16, 48, 128), F32),
            vm((16, 48, 256), BF16),
            vm((16, 48, 128), BF16),
            vm((8, 16, 48, 256), BF16),
            vm((8, 16, 48, 256), BF16),
            vm((2, 4, 16, 48, 128), BF16),
            vm((2, 4, 16, 48, 128), BF16),
            vm((2, 4, 16, 48, 128), BF16),
            vm((2, 4, 16, 48, 128), BF16),
            vm((2, 16, 48, 128), BF16),
            vm((16, 256, 256), BF16),
            vm((128, 4096), BF16),
            vm((2, 16, 48, 128), BF16),
            vm((16, 256, 256), BF16),
            vm((256, 256), F32),
            vm((256, 256), F32),
            vm((2, 2, 8, 256), F32),
            vm((256, 4096), BF16),
            vm((2, 16, 4, 64, 128), BF16),
            vm((2, 16, 4, 64, 128), BF16),
            vm((256, 256), F32),
            dma(9), dma(3), dma(14),
            dma(4), dma(4, 4), dma(4, 4), dma(8, 4), dma(8, 2), dma(2, 4, 2), dma(2, 4, 2), dma(2),
            dma(2, 2), dma(1), dma(2, 4, 2), dma(2, 4, 2), dma(2, 8), dma(2, 4), dma(2, 4),
            dma(4, 2), dma(4, 2), dma(8), dma(8),
        ],
        compiler_params=pltpu.CompilerParams(
            collective_id=1, has_side_effects=True, vmem_limit_bytes=67043328
        ),
        cost_estimate=pl.CostEstimate(flops=8_000_000_000, bytes_accessed=20_000_000, transcendentals=100_000),
        name="mixer_and_experts",
    )(*operands)


def write_out(*refs):
    sources, targets, held = refs[:7], refs[7:14], refs[14:21]
    wide, in_sem, out_sem = refs[21:24], refs[24], refs[25]
    steps = []
    for i, ref in enumerate(sources):
        pieces = 4 if i < 3 else 1
        size = ref.shape[0] // pieces
        staged = wide[i] if i < 3 else held[i]
        for p in range(pieces):
            at = pl.ds(p * size, size)
            n = len(steps)
            steps.append((
                i, at,
                pltpu.make_async_copy(ref.at[at], held[i].at[at], in_sem.at[n]),
                pltpu.make_async_copy(staged.at[at], targets[i].at[at], out_sem.at[n]),
            ))
    for _, _, fetch, _ in steps:
        fetch.start()
    for i, at, fetch, store in steps:
        fetch.wait()
        if i < 3:
            wide[i][at, :] = held[i][at, :].astype(F32)
        store.start()
    for _, _, _, store in steps:
        store.wait()


def written(*arrays):
    any_ = pl.BlockSpec(memory_space=pl.ANY)
    shapes = [jax.ShapeDtypeStruct(a.shape, F32 if i < 3 else a.dtype) for i, a in enumerate(arrays)]
    return pl.pallas_call(
        write_out,
        out_shape=tuple(shapes),
        in_specs=[any_] * len(shapes),
        out_specs=(any_,) * len(shapes),
        scratch_shapes=[pltpu.VMEM(a.shape, a.dtype) for a in arrays]
        + [pltpu.VMEM(a.shape, F32) for a in arrays[:3]]
        + [pltpu.SemaphoreType.DMA((16,)), pltpu.SemaphoreType.DMA((16,))],
        compiler_params=pltpu.CompilerParams(vmem_limit_bytes=67043328),
        name="write_out",
    )(*arrays)


def body(moe_input, out_gate, in_gate, values, conv_taps, out_proj, route_ids, route_gates, expert_gate, expert_up, expert_down, cotangent):
    gog, gig, gval, gop, gg, gu, gd = mixer_and_experts(
        route_ids.T, route_gates.T, conv_taps, moe_input, cotangent, out_gate, in_gate, values,
        expert_gate.reshape(16, 256, 128),
        expert_up.reshape(16, 256, 128),
        expert_down.reshape(128, 4096),
        out_proj.reshape(16, 256, 256),
    )
    gg, gu, gd, gop, gog, gig, gval = written(
        gg.reshape(4096, 128), gu.reshape(4096, 128), gd, gop, gog, gig, gval
    )
    return (gog, gig, gval, gop, gg.reshape(1, 4096, 128), gu.reshape(1, 4096, 128), gd.reshape(1, 128, 4096))


def solution(mesh):
    in_specs = (
        P("sp", "tp"), P("sp", "tp"), P("sp", "tp"), P("sp", "tp"), P(None, "tp"), P(None, "tp"),
        P("sp", None), P("sp", None),
        P("sp", None, "tp"), P("sp", None, "tp"), P("sp", "tp", None), P("sp", "tp"),
    )
    out_specs = (
        P("sp", "tp"), P("sp", "tp"), P("sp", "tp"), P("sp", "tp"),
        P("sp", None, "tp"), P("sp", None, "tp"), P("sp", "tp", None),
    )
    return jax.shard_map(body, mesh=mesh, in_specs=in_specs, out_specs=out_specs, check_vma=False)
```

```python
import functools
import jax
import jax.numpy as jnp
from jax import lax
from jax.experimental import pallas as pl
from jax.experimental.pallas import tpu as pltpu
from jax.sharding import PartitionSpec as P

F32 = jnp.float32
BF16 = jnp.bfloat16
MESH = pl.DeviceIdType.MESH
NT = (((1,), (1,)), ((), ()))
TN = (((0,), (0,)), ((), ()))
NN = (((1,), (0,)), ((), ()))


def dot(a, b, dims):
    return lax.dot_general(a, b, dims, preferred_element_type=F32)


(DISPATCH, ROWS, COT, COT_MATE, TOKEN_RING, HALO, HALO_BACK, MIXED, MATE_SUMS, SUMS, RETURNED,
 MIXER, COLUMN, COLUMN_MATE) = range(14)


def moe_kernel(
    ids_ref, gates_ref, taps_ref, x_hbm, cot_hbm, og_hbm, ig_hbm, val_hbm, wg_ref, wu_ref, wd_ref, op_ref,
    gog_hbm, gig_hbm, gval_hbm, gop_hbm, gg_ref, gu_ref, gd_ref,
    gog_ref, gig_ref, gval_ref, gop_ref,
    x_ref, cot_ref, og_ref, ig_ref, val_ref,
    pick_ref, scale, tokens, x_send, cot_send, rows, cots, wgu, wd, acc, acc_h, g2, hid, q, r, in_f, in_b, out_f, out_b, fin, grad_gu, grad_d,
    ret_ref, op, cin, cout, halo, mix_t, mcf, col,
    w_sem, out_sem, sent,
    disp_recv, af_recv, ab_recv, ap_recv, rp_recv, rf_recv, rb_recv, ret_recv,
    halo_recv, mix_recv, mf_recv, mb_recv, mp_recv, col_recv, colp_recv,
    tf_recv, tb_recv, cot_recv, cp_recv,
):
    s = lax.axis_index("sp")
    t = lax.axis_index("tp")
    z, c = t // 2, t % 2
    y = s // 4
    up, down, mate = ((z + 1) % 8) * 2 + c, ((z + 7) % 8) * 2 + c, z * 2 + (1 - c)

    barrier = pltpu.get_barrier_semaphore()

    @pl.loop(1, 16)
    def _(i):
        pl.semaphore_signal(barrier, inc=1, device_id={"sp": (s + i) % 16}, device_id_type=MESH)

    for other in (up, down, mate):
        pl.semaphore_signal(barrier, inc=1, device_id={"tp": other}, device_id_type=MESH)

    tiles = [
        pltpu.make_async_copy(source, held, w_sem.at[4 + i])
        for i, (source, held) in enumerate((
            (ig_hbm, ig_ref), (val_hbm, val_ref), (cot_hbm, cot_ref), (x_hbm, x_ref), (og_hbm, og_ref)
        ))
    ]
    for tile in tiles:
        tile.start()

    weights = [
        pltpu.make_async_copy(wg_ref, wgu.at[:, :, pl.ds(0, 128)], w_sem.at[0]),
        pltpu.make_async_copy(wu_ref, wgu.at[:, :, pl.ds(128, 128)], w_sem.at[1]),
        pltpu.make_async_copy(wd_ref, wd, w_sem.at[2]),
        pltpu.make_async_copy(op_ref, op, w_sem.at[3]),
    ]
    for w in weights:
        w.start()

    expert = lax.broadcasted_iota(jnp.int32, (16, 256), 0)
    named = [ids_ref[i : i + 1, :] == expert for i in range(2)]
    member = jnp.where(named[0] | named[1], 1.0, 0.0)
    weight = jnp.where(named[0], gates_ref[0:1, :], 0.0) + jnp.where(named[1], gates_ref[1:2, :], 0.0)
    row = lax.broadcasted_iota(jnp.int32, (256, 256), 0)
    earlier = jnp.where(row < lax.broadcasted_iota(jnp.int32, (256, 256), 1), 1.0, 0.0).astype(BF16)
    place = jnp.where(member > 0, dot(member.astype(BF16), earlier, NN), -1.0)
    position = lax.broadcasted_iota(jnp.int32, (48, 256), 0).astype(F32)
    for e in range(16):
        hit = place[e : e + 1, :] == position
        pick_ref[e] = jnp.where(hit, 1.0, 0.0).astype(BF16)
        slot_weight = jnp.sum(jnp.where(hit, weight[e : e + 1, :], 0.0), axis=1, keepdims=True)
        scale[e] = jnp.broadcast_to(slot_weight, (48, 128))
    for tile in tiles:
        tile.wait()
    cin[...] = ig_ref[...].astype(F32) * val_ref[...].astype(F32)
    tokens[z] = cot_ref[...].reshape(2, 128, 256)
    acc[...] = jnp.zeros_like(acc)
    acc_h[...] = jnp.zeros_like(acc_h)

    pl.semaphore_wait(barrier, 18)

    def remote(src, dst, send_sem, recv_sem, **where):
        return pltpu.make_async_remote_copy(
            src_ref=src, dst_ref=dst, send_sem=send_sem, recv_sem=recv_sem,
            device_id=where, device_id_type=MESH,
        )

    def part(k):
        return pl.ds(4 * ((y + 4 - k) % 4), 4)

    def token_f(d, k):
        at = tokens.at[(z + 8 - d) % 8, k]
        return remote(at, at, sent.at[TOKEN_RING], tf_recv.at[d, k], tp=up)

    def token_b(d, k):
        at = tokens.at[(z + d) % 8, k]
        return remote(at, at, sent.at[TOKEN_RING], tb_recv.at[d, k], tp=down)

    for k in range(2):
        from_cot = cot_ref.at[pl.ds(128 * k, 128)]
        remote(from_cot, tokens.at[z, k], sent.at[TOKEN_RING], tf_recv.at[0, k], tp=up).start()
        remote(from_cot, tokens.at[z, k], sent.at[TOKEN_RING], tb_recv.at[0, k], tp=down).start()

    def dispatch(peer):
        return remote(x_send.at[peer], rows.at[t, s], sent.at[DISPATCH], disp_recv.at[y], sp=peer)

    own = pltpu.make_async_copy(x_send.at[s], rows.at[t, s], disp_recv.at[y])

    def dispatch_cot(zz, peer):
        return remote(
            cot_send.at[zz, peer], cots.at[zz * 2 + c, s], sent.at[COT], cot_recv.at[zz], sp=peer
        )

    def own_cot(zz):
        return pltpu.make_async_copy(cot_send.at[zz, s], cots.at[zz * 2 + c, s], cot_recv.at[zz])

    def arrived(at, recv_sem):
        remote(at, at, recv_sem, recv_sem, tp=mate).wait_recv()

    def sent_all(at, index):
        remote(at, at, sent.at[index], sent.at[index], tp=mate).wait_send()

    def halo_copies(h):
        return [
            remote(cin.at[pl.ds(248, 8)], halo.at[h, 0], sent.at[HALO + h], halo_recv.at[h, 0], sp=(s + 1) % 16),
            remote(cin.at[pl.ds(0, 8)], halo.at[h, 1], sent.at[HALO + h], halo_recv.at[h, 1], sp=(s + 15) % 16),
        ]

    def neighbours(h):
        for copy in halo_copies(h):
            copy.wait_recv()
        sent_all(halo.at[h], HALO + h)
        array = cin[...]
        first = jnp.where(s > 0, halo[h, 0, 7:8, :], 0.0)
        last = jnp.where(s < 15, halo[h, 1, 0:1, :], 0.0)
        before = jnp.where(row == 0, first, pltpu.roll(array, 1, 0))
        after = jnp.where(row == 255, last, pltpu.roll(array, 255, 0))
        return before, array, after

    for copy in halo_copies(0):
        copy.start()

    def selected(k, table):
        return dot(pick_ref[part(k)].reshape(192, 256), table, NN)

    @pl.loop(0, 4)
    def _(k):
        x_send[part(k)] = selected(k, x_ref[...]).astype(BF16).reshape(4, 48, 256)
        for x in range(4):
            peer = 4 * ((y + 4 - k) % 4) + x

            @pl.when(peer == s)
            def _():
                own.start()

            @pl.when(peer != s)
            def _():
                dispatch(peer).start()

    def send_cot(zz):
        @pl.loop(0, 4)
        def _(k):
            value = selected(k, tokens[zz].reshape(256, 256))
            factor = scale[part(k)].reshape(192, 128)
            cot_send[zz, part(k), :, pl.ds(0, 128)] = (value[:, :128] * factor).astype(BF16).reshape(4, 48, 128)
            cot_send[zz, part(k), :, pl.ds(128, 128)] = (value[:, 128:] * factor).astype(BF16).reshape(4, 48, 128)
            for x in range(4):
                peer = 4 * ((y + 4 - k) % 4) + x

                @pl.when(peer == s)
                def _():
                    own_cot(zz).start()

                @pl.when(peer != s)
                def _():
                    dispatch_cot(zz, peer).start()

    send_cot(z)

    for w in weights:
        w.wait()

    def slice_of(zz, core, k):
        return rows.at[zz * 2 + core, part(k)]

    def along_f(d, k):
        at = slice_of((z + 8 - d) % 8, c, k)
        return remote(at, at, sent.at[ROWS], af_recv.at[d, k], tp=up)

    def along_b(d, k):
        at = slice_of((z + d) % 8, c, k)
        return remote(at, at, sent.at[ROWS], ab_recv.at[d, k], tp=down)

    def to_mate(zz, core, k):
        at = slice_of(zz, core, k)
        return remote(at, at, sent.at[ROWS], ap_recv.at[zz], tp=mate)

    def multiply(tt):
        acc[...] += dot(rows[tt].reshape(768, 256), wgu[tt], NN).reshape(16, 48, 256)

    def ring_start(k):
        arrived(slice_of(z, c, k), disp_recv.at[(y + 4 - k) % 4])
        along_f(0, k).start()
        along_b(0, k).start()
        to_mate(z, c, k).start()

    @pl.loop(1, 5)
    def _(d):
        zf, zb = (z + 8 - d) % 8, (z + d) % 8
        for k in range(2):
            @pl.when((d < 4) | (k == 0))
            def _():
                at = tokens.at[zf, k]
                remote(at, at, sent.at[TOKEN_RING], tf_recv.at[d - 1, k], tp=up).wait_recv()

                @pl.when((d < 3) | ((d == 3) & (k == 0)))
                def _():
                    token_f(d, k).start()

            @pl.when((d < 4) | (k == 1))
            def _():
                at = tokens.at[zb, k]
                remote(at, at, sent.at[TOKEN_RING], tb_recv.at[d - 1, k], tp=down).wait_recv()

                @pl.when((d < 3) | ((d == 3) & (k == 1)))
                def _():
                    token_b(d, k).start()

        ring_start(d - 1)
        send_cot(zf)

        @pl.when(d < 4)
        def _():
            send_cot(zb)

    def cot_mate(zz, core):
        at = cots.at[zz * 2 + core]
        return remote(at, at, sent.at[COT_MATE], cp_recv.at[zz], tp=mate)

    def multiply_cot(tt):
        columns = pl.ds(pl.multiple_of(tt * 256, 256), 256)
        acc_h[...] += dot(cots[tt].reshape(768, 256), wd[:, columns], NT).reshape(16, 48, 128)

    def nth(n):
        return (z + 8 + (1 - 2 * (n % 2)) * ((n + 1) // 2)) % 8

    def cot_own_part(n):
        zz = nth(n)
        arrived(cots.at[zz * 2 + c], cot_recv.at[zz])
        cot_mate(zz, c).start()
        multiply_cot(zz * 2 + c)

    def cot_mate_part(n):
        zz = nth(n)
        cot_mate(zz, 1 - c).wait_recv()
        multiply_cot(zz * 2 + 1 - c)

    def mate_part(zz):
        arrived(rows.at[zz * 2 + 1 - c], ap_recv.at[zz])
        multiply(zz * 2 + 1 - c)

    @pl.loop(0, 16)
    def _(i):
        d, k = i // 4 + 1, i % 4
        even = (k % 2) == 0
        zf, zb = (z + 8 - d) % 8, (z + d) % 8

        @pl.when((d < 4) | even)
        def _():
            at = slice_of(zf, c, k)
            remote(at, at, sent.at[ROWS], af_recv.at[d - 1, k], tp=up).wait_recv()

            @pl.when((d < 3) | ((d == 3) & even))
            def _():
                along_f(d, k).start()

            to_mate(zf, c, k).start()

        @pl.when((d < 4) | (~even))
        def _():
            at = slice_of(zb, c, k)
            remote(at, at, sent.at[ROWS], ab_recv.at[d - 1, k], tp=down).wait_recv()

            @pl.when((d < 3) | ((d == 3) & (~even)))
            def _():
                along_b(d, k).start()

        @pl.when((d < 4) | (~even))
        def _():
            to_mate(zb, c, k).start()

        last_f, last_b = (zf + 1) % 8, (zb + 7) % 8

        @pl.when(k == 0)
        def _():
            multiply(last_f * 2 + c)

        @pl.when((k == 1) & (d > 1))
        def _():
            multiply(last_b * 2 + c)

        @pl.when(k == 2)
        def _():
            mate_part(last_f)

        @pl.when((k == 3) & (d > 1))
        def _():
            mate_part(last_b)

        @pl.when((i >= 3) & (i % 2 == 1))
        def _():
            cot_own_part((i - 3) // 2)

        @pl.when((i >= 6) & (i % 2 == 0))
        def _():
            cot_mate_part((i - 6) // 2)

    cot_own_part(7)
    multiply(((z + 4) % 8) * 2 + c)
    mate_part((z + 4) % 8)

    @pl.loop(5, 8)
    def _(n):
        cot_mate_part(n)

    before, here, after = neighbours(0)
    conv = before * taps_ref[0:1, :] + here * taps_ref[1:2, :] + after * taps_ref[2:3, :]
    cout[...] = conv
    mine_t = pl.ds(pl.multiple_of(s * 256, 256), 256)
    mix_t[:, mine_t] = (og_ref[...].astype(F32) * conv).T.astype(BF16)

    @pl.loop(1, 16)
    def _(i):
        remote(
            mix_t.at[:, mine_t], mix_t.at[:, mine_t], sent.at[MIXED], mix_recv.at[0], sp=(s + i) % 16
        ).start()

    def eight(k):
        return pl.ds(8 * k, 8)

    def dots_of(tt, k):
        return dot(g2[eight(k)].reshape(384, 256), wgu[tt], NT)

    def prepare(zz, k):
        value = dots_of(zz * 2 + 1 - c, k)
        q[zz, eight(k)] = value.astype(BF16).reshape(8, 48, 256)
        remote(
            q.at[zz, eight(k)], r.at[zz, eight(k)], sent.at[MATE_SUMS], rp_recv.at[zz, k], tp=mate
        ).start()

    @pl.loop(0, 4)
    def _(k):
        block = acc[pl.ds(4 * k, 4)].reshape(192, 256)
        pre_gate, pre_up = block[:, :128], block[:, 128:]
        grad_hidden = acc_h[pl.ds(4 * k, 4)].reshape(192, 128)
        sig = jax.nn.sigmoid(pre_gate)
        activated = pre_gate * sig
        hid[pl.ds(4 * k, 4)] = (activated * pre_up).astype(BF16).reshape(4, 48, 128)
        grad_gate = (grad_hidden * pre_up * sig * (1.0 + pre_gate * (1.0 - sig))).astype(BF16)
        grad_up = (grad_hidden * activated).astype(BF16)
        g2[pl.ds(4 * k, 4), :, pl.ds(0, 128)] = grad_gate.reshape(4, 48, 128)
        g2[pl.ds(4 * k, 4), :, pl.ds(128, 128)] = grad_up.reshape(4, 48, 128)

        @pl.when(k % 2 == 1)
        def _():
            prepare((z + 4) % 8, k // 2)

    def summed(zz, k):
        at = r.at[zz, eight(k)]
        remote(at, at, sent.at[MATE_SUMS], rp_recv.at[zz, k], tp=mate).wait_recv()
        return dots_of(zz * 2 + c, k) + r[zz, eight(k)].reshape(384, 256).astype(F32)

    def ring_send(h, d, k, incoming, outgoing, recv_sem, to):
        remote(
            outgoing.at[h, d - 1, eight(k)], incoming.at[h, d - 1, eight(k)],
            sent.at[SUMS], recv_sem.at[h, d - 1, k], tp=to,
        ).start()

    def half_of(ref, *index):
        return ref[index].reshape(384, 128).astype(F32)

    def ring_step(d, k, zz, incoming, outgoing, recv_sem, to, starts):
        value = summed(zz, k)
        outgoing[1, d - 1, eight(k)] = value[:, 128:].astype(BF16).reshape(8, 48, 128)

        @pl.when(starts)
        def _():
            outgoing[0, d - 1, eight(k)] = value[:, :128].astype(BF16).reshape(8, 48, 128)

        @pl.when(jnp.logical_not(starts))
        def _():
            arrived(incoming.at[0, d, eight(k)], recv_sem.at[0, d, k])
            both = value[:, :128] + half_of(incoming, 0, d, eight(k))
            outgoing[0, d - 1, eight(k)] = both.astype(BF16).reshape(8, 48, 128)

        ring_send(0, d, k, incoming, outgoing, recv_sem, to)

    def ring_step_2(d, k, incoming, outgoing, recv_sem, to, starts):
        @pl.when(jnp.logical_not(starts))
        def _():
            arrived(incoming.at[1, d, eight(k)], recv_sem.at[1, d, k])
            both = half_of(outgoing, 1, d - 1, eight(k)) + half_of(incoming, 1, d, eight(k))
            outgoing[1, d - 1, eight(k)] = both.astype(BF16).reshape(8, 48, 128)

        ring_send(1, d, k, incoming, outgoing, recv_sem, to)

    def grads(tt):
        x = rows[tt].reshape(768, 256)
        cot = cots[tt].reshape(768, 256)
        grad_gu[tt] = dot(x, g2[...].reshape(768, 256), TN).astype(BF16)
        columns = pl.ds(pl.multiple_of(tt * 256, 256), 256)
        grad_d[:, columns] = dot(hid[...].reshape(768, 128), cot, TN).astype(BF16)
        for copy in outputs(tt):
            copy.start()

    def outputs(tt):
        columns = pl.ds(pl.multiple_of(tt * 256, 256), 256)
        return [
            pltpu.make_async_copy(grad_gu.at[tt, :, pl.ds(0, 128)], gg_ref.at[tt], out_sem.at[0]),
            pltpu.make_async_copy(grad_gu.at[tt, :, pl.ds(128, 128)], gu_ref.at[tt], out_sem.at[1]),
            pltpu.make_async_copy(grad_d.at[:, columns], gd_ref.at[:, columns], out_sem.at[2]),
        ]

    def giving_back(h, peer):
        return remote(fin.at[h, peer], ret_ref.at[h, s], sent.at[RETURNED], ret_recv.at[h], sp=peer)

    def mine(h):
        return pltpu.make_async_copy(fin.at[h, s], ret_ref.at[h, s], ret_recv.at[h])

    def finish(h, k, value):
        for incoming, recv_sem in ((in_f, rf_recv), (in_b, rb_recv)):
            arrived(incoming.at[h, 0, eight(k)], recv_sem.at[h, 0, k])
            value = value + half_of(incoming, h, 0, eight(k))
        fin[h, eight(k)] = value.astype(BF16).reshape(8, 48, 128)
        for x in range(8):
            peer = 8 * k + x

            @pl.when(peer == s)
            def _():
                mine(h).start()

            @pl.when(peer != s)
            def _():
                giving_back(h, peer).start()

    def mc_f(h, d, k):
        at = mcf.at[h, ((z + 8 - d) % 8) * 2 + c, pl.ds(2 * k, 2)]
        return remote(at, at, sent.at[MIXER], mf_recv.at[h, d, k], tp=up)

    def mc_b(h, d, k):
        at = mcf.at[h, ((z + d) % 8) * 2 + c, pl.ds(2 * k, 2)]
        return remote(at, at, sent.at[MIXER], mb_recv.at[h, d, k], tp=down)

    def mc_mate(h, zz, core):
        at = mcf.at[h, zz * 2 + core]
        return remote(at, at, sent.at[MIXER], mp_recv.at[h, zz], tp=mate)

    tokens_half = pl.ds(2 * c, 2)

    def send_column(h, tt):
        @pl.when(tt == s)
        def _():
            pltpu.make_async_copy(
                mcf.at[h, s, tokens_half], col.at[h, s, tokens_half], col_recv.at[h, y]
            ).start()

        @pl.when(tt != s)
        def _():
            remote(
                mcf.at[h, tt, tokens_half], col.at[h, s, tokens_half],
                sent.at[COLUMN], col_recv.at[h, y], sp=tt,
            ).start()

    def from_mate(h, zz):
        mc_mate(h, zz, 1 - c).wait_recv()
        send_column(h, zz * 2 + 1 - c)

    def mixer_start(h):
        arrived(ret_ref.at[h], ret_recv.at[h])
        moe_grad = dot(pick_ref[...].reshape(768, 256), ret_ref[h].reshape(768, 128), TN)
        mixer = cot_ref[:, pl.ds(128 * h, 128)].astype(F32) + moe_grad
        mcf[h, t] = mixer.astype(BF16).reshape(4, 64, 128)
        for k in range(2):
            mc_f(h, 0, k).start()
            mc_b(h, 0, k).start()
        mc_mate(h, z, c).start()
        send_column(h, t)

    def mixer_step(h, d):
        zf, zb = (z + 8 - d) % 8, (z + d) % 8
        for k in range(2):
            @pl.when((d < 4) | (k == 0))
            def _():
                arrived(mcf.at[h, zf * 2 + c, pl.ds(2 * k, 2)], mf_recv.at[h, d - 1, k])

                @pl.when((d < 3) | ((d == 3) & (k == 0)))
                def _():
                    mc_f(h, d, k).start()

            @pl.when((d < 4) | (k == 1))
            def _():
                arrived(mcf.at[h, zb * 2 + c, pl.ds(2 * k, 2)], mb_recv.at[h, d - 1, k])

                @pl.when((d < 3) | ((d == 3) & (k == 1)))
                def _():
                    mc_b(h, d, k).start()

        mc_mate(h, zf, c).start()
        send_column(h, zf * 2 + c)

        @pl.when(d < 4)
        def _():
            mc_mate(h, zb, c).start()
            send_column(h, zb * 2 + c)

        lf, lb = (zf + 1) % 8, (zb + 7) % 8
        from_mate(h, lf)

        @pl.when(d > 1)
        def _():
            from_mate(h, lb)

    @pl.loop(0, 12)
    def _(i):
        k = i % 2
        even = k == 0

        @pl.when(i < 8)
        def _():
            d = 4 - i // 2
            zf, zb = (z + d) % 8, (z + 8 - d) % 8

            @pl.when((d < 4) | even)
            def _():
                ring_step(d, k, zf, in_f, out_f, rf_recv, up, (d == 4) | ((d == 3) & (~even)))

            @pl.when((d < 4) | (~even))
            def _():
                ring_step(d, k, zb, in_b, out_b, rb_recv, down, (d == 4) | ((d == 3) & even))

            prepare((z + d - 1) % 8, k)

            @pl.when(d > 1)
            def _():
                prepare((z + 9 - d) % 8, k)

        @pl.when(i >= 4)
        def _():
            d = 6 - i // 2

            @pl.when((d < 4) | even)
            def _():
                ring_step_2(d, k, in_f, out_f, rf_recv, up, (d == 4) | ((d == 3) & (~even)))

            @pl.when((d < 4) | (~even))
            def _():
                ring_step_2(d, k, in_b, out_b, rb_recv, down, (d == 4) | ((d == 3) & even))

        @pl.when((i >= 8) & (i < 10))
        def _():
            value = summed(z, k)
            fin[1, eight(k)] = value[:, 128:].astype(BF16).reshape(8, 48, 128)
            finish(0, k, value[:, :128])

        @pl.when(i < 4)
        def _():
            grads(12 + i)

        grads(i)

    finish(1, 0, half_of(fin, 1, eight(0)))
    finish(1, 1, half_of(fin, 1, eight(1)))
    mixer_start(0)
    mixer_step(0, jnp.int32(1))
    mixer_start(1)

    @pl.loop(2, 5)
    def _(d):
        mixer_step(0, d)
        mixer_step(1, d - 1)

    from_mate(0, (z + 4) % 8)
    mixer_step(1, jnp.int32(4))
    from_mate(1, (z + 4) % 8)

    full = jnp.concatenate([mcf[h, tt].reshape(256, 128) for tt in range(16) for h in range(2)], axis=1)
    grad_mixed = dot(full, op[...].reshape(4096, 256), NN)
    gog_ref[...] = (grad_mixed * cout[...]).astype(BF16)
    cin[...] = grad_mixed * og_ref[...].astype(F32)
    for copy in halo_copies(1):
        copy.start()

    def column_mate(h, k, core):
        at = col.at[h, part(k), pl.ds(2 * core, 2)]
        return remote(at, at, sent.at[COLUMN_MATE], colp_recv.at[h, (y + 4 - k) % 4], tp=mate)

    def put(i):
        held, out = ((gog_ref, gog_hbm), (gig_ref, gig_hbm), (gval_ref, gval_hbm))[i]
        return pltpu.make_async_copy(held, out, out_sem.at[3 + i])

    put_sums = pltpu.make_async_copy(gop_ref, gop_hbm, out_sem.at[6])

    put(0).start()
    for h in range(2):
        for k in range(4):
            arrived(col.at[h, part(k), tokens_half], col_recv.at[h, (y + 4 - k) % 4])
            column_mate(h, k, c).start()
        if h == 0:
            before, here, after = neighbours(1)
            grad_in = after * taps_ref[0:1, :] + here * taps_ref[1:2, :] + before * taps_ref[2:3, :]
            gig_ref[...] = (grad_in * val_ref[...].astype(F32)).astype(BF16)
            gval_ref[...] = (grad_in * ig_ref[...].astype(F32)).astype(BF16)
            put(1).start()
            put(2).start()
            arrived(mix_t.at[:, pl.ds(0, 15 * 256)], mix_recv.at[0])
    for h in range(2):
        for k in range(4):
            column_mate(h, k, 1 - c).wait_recv()
    columns = jnp.concatenate([col[h].reshape(4096, 128) for h in range(2)], axis=1)
    gop_ref[...] = dot(mix_t[...], columns, NN).T
    put_sums.start()

    sent_all(rows.at[0, pl.ds(0, 15)], DISPATCH)
    sent_all(rows.at[pl.ds(0, 15)], ROWS)
    sent_all(cots.at[pl.ds(0, 8), pl.ds(0, 15)], COT)
    sent_all(cots.at[pl.ds(0, 8)], COT_MATE)
    sent_all(tokens.at[pl.ds(0, 7)], TOKEN_RING)
    sent_all(mix_t.at[:, pl.ds(0, 15 * 256)], MIXED)
    sent_all(q, MATE_SUMS)
    sent_all(q.at[pl.ds(0, 7)], SUMS)
    sent_all(fin.at[:, pl.ds(0, 15)], RETURNED)
    sent_all(mcf.at[:, pl.ds(0, 15)], MIXER)
    sent_all(mcf.at[:, pl.ds(0, 15), pl.ds(0, 2)], COLUMN)
    sent_all(col.at[:, :, pl.ds(0, 2)], COLUMN_MATE)
    pltpu.make_async_copy(grad_gu.at[:, :, pl.ds(0, 128)], gg_ref, out_sem.at[0]).wait()
    pltpu.make_async_copy(grad_gu.at[:, :, pl.ds(128, 128)], gu_ref, out_sem.at[1]).wait()
    pltpu.make_async_copy(grad_d, gd_ref, out_sem.at[2]).wait()
    for i in range(3):
        put(i).wait()
    put_sums.wait()


def mixer_and_experts(*operands):
    vm = lambda shape, dtype: pltpu.VMEM(shape, dtype)
    dma = lambda *shape: pltpu.SemaphoreType.DMA(shape)
    any_ = pl.BlockSpec(memory_space=pl.ANY)
    vmem = pl.BlockSpec(memory_space=pltpu.VMEM)
    tile = jax.ShapeDtypeStruct((256, 256), BF16)
    return pl.pallas_call(
        moe_kernel,
        out_shape=(
            tile, tile, tile,
            jax.ShapeDtypeStruct((256, 256), F32),
            jax.ShapeDtypeStruct((16, 256, 128), BF16),
            jax.ShapeDtypeStruct((16, 256, 128), BF16),
            jax.ShapeDtypeStruct((128, 4096), BF16),
        ),
        in_specs=[vmem] * 3 + [any_] * 9,
        out_specs=(any_,) * 7,
        scratch_shapes=[
            vm((256, 256), BF16),
            vm((256, 256), BF16),
            vm((256, 256), BF16),
            vm((256, 256), F32),
            vm((256, 256), BF16),
            vm((256, 256), BF16),
            vm((256, 256), BF16),
            vm((256, 256), BF16),
            vm((256, 256), BF16),
            vm((16, 48, 256), BF16),
            vm((16, 48, 128), F32),
            vm((8, 2, 128, 256), BF16),
            vm((16, 48, 256), BF16),
            vm((8, 16, 48, 256), BF16),
            vm((16, 16, 48, 256), BF16),
            vm((16, 16, 48, 256), BF16),
            vm((16, 256, 256), BF16),
            vm((128, 4096), BF16),
            vm((16, 48, 256), F32),
            vm((16, 48, 128), F32),
            vm((16, 48, 256), BF16),
            vm((16, 48, 128), BF16),
            vm((8, 16, 48, 256), BF16),
            vm((8, 16, 48, 256), BF16),
            vm((2, 4, 16, 48, 128), BF16),
            vm((2, 4, 16, 48, 128), BF16),
            vm((2, 4, 16, 48, 128), BF16),
            vm((2, 4, 16, 48, 128), BF16),
            vm((2, 16, 48, 128), BF16),
            vm((16, 256, 256), BF16),
            vm((128, 4096), BF16),
            vm((2, 16, 48, 128), BF16),
            vm((16, 256, 256), BF16),
            vm((256, 256), F32),
            vm((256, 256), F32),
            vm((2, 2, 8, 256), F32),
            vm((256, 4096), BF16),
            vm((2, 16, 4, 64, 128), BF16),
            vm((2, 16, 4, 64, 128), BF16),
            dma(9), dma(7), dma(14),
            dma(4), dma(4, 4), dma(4, 4), dma(8), dma(8, 2), dma(2, 4, 2), dma(2, 4, 2), dma(2),
            dma(2, 2), dma(1), dma(2, 4, 2), dma(2, 4, 2), dma(2, 8), dma(2, 4), dma(2, 4),
            dma(4, 2), dma(4, 2), dma(8), dma(8),
        ],
        compiler_params=pltpu.CompilerParams(
            collective_id=1, has_side_effects=True, vmem_limit_bytes=67043328
        ),
        cost_estimate=pl.CostEstimate(flops=8_000_000_000, bytes_accessed=20_000_000, transcendentals=100_000),
        name="mixer_and_experts",
    )(*operands)


def write_out(*refs):
    sources, targets, held = refs[:7], refs[7:14], refs[14:21]
    wide, in_sem, out_sem = refs[21:24], refs[24], refs[25]
    steps = []
    for i, ref in enumerate(sources):
        pieces = 4 if i < 3 else 1
        size = ref.shape[0] // pieces
        staged = wide[i] if i < 3 else held[i]
        for p in range(pieces):
            at = pl.ds(p * size, size)
            n = len(steps)
            steps.append((
                i, at,
                pltpu.make_async_copy(ref.at[at], held[i].at[at], in_sem.at[n]),
                pltpu.make_async_copy(staged.at[at], targets[i].at[at], out_sem.at[n]),
            ))
    for _, _, fetch, _ in steps:
        fetch.start()
    for i, at, fetch, store in steps:
        fetch.wait()
        if i < 3:
            wide[i][at, :] = held[i][at, :].astype(F32)
        store.start()
    for _, _, _, store in steps:
        store.wait()


def written(*arrays):
    any_ = pl.BlockSpec(memory_space=pl.ANY)
    shapes = [jax.ShapeDtypeStruct(a.shape, F32 if i < 3 else a.dtype) for i, a in enumerate(arrays)]
    return pl.pallas_call(
        write_out,
        out_shape=tuple(shapes),
        in_specs=[any_] * len(shapes),
        out_specs=(any_,) * len(shapes),
        scratch_shapes=[pltpu.VMEM(a.shape, a.dtype) for a in arrays]
        + [pltpu.VMEM(a.shape, F32) for a in arrays[:3]]
        + [pltpu.SemaphoreType.DMA((16,)), pltpu.SemaphoreType.DMA((16,))],
        compiler_params=pltpu.CompilerParams(vmem_limit_bytes=67043328),
        name="write_out",
    )(*arrays)


def body(moe_input, out_gate, in_gate, values, conv_taps, out_proj, route_ids, route_gates, expert_gate, expert_up, expert_down, cotangent):
    gog, gig, gval, gop, gg, gu, gd = mixer_and_experts(
        route_ids.T, route_gates.T, conv_taps, moe_input, cotangent, out_gate, in_gate, values,
        expert_gate.reshape(16, 256, 128),
        expert_up.reshape(16, 256, 128),
        expert_down.reshape(128, 4096),
        out_proj.reshape(16, 256, 256),
    )
    gg, gu, gd, gop, gog, gig, gval = written(
        gg.reshape(4096, 128), gu.reshape(4096, 128), gd, gop, gog, gig, gval
    )
    return (gog, gig, gval, gop, gg.reshape(1, 4096, 128), gu.reshape(1, 4096, 128), gd.reshape(1, 128, 4096))


def solution(mesh):
    in_specs = (
        P("sp", "tp"), P("sp", "tp"), P("sp", "tp"), P("sp", "tp"), P(None, "tp"), P(None, "tp"),
        P("sp", None), P("sp", None),
        P("sp", None, "tp"), P("sp", None, "tp"), P("sp", "tp", None), P("sp", "tp"),
    )
    out_specs = (
        P("sp", "tp"), P("sp", "tp"), P("sp", "tp"), P("sp", "tp"),
        P("sp", None, "tp"), P("sp", None, "tp"), P("sp", "tp", None),
    )
    return jax.shard_map(body, mesh=mesh, in_specs=in_specs, out_specs=out_specs, check_vma=False)
```

```python
import functools
import jax
import jax.numpy as jnp
from jax import lax
from jax.experimental import pallas as pl
from jax.experimental.pallas import tpu as pltpu
from jax.sharding import PartitionSpec as P

F32 = jnp.float32
BF16 = jnp.bfloat16
MESH = pl.DeviceIdType.MESH
NT = (((1,), (1,)), ((), ()))
TN = (((0,), (0,)), ((), ()))
NN = (((1,), (0,)), ((), ()))


def dot(a, b, dims):
    return lax.dot_general(a, b, dims, preferred_element_type=F32)


(DISPATCH, ROWS, COT, COT_MATE, TOKEN_RING, HALO, HALO_BACK, MIXED, MATE_SUMS, SUMS, RETURNED,
 MIXER, COLUMN, COLUMN_MATE) = range(14)


def moe_kernel(
    ids_ref, gates_ref, taps_ref, x_hbm, cot_hbm, og_hbm, ig_hbm, val_hbm, wg_ref, wu_ref, wd_ref, op_ref,
    gog_hbm, gig_hbm, gval_hbm, gop_hbm, gg_ref, gu_ref, gd_ref,
    gog_ref, gig_ref, gval_ref, gop_ref,
    x_ref, cot_ref, og_ref, ig_ref, val_ref,
    pick_ref, scale, tokens, x_send, cot_send, rows, cots, wgu, wd, acc, acc_h, g2, hid, q, r, in_f, in_b, out_f, out_b, fin, grad_gu, grad_d,
    ret_ref, op, cin, cout, halo, mix_t, mcf, col,
    w_sem, out_sem, sent,
    disp_recv, af_recv, ab_recv, ap_recv, rp_recv, rf_recv, rb_recv, ret_recv,
    halo_recv, mix_recv, mf_recv, mb_recv, mp_recv, col_recv, colp_recv,
    tf_recv, tb_recv, cot_recv, cp_recv,
):
    s = lax.axis_index("sp")
    t = lax.axis_index("tp")
    z, c = t // 2, t % 2
    y = s // 4
    up, down, mate = ((z + 1) % 8) * 2 + c, ((z + 7) % 8) * 2 + c, z * 2 + (1 - c)

    barrier = pltpu.get_barrier_semaphore()

    @pl.loop(1, 16)
    def _(i):
        pl.semaphore_signal(barrier, inc=1, device_id={"sp": (s + i) % 16}, device_id_type=MESH)

    for other in (up, down, mate):
        pl.semaphore_signal(barrier, inc=1, device_id={"tp": other}, device_id_type=MESH)

    tiles = [
        pltpu.make_async_copy(source, held, w_sem.at[4 + i])
        for i, (source, held) in enumerate((
            (ig_hbm, ig_ref), (val_hbm, val_ref), (cot_hbm, cot_ref), (x_hbm, x_ref), (og_hbm, og_ref)
        ))
    ]
    for tile in tiles:
        tile.start()

    weights = [
        pltpu.make_async_copy(wg_ref, wgu.at[:, :, pl.ds(0, 128)], w_sem.at[0]),
        pltpu.make_async_copy(wu_ref, wgu.at[:, :, pl.ds(128, 128)], w_sem.at[1]),
        pltpu.make_async_copy(wd_ref, wd, w_sem.at[2]),
        pltpu.make_async_copy(op_ref, op, w_sem.at[3]),
    ]
    for w in weights:
        w.start()

    expert = lax.broadcasted_iota(jnp.int32, (16, 256), 0)
    named = [ids_ref[i : i + 1, :] == expert for i in range(2)]
    member = jnp.where(named[0] | named[1], 1.0, 0.0)
    weight = jnp.where(named[0], gates_ref[0:1, :], 0.0) + jnp.where(named[1], gates_ref[1:2, :], 0.0)
    row = lax.broadcasted_iota(jnp.int32, (256, 256), 0)
    earlier = jnp.where(row < lax.broadcasted_iota(jnp.int32, (256, 256), 1), 1.0, 0.0).astype(BF16)
    place = jnp.where(member > 0, dot(member.astype(BF16), earlier, NN), -1.0)
    position = lax.broadcasted_iota(jnp.int32, (48, 256), 0).astype(F32)
    for e in range(16):
        hit = place[e : e + 1, :] == position
        pick_ref[e] = jnp.where(hit, 1.0, 0.0).astype(BF16)
        slot_weight = jnp.sum(jnp.where(hit, weight[e : e + 1, :], 0.0), axis=1, keepdims=True)
        scale[e] = jnp.broadcast_to(slot_weight, (48, 128))
    for tile in tiles:
        tile.wait()
    cin[...] = ig_ref[...].astype(F32) * val_ref[...].astype(F32)
    tokens[z] = cot_ref[...].reshape(2, 128, 256)
    acc[...] = jnp.zeros_like(acc)
    acc_h[...] = jnp.zeros_like(acc_h)

    pl.semaphore_wait(barrier, 18)

    def remote(src, dst, send_sem, recv_sem, **where):
        return pltpu.make_async_remote_copy(
            src_ref=src, dst_ref=dst, send_sem=send_sem, recv_sem=recv_sem,
            device_id=where, device_id_type=MESH,
        )

    def part(k):
        return pl.ds(4 * ((y + 4 - k) % 4), 4)

    def token_f(d, k):
        at = tokens.at[(z + 8 - d) % 8, k]
        return remote(at, at, sent.at[TOKEN_RING], tf_recv.at[d, k], tp=up)

    def token_b(d, k):
        at = tokens.at[(z + d) % 8, k]
        return remote(at, at, sent.at[TOKEN_RING], tb_recv.at[d, k], tp=down)

    for k in range(2):
        from_cot = cot_ref.at[pl.ds(128 * k, 128)]
        remote(from_cot, tokens.at[z, k], sent.at[TOKEN_RING], tf_recv.at[0, k], tp=up).start()
        remote(from_cot, tokens.at[z, k], sent.at[TOKEN_RING], tb_recv.at[0, k], tp=down).start()

    def dispatch(peer):
        return remote(x_send.at[peer], rows.at[t, s], sent.at[DISPATCH], disp_recv.at[y], sp=peer)

    own = pltpu.make_async_copy(x_send.at[s], rows.at[t, s], disp_recv.at[y])

    def dispatch_cot(zz, peer):
        return remote(
            cot_send.at[zz, peer], cots.at[zz * 2 + c, s], sent.at[COT], cot_recv.at[zz], sp=peer
        )

    def own_cot(zz):
        return pltpu.make_async_copy(cot_send.at[zz, s], cots.at[zz * 2 + c, s], cot_recv.at[zz])

    def arrived(at, recv_sem):
        remote(at, at, recv_sem, recv_sem, tp=mate).wait_recv()

    def sent_all(at, index):
        remote(at, at, sent.at[index], sent.at[index], tp=mate).wait_send()

    def halo_copies(h):
        return [
            remote(cin.at[pl.ds(248, 8)], halo.at[h, 0], sent.at[HALO + h], halo_recv.at[h, 0], sp=(s + 1) % 16),
            remote(cin.at[pl.ds(0, 8)], halo.at[h, 1], sent.at[HALO + h], halo_recv.at[h, 1], sp=(s + 15) % 16),
        ]

    def neighbours(h):
        for copy in halo_copies(h):
            copy.wait_recv()
        sent_all(halo.at[h], HALO + h)
        array = cin[...]
        first = jnp.where(s > 0, halo[h, 0, 7:8, :], 0.0)
        last = jnp.where(s < 15, halo[h, 1, 0:1, :], 0.0)
        before = jnp.where(row == 0, first, pltpu.roll(array, 1, 0))
        after = jnp.where(row == 255, last, pltpu.roll(array, 255, 0))
        return before, array, after

    for copy in halo_copies(0):
        copy.start()

    def selected(k, table):
        return dot(pick_ref[part(k)].reshape(192, 256), table, NN)

    @pl.loop(0, 4)
    def _(k):
        x_send[part(k)] = selected(k, x_ref[...]).astype(BF16).reshape(4, 48, 256)
        for x in range(4):
            peer = 4 * ((y + 4 - k) % 4) + x

            @pl.when(peer == s)
            def _():
                own.start()

            @pl.when(peer != s)
            def _():
                dispatch(peer).start()

    def send_cot(zz):
        @pl.loop(0, 4)
        def _(k):
            value = selected(k, tokens[zz].reshape(256, 256))
            factor = scale[part(k)].reshape(192, 128)
            cot_send[zz, part(k), :, pl.ds(0, 128)] = (value[:, :128] * factor).astype(BF16).reshape(4, 48, 128)
            cot_send[zz, part(k), :, pl.ds(128, 128)] = (value[:, 128:] * factor).astype(BF16).reshape(4, 48, 128)
            for x in range(4):
                peer = 4 * ((y + 4 - k) % 4) + x

                @pl.when(peer == s)
                def _():
                    own_cot(zz).start()

                @pl.when(peer != s)
                def _():
                    dispatch_cot(zz, peer).start()

    send_cot(z)

    for w in weights:
        w.wait()

    def slice_of(zz, core, k):
        return rows.at[zz * 2 + core, part(k)]

    def along_f(d, k):
        at = slice_of((z + 8 - d) % 8, c, k)
        return remote(at, at, sent.at[ROWS], af_recv.at[d, k], tp=up)

    def along_b(d, k):
        at = slice_of((z + d) % 8, c, k)
        return remote(at, at, sent.at[ROWS], ab_recv.at[d, k], tp=down)

    def to_mate(zz, core, k):
        at = slice_of(zz, core, k)
        return remote(at, at, sent.at[ROWS], ap_recv.at[zz], tp=mate)

    def multiply(tt):
        acc[...] += dot(rows[tt].reshape(768, 256), wgu[tt], NN).reshape(16, 48, 256)

    def ring_start(k):
        arrived(slice_of(z, c, k), disp_recv.at[(y + 4 - k) % 4])
        along_f(0, k).start()
        along_b(0, k).start()
        to_mate(z, c, k).start()

    @pl.loop(1, 5)
    def _(d):
        zf, zb = (z + 8 - d) % 8, (z + d) % 8
        for k in range(2):
            @pl.when((d < 4) | (k == 0))
            def _():
                at = tokens.at[zf, k]
                remote(at, at, sent.at[TOKEN_RING], tf_recv.at[d - 1, k], tp=up).wait_recv()

                @pl.when((d < 3) | ((d == 3) & (k == 0)))
                def _():
                    token_f(d, k).start()

            @pl.when((d < 4) | (k == 1))
            def _():
                at = tokens.at[zb, k]
                remote(at, at, sent.at[TOKEN_RING], tb_recv.at[d - 1, k], tp=down).wait_recv()

                @pl.when((d < 3) | ((d == 3) & (k == 1)))
                def _():
                    token_b(d, k).start()

        ring_start(d - 1)
        send_cot(zf)

        @pl.when(d < 4)
        def _():
            send_cot(zb)

    def cot_mate(zz, core):
        at = cots.at[zz * 2 + core]
        return remote(at, at, sent.at[COT_MATE], cp_recv.at[zz], tp=mate)

    def multiply_cot(tt):
        columns = pl.ds(pl.multiple_of(tt * 256, 256), 256)
        acc_h[...] += dot(cots[tt].reshape(768, 256), wd[:, columns], NT).reshape(16, 48, 128)

    def nth(n):
        return (z + 8 + (1 - 2 * (n % 2)) * ((n + 1) // 2)) % 8

    def cot_own_part(n):
        zz = nth(n)
        arrived(cots.at[zz * 2 + c], cot_recv.at[zz])
        cot_mate(zz, c).start()
        multiply_cot(zz * 2 + c)

    def cot_mate_part(n):
        zz = nth(n)
        cot_mate(zz, 1 - c).wait_recv()
        multiply_cot(zz * 2 + 1 - c)

    def mate_part(zz):
        arrived(rows.at[zz * 2 + 1 - c], ap_recv.at[zz])
        multiply(zz * 2 + 1 - c)

    @pl.loop(0, 16)
    def _(i):
        d, k = i // 4 + 1, i % 4
        even = (k % 2) == 0
        zf, zb = (z + 8 - d) % 8, (z + d) % 8

        @pl.when((d < 4) | even)
        def _():
            at = slice_of(zf, c, k)
            remote(at, at, sent.at[ROWS], af_recv.at[d - 1, k], tp=up).wait_recv()

            @pl.when((d < 3) | ((d == 3) & even))
            def _():
                along_f(d, k).start()

            to_mate(zf, c, k).start()

        @pl.when((d < 4) | (~even))
        def _():
            at = slice_of(zb, c, k)
            remote(at, at, sent.at[ROWS], ab_recv.at[d - 1, k], tp=down).wait_recv()

            @pl.when((d < 3) | ((d == 3) & (~even)))
            def _():
                along_b(d, k).start()

        @pl.when((d < 4) | (~even))
        def _():
            to_mate(zb, c, k).start()

        last_f, last_b = (zf + 1) % 8, (zb + 7) % 8

        @pl.when(k == 0)
        def _():
            multiply(last_f * 2 + c)

        @pl.when((k == 1) & (d > 1))
        def _():
            multiply(last_b * 2 + c)

        @pl.when(k == 2)
        def _():
            mate_part(last_f)

        @pl.when((k == 3) & (d > 1))
        def _():
            mate_part(last_b)

        @pl.when((i >= 3) & (i % 2 == 1))
        def _():
            cot_own_part((i - 3) // 2)

        @pl.when((i >= 6) & (i % 2 == 0))
        def _():
            cot_mate_part((i - 6) // 2)

    cot_own_part(7)
    multiply(((z + 4) % 8) * 2 + c)
    mate_part((z + 4) % 8)

    @pl.loop(5, 8)
    def _(n):
        cot_mate_part(n)

    before, here, after = neighbours(0)
    conv = before * taps_ref[0:1, :] + here * taps_ref[1:2, :] + after * taps_ref[2:3, :]
    cout[...] = conv
    mine_t = pl.ds(pl.multiple_of(s * 256, 256), 256)
    mix_t[:, mine_t] = (og_ref[...].astype(F32) * conv).T.astype(BF16)

    @pl.loop(1, 16)
    def _(i):
        remote(
            mix_t.at[:, mine_t], mix_t.at[:, mine_t], sent.at[MIXED], mix_recv.at[0], sp=(s + i) % 16
        ).start()

    def eight(k):
        return pl.ds(8 * k, 8)

    def dots_of(tt, k):
        return dot(g2[eight(k)].reshape(384, 256), wgu[tt], NT)

    def prepare(zz, k):
        value = dots_of(zz * 2 + 1 - c, k)
        q[zz, eight(k)] = value.astype(BF16).reshape(8, 48, 256)
        remote(
            q.at[zz, eight(k)], r.at[zz, eight(k)], sent.at[MATE_SUMS], rp_recv.at[zz, k], tp=mate
        ).start()

    @pl.loop(0, 4)
    def _(k):
        block = acc[pl.ds(4 * k, 4)].reshape(192, 256)
        pre_gate, pre_up = block[:, :128], block[:, 128:]
        grad_hidden = acc_h[pl.ds(4 * k, 4)].reshape(192, 128)
        sig = jax.nn.sigmoid(pre_gate)
        activated = pre_gate * sig
        hid[pl.ds(4 * k, 4)] = (activated * pre_up).astype(BF16).reshape(4, 48, 128)
        grad_gate = (grad_hidden * pre_up * sig * (1.0 + pre_gate * (1.0 - sig))).astype(BF16)
        grad_up = (grad_hidden * activated).astype(BF16)
        g2[pl.ds(4 * k, 4), :, pl.ds(0, 128)] = grad_gate.reshape(4, 48, 128)
        g2[pl.ds(4 * k, 4), :, pl.ds(128, 128)] = grad_up.reshape(4, 48, 128)

        @pl.when(k % 2 == 1)
        def _():
            prepare((z + 4) % 8, k // 2)

    def summed(zz, k):
        at = r.at[zz, eight(k)]
        remote(at, at, sent.at[MATE_SUMS], rp_recv.at[zz, k], tp=mate).wait_recv()
        return dots_of(zz * 2 + c, k) + r[zz, eight(k)].reshape(384, 256).astype(F32)

    def ring_send(h, d, k, incoming, outgoing, recv_sem, to):
        remote(
            outgoing.at[h, d - 1, eight(k)], incoming.at[h, d - 1, eight(k)],
            sent.at[SUMS], recv_sem.at[h, d - 1, k], tp=to,
        ).start()

    def half_of(ref, *index):
        return ref[index].reshape(384, 128).astype(F32)

    def ring_step(d, k, zz, incoming, outgoing, recv_sem, to, starts):
        value = summed(zz, k)
        outgoing[1, d - 1, eight(k)] = value[:, 128:].astype(BF16).reshape(8, 48, 128)

        @pl.when(starts)
        def _():
            outgoing[0, d - 1, eight(k)] = value[:, :128].astype(BF16).reshape(8, 48, 128)

        @pl.when(jnp.logical_not(starts))
        def _():
            arrived(incoming.at[0, d, eight(k)], recv_sem.at[0, d, k])
            both = value[:, :128] + half_of(incoming, 0, d, eight(k))
            outgoing[0, d - 1, eight(k)] = both.astype(BF16).reshape(8, 48, 128)

        ring_send(0, d, k, incoming, outgoing, recv_sem, to)

    def ring_step_2(d, k, incoming, outgoing, recv_sem, to, starts):
        @pl.when(jnp.logical_not(starts))
        def _():
            arrived(incoming.at[1, d, eight(k)], recv_sem.at[1, d, k])
            both = half_of(outgoing, 1, d - 1, eight(k)) + half_of(incoming, 1, d, eight(k))
            outgoing[1, d - 1, eight(k)] = both.astype(BF16).reshape(8, 48, 128)

        ring_send(1, d, k, incoming, outgoing, recv_sem, to)

    def grads(tt):
        x = rows[tt].reshape(768, 256)
        cot = cots[tt].reshape(768, 256)
        grad_gu[tt] = dot(x, g2[...].reshape(768, 256), TN).astype(BF16)
        columns = pl.ds(pl.multiple_of(tt * 256, 256), 256)
        grad_d[:, columns] = dot(hid[...].reshape(768, 128), cot, TN).astype(BF16)
        for copy in outputs(tt):
            copy.start()

    def outputs(tt):
        columns = pl.ds(pl.multiple_of(tt * 256, 256), 256)
        return [
            pltpu.make_async_copy(grad_gu.at[tt, :, pl.ds(0, 128)], gg_ref.at[tt], out_sem.at[0]),
            pltpu.make_async_copy(grad_gu.at[tt, :, pl.ds(128, 128)], gu_ref.at[tt], out_sem.at[1]),
            pltpu.make_async_copy(grad_d.at[:, columns], gd_ref.at[:, columns], out_sem.at[2]),
        ]

    def giving_back(h, peer):
        return remote(fin.at[h, peer], ret_ref.at[h, s], sent.at[RETURNED], ret_recv.at[h], sp=peer)

    def mine(h):
        return pltpu.make_async_copy(fin.at[h, s], ret_ref.at[h, s], ret_recv.at[h])

    def finish(h, k, value):
        for incoming, recv_sem in ((in_f, rf_recv), (in_b, rb_recv)):
            arrived(incoming.at[h, 0, eight(k)], recv_sem.at[h, 0, k])
            value = value + half_of(incoming, h, 0, eight(k))
        fin[h, eight(k)] = value.astype(BF16).reshape(8, 48, 128)
        for x in range(8):
            peer = 8 * k + x

            @pl.when(peer == s)
            def _():
                mine(h).start()

            @pl.when(peer != s)
            def _():
                giving_back(h, peer).start()

    def mc_f(h, d, k):
        at = mcf.at[h, ((z + 8 - d) % 8) * 2 + c, pl.ds(2 * k, 2)]
        return remote(at, at, sent.at[MIXER], mf_recv.at[h, d, k], tp=up)

    def mc_b(h, d, k):
        at = mcf.at[h, ((z + d) % 8) * 2 + c, pl.ds(2 * k, 2)]
        return remote(at, at, sent.at[MIXER], mb_recv.at[h, d, k], tp=down)

    def mc_mate(h, zz, core):
        at = mcf.at[h, zz * 2 + core]
        return remote(at, at, sent.at[MIXER], mp_recv.at[h, zz], tp=mate)

    tokens_half = pl.ds(2 * c, 2)

    def lanes(h):
        return pl.ds(128 * h, 128)

    def send_column(h, tt):
        @pl.when(tt == s)
        def _():
            pltpu.make_async_copy(
                mcf.at[h, s, tokens_half], col.at[s, tokens_half, :, lanes(h)], col_recv.at[h, y]
            ).start()

        @pl.when(tt != s)
        def _():
            remote(
                mcf.at[h, tt, tokens_half], col.at[s, tokens_half, :, lanes(h)],
                sent.at[COLUMN], col_recv.at[h, y], sp=tt,
            ).start()

    def from_mate(h, zz):
        mc_mate(h, zz, 1 - c).wait_recv()
        send_column(h, zz * 2 + 1 - c)

    def mixer_start(h):
        arrived(ret_ref.at[h], ret_recv.at[h])
        moe_grad = dot(pick_ref[...].reshape(768, 256), ret_ref[h].reshape(768, 128), TN)
        mixer = cot_ref[:, pl.ds(128 * h, 128)].astype(F32) + moe_grad
        mcf[h, t] = mixer.astype(BF16).reshape(4, 64, 128)
        for k in range(2):
            mc_f(h, 0, k).start()
            mc_b(h, 0, k).start()
        mc_mate(h, z, c).start()
        send_column(h, t)

    def mixer_step(h, d):
        zf, zb = (z + 8 - d) % 8, (z + d) % 8
        for k in range(2):
            @pl.when((d < 4) | (k == 0))
            def _():
                arrived(mcf.at[h, zf * 2 + c, pl.ds(2 * k, 2)], mf_recv.at[h, d - 1, k])

                @pl.when((d < 3) | ((d == 3) & (k == 0)))
                def _():
                    mc_f(h, d, k).start()

            @pl.when((d < 4) | (k == 1))
            def _():
                arrived(mcf.at[h, zb * 2 + c, pl.ds(2 * k, 2)], mb_recv.at[h, d - 1, k])

                @pl.when((d < 3) | ((d == 3) & (k == 1)))
                def _():
                    mc_b(h, d, k).start()

        mc_mate(h, zf, c).start()
        send_column(h, zf * 2 + c)

        @pl.when(d < 4)
        def _():
            mc_mate(h, zb, c).start()
            send_column(h, zb * 2 + c)

        lf, lb = (zf + 1) % 8, (zb + 7) % 8
        from_mate(h, lf)

        @pl.when(d > 1)
        def _():
            from_mate(h, lb)

    @pl.loop(0, 12)
    def _(i):
        k = i % 2
        even = k == 0

        @pl.when(i < 8)
        def _():
            d = 4 - i // 2
            zf, zb = (z + d) % 8, (z + 8 - d) % 8

            @pl.when((d < 4) | even)
            def _():
                ring_step(d, k, zf, in_f, out_f, rf_recv, up, (d == 4) | ((d == 3) & (~even)))

            @pl.when((d < 4) | (~even))
            def _():
                ring_step(d, k, zb, in_b, out_b, rb_recv, down, (d == 4) | ((d == 3) & even))

            prepare((z + d - 1) % 8, k)

            @pl.when(d > 1)
            def _():
                prepare((z + 9 - d) % 8, k)

        @pl.when(i >= 4)
        def _():
            d = 6 - i // 2

            @pl.when((d < 4) | even)
            def _():
                ring_step_2(d, k, in_f, out_f, rf_recv, up, (d == 4) | ((d == 3) & (~even)))

            @pl.when((d < 4) | (~even))
            def _():
                ring_step_2(d, k, in_b, out_b, rb_recv, down, (d == 4) | ((d == 3) & even))

        @pl.when((i >= 8) & (i < 10))
        def _():
            value = summed(z, k)
            fin[1, eight(k)] = value[:, 128:].astype(BF16).reshape(8, 48, 128)
            finish(0, k, value[:, :128])

        @pl.when(i < 4)
        def _():
            grads(12 + i)

        grads(i)

    finish(1, 0, half_of(fin, 1, eight(0)))
    finish(1, 1, half_of(fin, 1, eight(1)))
    mixer_start(0)
    mixer_step(0, jnp.int32(1))
    mixer_start(1)

    @pl.loop(2, 5)
    def _(d):
        mixer_step(0, d)
        mixer_step(1, d - 1)

    from_mate(0, (z + 4) % 8)
    mixer_step(1, jnp.int32(4))
    from_mate(1, (z + 4) % 8)

    full = jnp.concatenate([mcf[h, tt].reshape(256, 128) for tt in range(16) for h in range(2)], axis=1)
    grad_mixed = dot(full, op[...].reshape(4096, 256), NN)
    gog_ref[...] = (grad_mixed * cout[...]).astype(BF16)
    cin[...] = grad_mixed * og_ref[...].astype(F32)
    for copy in halo_copies(1):
        copy.start()

    def column_mate(h, k, core):
        at = col.at[part(k), pl.ds(2 * core, 2), :, lanes(h)]
        return remote(at, at, sent.at[COLUMN_MATE], colp_recv.at[h, (y + 4 - k) % 4], tp=mate)

    def put(i):
        held, out = ((gog_ref, gog_hbm), (gig_ref, gig_hbm), (gval_ref, gval_hbm))[i]
        return pltpu.make_async_copy(held, out, out_sem.at[3 + i])

    put_sums = pltpu.make_async_copy(gop_ref, gop_hbm, out_sem.at[6])

    put(0).start()
    for h in range(2):
        for k in range(4):
            arrived(col.at[part(k), tokens_half, :, lanes(h)], col_recv.at[h, (y + 4 - k) % 4])
            column_mate(h, k, c).start()
    arrived(mix_t.at[:, pl.ds(0, 15 * 256)], mix_recv.at[0])
    for h in range(2):
        for k in range(4):
            column_mate(h, k, 1 - c).wait_recv()
    gop_ref[...] = dot(mix_t[...], col[...].reshape(4096, 256), NN).T
    put_sums.start()

    before, here, after = neighbours(1)
    grad_in = after * taps_ref[0:1, :] + here * taps_ref[1:2, :] + before * taps_ref[2:3, :]
    gig_ref[...] = (grad_in * val_ref[...].astype(F32)).astype(BF16)
    gval_ref[...] = (grad_in * ig_ref[...].astype(F32)).astype(BF16)
    put(1).start()
    put(2).start()

    sent_all(rows.at[0, pl.ds(0, 15)], DISPATCH)
    sent_all(rows.at[pl.ds(0, 15)], ROWS)
    sent_all(cots.at[pl.ds(0, 8), pl.ds(0, 15)], COT)
    sent_all(cots.at[pl.ds(0, 8)], COT_MATE)
    sent_all(tokens.at[pl.ds(0, 7)], TOKEN_RING)
    sent_all(mix_t.at[:, pl.ds(0, 15 * 256)], MIXED)
    sent_all(q, MATE_SUMS)
    sent_all(q.at[pl.ds(0, 7)], SUMS)
    sent_all(fin.at[:, pl.ds(0, 15)], RETURNED)
    sent_all(mcf.at[:, pl.ds(0, 15)], MIXER)
    sent_all(mcf.at[:, pl.ds(0, 15), pl.ds(0, 2)], COLUMN)
    sent_all(col.at[:, pl.ds(0, 2)], COLUMN_MATE)
    pltpu.make_async_copy(grad_gu.at[:, :, pl.ds(0, 128)], gg_ref, out_sem.at[0]).wait()
    pltpu.make_async_copy(grad_gu.at[:, :, pl.ds(128, 128)], gu_ref, out_sem.at[1]).wait()
    pltpu.make_async_copy(grad_d, gd_ref, out_sem.at[2]).wait()
    for i in range(3):
        put(i).wait()
    put_sums.wait()


def mixer_and_experts(*operands):
    vm = lambda shape, dtype: pltpu.VMEM(shape, dtype)
    dma = lambda *shape: pltpu.SemaphoreType.DMA(shape)
    any_ = pl.BlockSpec(memory_space=pl.ANY)
    vmem = pl.BlockSpec(memory_space=pltpu.VMEM)
    tile = jax.ShapeDtypeStruct((256, 256), BF16)
    return pl.pallas_call(
        moe_kernel,
        out_shape=(
            tile, tile, tile,
            jax.ShapeDtypeStruct((256, 256), F32),
            jax.ShapeDtypeStruct((16, 256, 128), BF16),
            jax.ShapeDtypeStruct((16, 256, 128), BF16),
            jax.ShapeDtypeStruct((128, 4096), BF16),
        ),
        in_specs=[vmem] * 3 + [any_] * 9,
        out_specs=(any_,) * 7,
        scratch_shapes=[
            vm((256, 256), BF16),
            vm((256, 256), BF16),
            vm((256, 256), BF16),
            vm((256, 256), F32),
            vm((256, 256), BF16),
            vm((256, 256), BF16),
            vm((256, 256), BF16),
            vm((256, 256), BF16),
            vm((256, 256), BF16),
            vm((16, 48, 256), BF16),
            vm((16, 48, 128), F32),
            vm((8, 2, 128, 256), BF16),
            vm((16, 48, 256), BF16),
            vm((8, 16, 48, 256), BF16),
            vm((16, 16, 48, 256), BF16),
            vm((16, 16, 48, 256), BF16),
            vm((16, 256, 256), BF16),
            vm((128, 4096), BF16),
            vm((16, 48, 256), F32),
            vm((16, 48, 128), F32),
            vm((16, 48, 256), BF16),
            vm((16, 48, 128), BF16),
            vm((8, 16, 48, 256), BF16),
            vm((8, 16, 48, 256), BF16),
            vm((2, 4, 16, 48, 128), BF16),
            vm((2, 4, 16, 48, 128), BF16),
            vm((2, 4, 16, 48, 128), BF16),
            vm((2, 4, 16, 48, 128), BF16),
            vm((2, 16, 48, 128), BF16),
            vm((16, 256, 256), BF16),
            vm((128, 4096), BF16),
            vm((2, 16, 48, 128), BF16),
            vm((16, 256, 256), BF16),
            vm((256, 256), F32),
            vm((256, 256), F32),
            vm((2, 2, 8, 256), F32),
            vm((256, 4096), BF16),
            vm((2, 16, 4, 64, 128), BF16),
            vm((16, 4, 64, 256), BF16),
            dma(9), dma(7), dma(14),
            dma(4), dma(4, 4), dma(4, 4), dma(8), dma(8, 2), dma(2, 4, 2), dma(2, 4, 2), dma(2),
            dma(2, 2), dma(1), dma(2, 4, 2), dma(2, 4, 2), dma(2, 8), dma(2, 4), dma(2, 4),
            dma(4, 2), dma(4, 2), dma(8), dma(8),
        ],
        compiler_params=pltpu.CompilerParams(
            collective_id=1, has_side_effects=True, vmem_limit_bytes=67043328
        ),
        cost_estimate=pl.CostEstimate(flops=8_000_000_000, bytes_accessed=20_000_000, transcendentals=100_000),
        name="mixer_and_experts",
    )(*operands)


def write_out(*refs):
    sources, targets, held = refs[:7], refs[7:14], refs[14:21]
    wide, in_sem, out_sem = refs[21:24], refs[24], refs[25]
    steps = []
    for i, ref in enumerate(sources):
        pieces = 4 if i < 3 else 1
        size = ref.shape[0] // pieces
        staged = wide[i] if i < 3 else held[i]
        for p in range(pieces):
            at = pl.ds(p * size, size)
            n = len(steps)
            steps.append((
                i, at,
                pltpu.make_async_copy(ref.at[at], held[i].at[at], in_sem.at[n]),
                pltpu.make_async_copy(staged.at[at], targets[i].at[at], out_sem.at[n]),
            ))
    for _, _, fetch, _ in steps:
        fetch.start()
    for i, at, fetch, store in steps:
        fetch.wait()
        if i < 3:
            wide[i][at, :] = held[i][at, :].astype(F32)
        store.start()
    for _, _, _, store in steps:
        store.wait()


def written(*arrays):
    any_ = pl.BlockSpec(memory_space=pl.ANY)
    shapes = [jax.ShapeDtypeStruct(a.shape, F32 if i < 3 else a.dtype) for i, a in enumerate(arrays)]
    return pl.pallas_call(
        write_out,
        out_shape=tuple(shapes),
        in_specs=[any_] * len(shapes),
        out_specs=(any_,) * len(shapes),
        scratch_shapes=[pltpu.VMEM(a.shape, a.dtype) for a in arrays]
        + [pltpu.VMEM(a.shape, F32) for a in arrays[:3]]
        + [pltpu.SemaphoreType.DMA((16,)), pltpu.SemaphoreType.DMA((16,))],
        compiler_params=pltpu.CompilerParams(vmem_limit_bytes=67043328),
        name="write_out",
    )(*arrays)


def body(moe_input, out_gate, in_gate, values, conv_taps, out_proj, route_ids, route_gates, expert_gate, expert_up, expert_down, cotangent):
    gog, gig, gval, gop, gg, gu, gd = mixer_and_experts(
        route_ids.T, route_gates.T, conv_taps, moe_input, cotangent, out_gate, in_gate, values,
        expert_gate.reshape(16, 256, 128),
        expert_up.reshape(16, 256, 128),
        expert_down.reshape(128, 4096),
        out_proj.reshape(16, 256, 256),
    )
    gg, gu, gd, gop, gog, gig, gval = written(
        gg.reshape(4096, 128), gu.reshape(4096, 128), gd, gop, gog, gig, gval
    )
    return (gog, gig, gval, gop, gg.reshape(1, 4096, 128), gu.reshape(1, 4096, 128), gd.reshape(1, 128, 4096))


def solution(mesh):
    in_specs = (
        P("sp", "tp"), P("sp", "tp"), P("sp", "tp"), P("sp", "tp"), P(None, "tp"), P(None, "tp"),
        P("sp", None), P("sp", None),
        P("sp", None, "tp"), P("sp", None, "tp"), P("sp", "tp", None), P("sp", "tp"),
    )
    out_specs = (
        P("sp", "tp"), P("sp", "tp"), P("sp", "tp"), P("sp", "tp"),
        P("sp", None, "tp"), P("sp", None, "tp"), P("sp", "tp", None),
    )
    return jax.shard_map(body, mesh=mesh, in_specs=in_specs, out_specs=out_specs, check_vma=False)
```
